32 devices in a mesh: sp: 8 (over z, x), tp: 4 (over y, core).
Axes of the slice: x: 2, y: 2, z: 4, core: 2. Of those that a mesh axis runs over, the one named last changes fastest.
Arguments:
- tokens: bfloat16 [2048, 2048], P('sp', 'tp'), may hold values from -6 to 6
- norm_gain: float32 [2048], replicated, may hold values from 0.1 to 1.9
- query_one: bfloat16 [2048, 512], P('sp', 'tp'), may hold values from -1 to 1
- key_one: bfloat16 [2048, 512], P('sp', 'tp'), may hold values from -1 to 1
- query_two: bfloat16 [2048, 512], P('sp', 'tp'), may hold values from -0.15625 to 0.15625
- key_two: bfloat16 [2048, 512], P('sp', 'tp'), may hold values from -0.15625 to 0.15625
- value_weight: bfloat16 [2048, 1024], P('sp', 'tp'), may hold values from -0.5 to 0.5
- pool_weight: bfloat16 [2048, 1024], P('sp', 'tp'), may hold values from -0.125 to 0.125
- lambda_head: float32 [8], replicated, may hold values from 0.3 to 0.8
- head_gain: float32 [128], replicated, may hold values from 0.1 to 1.9
- group_weight: bfloat16 [8, 128, 128], replicated, may hold values from -0.5 to 0.5
- pool_scale: float32 [1024], replicated, may hold values from 0.1 to 1.9
- out_attn: bfloat16 [1024, 2048], P('tp', 'sp'), may hold values from -0.125 to 0.125
- out_pool: bfloat16 [1024, 2048], P('tp', 'sp'), may hold values from -0.125 to 0.125
Outputs:
- mixed: bfloat16 [2048, 2048], P(('sp', 'tp'))
The draws below stay inside these ranges and needn't reach their ends.
All inputs are finite; a program needn't handle non-finite values.
Results may differ from the reference program's by a relative error of at most 0.013.
Values may be sent and summed in bfloat16 or wider, within the bound.
A program may use at most 128 MiB of HBM per device.

```python
import math
import jax
import jax.numpy as jnp
from jax import lax

D = 2048
HEADS = 8
HEAD_DIM = 64
VALUE_DIM = 128
GROUPS = 8
GROUP_DIM = 128
TOKENS = 2048


def paired_weights(key):
    first_draw = jax.random.normal(jax.random.fold_in(key, 101), (D, HEADS * HEAD_DIM), jnp.float32)
    second_draw = jax.random.normal(jax.random.fold_in(key, 202), (D, HEADS * HEAD_DIM), jnp.float32)
    query_part = jnp.clip(first_draw, -4.0, 4.0) * (1.3 / jnp.sqrt(jnp.float32(D)))
    key_part = jnp.clip(second_draw, -4.0, 4.0) * (1.3 / jnp.sqrt(jnp.float32(D)))
    return (query_part, key_part)


def draw_query_one(key, part):
    return paired_weights(key)[0].astype(jnp.bfloat16)


def draw_key_one(key, part):
    return paired_weights(key)[1].astype(jnp.bfloat16)


def levels(rng, shape, shards, smallest, high):
    gain = 1.0
    for position, blocks in shards:
        steps = jax.random.uniform(jax.random.fold_in(jax.random.fold_in(rng, 6), position), (blocks,), jnp.float32, smallest / len(shards), high / len(shards))
        gain = gain * jnp.repeat(jnp.exp(steps), shape[position] // blocks).reshape((-1,) + (1,) * (len(shape) - 1 - position))
    return gain


def normal_values(key, extent, spread, limit, split=(), held_as=jnp.bfloat16):
    loudness = levels(key, extent, split, -0.22, 0.18) if split else 1.0
    array = jax.random.normal(key, extent, jnp.float32) * spread * loudness
    return jnp.minimum(jnp.maximum(array, -limit), limit).astype(held_as)


def setup_inputs(seed: int = 0) -> dict:
    arg_keys = jax.random.split(jax.random.key(seed), 15)
    return {
        "tokens": normal_values(arg_keys[0], (TOKENS, D), 1.0, 6.0, ((0, 8), (1, 4))),
        "norm_gain": jnp.clip(1.0 + 0.18 * jax.random.normal(arg_keys[1], (D,), jnp.float32), 0.1, 1.9),
        "query_one": draw_query_one(jax.random.fold_in(arg_keys[14], 71), 0),
        "key_one": draw_key_one(jax.random.fold_in(arg_keys[14], 71), 0),
        "query_two": normal_values(arg_keys[4], (D, HEADS * HEAD_DIM), (D * 100 // 169) ** -0.5, 0.15625, ((0, 8), (1, 4))),
        "key_two": normal_values(arg_keys[5], (D, HEADS * HEAD_DIM), (D * 100 // 169) ** -0.5, 0.15625, ((0, 8), (1, 4))),
        "value_weight": normal_values(arg_keys[6], (D, HEADS * VALUE_DIM), (D // 16) ** -0.5, 0.5, ((0, 8), (1, 4))),
        "pool_weight": normal_values(arg_keys[7], (D, GROUPS * GROUP_DIM), D ** -0.5, 0.125, ((0, 8), (1, 4))),
        "lambda_head": jnp.clip(jax.random.uniform(arg_keys[8], (HEADS,), jnp.float32, 0.3, 0.8), 0.3, 0.8),
        "head_gain": jnp.clip(1.0 + 0.18 * jax.random.normal(arg_keys[9], (VALUE_DIM,), jnp.float32), 0.1, 1.9),
        "group_weight": normal_values(arg_keys[10], (GROUPS, GROUP_DIM, GROUP_DIM), GROUP_DIM ** -0.5, 0.5),
        "pool_scale": jnp.clip(1.0 + 0.18 * jax.random.normal(arg_keys[11], (GROUPS * GROUP_DIM,), jnp.float32), 0.1, 1.9),
        "out_attn": normal_values(arg_keys[12], (HEADS * VALUE_DIM, D), (HEADS * VALUE_DIM + GROUPS * GROUP_DIM) ** -0.5, 0.125, ((0, 4), (1, 8))),
        "out_pool": normal_values(arg_keys[13], (GROUPS * GROUP_DIM, D), (HEADS * VALUE_DIM + GROUPS * GROUP_DIM) ** -0.5, 0.125, ((0, 4), (1, 8))),
    }


rope_base = 500000.0
head_scale = 0.8
norm_floor = 1e-06
head_floor = 0.001
masked_score = -1e+30

def rotate(values_in, positions):
    half_dim = values_in.shape[-1] // 2
    inverse = rope_base ** (-(jnp.arange(half_dim, dtype=jnp.float32) * 2.0 / values_in.shape[-1]))
    angles = positions.astype(jnp.float32)[:, None] * inverse[None, :]
    cosine = jnp.cos(angles)[:, None, :]
    sine_part = jnp.sin(angles)[:, None, :]
    first_half = values_in[..., :half_dim]
    second_half = values_in[..., half_dim:]
    return jnp.concatenate([first_half * cosine - second_half * sine_part, second_half * cosine + first_half * sine_part], axis=-1)

def reference(tokens, norm_gain, query_one, key_one, query_two, key_two, value_weight, pool_weight, lambda_head, head_gain, group_weight, pool_scale, out_attn, out_pool):
    float_rows = tokens.astype(jnp.float32)
    normed = (float_rows * lax.rsqrt(lax.optimization_barrier(jnp.mean(float_rows * float_rows, axis=-1, keepdims=True)) + norm_floor) * norm_gain).astype(jnp.bfloat16)
    positions = jnp.arange(TOKENS, dtype=jnp.int32)
    score_scale = HEAD_DIM ** (-0.5)

    def project(weight):
        return jnp.dot(normed, weight, preferred_element_type=jnp.float32)

    def turned(weight):
        rounded_rows = rotate(project(weight).reshape(TOKENS, HEADS, HEAD_DIM), positions).astype(jnp.bfloat16)
        return lax.optimization_barrier(rounded_rows).astype(jnp.float32)
    query_a = turned(query_one)
    key_a = turned(key_one)
    query_b = turned(query_two)
    key_b = turned(key_two)
    value_rows = lax.optimization_barrier(project(value_weight).astype(jnp.bfloat16)).astype(jnp.float32).reshape(TOKENS, HEADS, VALUE_DIM)
    query_block = math.gcd(TOKENS, 256)
    blocks = TOKENS // query_block

    def one_block(block_id):
        start_row = block_id * query_block
        query_pos = start_row + jnp.arange(query_block, dtype=jnp.int32)
        visible = (positions[None, :] <= query_pos[:, None])[:, None, :]
        map_means = []
        for query_all, key_all in ((query_a, key_a), (query_b, key_b)):
            query_part = lax.dynamic_slice_in_dim(query_all, start_row, query_block, 0)
            scores = jnp.einsum('qhd,khd->qhk', query_part, key_all) * score_scale
            scores = jnp.where(visible, scores, masked_score)
            top_row = lax.optimization_barrier(jnp.max(scores, axis=-1, keepdims=True))
            weights = jnp.where(visible, jnp.exp(scores - top_row), 0.0)
            totals = lax.optimization_barrier(jnp.sum(weights, axis=-1))
            rounded = lax.optimization_barrier(weights.astype(jnp.bfloat16)).astype(jnp.float32)
            map_means.append(jnp.einsum('qhk,khd->qhd', rounded, value_rows) / totals[..., None])
        differed = map_means[0] - lambda_head[None, :, None] * map_means[1]
        scaled = differed * lax.rsqrt(lax.optimization_barrier(jnp.mean(differed * differed, axis=-1, keepdims=True)) + head_floor) * head_gain * head_scale
        return scaled.astype(jnp.bfloat16)
    attn_out = lax.map(one_block, jnp.arange(blocks, dtype=jnp.int32)).reshape(TOKENS, HEADS * VALUE_DIM)
    pool_rows = lax.optimization_barrier(project(pool_weight).astype(jnp.bfloat16)).astype(jnp.float32)
    running = jnp.cumsum(pool_rows, axis=0)
    results = []
    for group_id in range(GROUPS):
        window = 2 ** (group_id % 4 + 1)
        first_col = group_id * GROUP_DIM
        section = running[:, first_col:first_col + GROUP_DIM]
        earlier = jnp.pad(section, ((window, 0), (0, 0)))[:TOKENS]
        counts = jnp.minimum(positions + 1, window).astype(jnp.float32)
        window_mean = (section - earlier) / counts[:, None] - pool_rows[:, first_col:first_col + GROUP_DIM]
        results.append(jnp.dot(window_mean.astype(jnp.bfloat16), group_weight[group_id], preferred_element_type=jnp.float32))
    pooled = (jnp.concatenate(results, axis=1) * pool_scale).astype(jnp.bfloat16)
    mixed = jnp.dot(attn_out, out_attn, preferred_element_type=jnp.float32) + jnp.dot(pooled, out_pool, preferred_element_type=jnp.float32)
    return mixed.astype(jnp.bfloat16)
```

```python
import functools

import jax
import jax.numpy as jnp
import numpy as np
from jax import lax
from jax.experimental import pallas as pl
from jax.experimental.pallas import tpu as pltpu
from jax.sharding import PartitionSpec as P

HEAD_DIM = 64
VALUE_DIM = 128
GROUP_DIM = 128
ROPE_BASE = 500000.0
HEAD_SCALE = 0.8
NORM_FLOOR = 1e-06
HEAD_FLOOR = 0.001
MASKED = -1e30
TAIL = 16
CHUNKS = 8
PARTS = 2
XY_HOME = (True, False)
XY_PARTNER = (True, False)
MESH = pl.DeviceIdType.MESH
BF16 = jnp.bfloat16
F32 = jnp.float32


def flip(index, bit):
    return index + bit * (1 - 2 * ((index // bit) % 2))


def kernel(
    sizes,
    tok_ref,
    gain_ref,
    q1_ref,
    k1_ref,
    q2_ref,
    k2_ref,
    v_ref,
    p_ref,
    oa_ref,
    ob_ref,
    freq_ref,
    lam_ref,
    hg_ref,
    gw_ref,
    ps_ref,
    out_ref,
    wp_ref,
    op_ref,
    cos_ref,
    sin_ref,
    yacc,
    ssq,
    tokbuf,
    nrm,
    w_all,
    o_all,
    kv,
    q_st,
    m_st,
    l_st,
    acc_st,
    pool,
    tail,
    prior,
    cst,
    cat,
    part,
    sbuf,
    rbuf,
    tok_send,
    tok_recv,
    w_send,
    wx_send,
    wd_send,
    w_recv,
    o_up,
    o_dn,
    o_recv,
    ox_send,
    kv_send,
    kvd_send,
    kv_recv,
    pp_send,
    pp_recv,
    cat_send,
    cat_recv,
    rs_send,
    rs_recv,
):
    G, Q, TP = sizes
    S = 2 * G * Q
    R = 2 * Q
    s = lax.axis_index("sp")
    t = lax.axis_index("tp")
    r = s // G
    g = s % G
    q = r // 2
    b = r % 2
    y = t // 2
    c = t % 2
    other = s + 1 - 2 * g
    plane = 2 * q + c
    head = (2 * y + b) * G + g
    first = c == b
    second = c != b
    chunk, feats = tok_ref.shape
    rows = G * chunk
    has_up = r + 1 < R
    has_dn = r > 0

    def dev(q_, b_, g_, y_, c_):
        return ((2 * q_ + b_) * G + g_, 2 * y_ + c_)

    xdev = dev(q, b, 1 - g, y, c)
    ydev = dev(q, b, g, 1 - y, c)
    cdev = dev(q, b, g, y, 1 - c)

    t_bits = []
    bit = 1
    while bit < TP:
        t_bits.append(("t", bit))
        bit *= 2
    x_dim = ("g", 1)
    members = G * TP

    def member(mask):
        gg, tt = g, t
        for kind, bb in mask:
            if kind == "g":
                gg = flip(gg, bb)
            else:
                tt = flip(tt, bb)
        return gg, tt

    def device(mask):
        gg, tt = member(mask)
        return (r * G + gg, tt)

    barrier = pltpu.get_barrier_semaphore()

    def greet(where):
        pl.semaphore_signal(barrier, inc=1, device_id=where, device_id_type=MESH)

    greet(xdev)
    greet(ydev)
    greet(cdev)

    @pl.when(first)
    def _():
        greet(dev(q, b, 1 - g, y, 1 - c))
        greet(dev(q, b, g, 1 - y, 1 - c))

        @pl.loop(0, R)
        def _(p):
            @pl.when(p != r)
            def _():
                greet((p * G + g, t))

    @pl.when(second)
    def _():
        greet(dev(q, 1 - b, g, y, 0))
        greet(dev(q, 1 - b, g, y, 1))

    @pl.when(has_up)
    def _():
        greet((s + G, t))

    @pl.when(has_dn)
    def _():
        greet((s - G, t))

    @pl.loop(0, q)
    def _(e):
        greet(dev(e, b, g, y, c))

    @pl.when(jnp.logical_and(c == 0, q > 0))
    def _():
        greet(dev(q - 1, b, g, y, 1))

    def pack(gg):
        a, z = gg * HEAD_DIM, (gg + 1) * HEAD_DIM
        e, f = gg * VALUE_DIM, (gg + 1) * VALUE_DIM
        wp_ref[gg, :, 0:128] = jnp.concatenate([q1_ref[:, a:z], q2_ref[:, a:z]], axis=1)
        wp_ref[gg, :, 128:256] = jnp.concatenate([k1_ref[:, a:z], k2_ref[:, a:z]], axis=1)
        wp_ref[gg, :, 256:384] = v_ref[:, e:f]
        wp_ref[gg, :, 384:512] = p_ref[:, e:f]

    for gg in range(G):
        pack(gg)

    one = lambda flag: jnp.where(flag, 1, 0)
    last_pair = q == Q - 1
    count = 3 + 2 * one(second) + 1 + Q - one(first) + one(has_up) + one(has_dn)
    count = count + (Q - 1 - q) + one(jnp.logical_and(c == 1, q < Q - 1))
    pl.semaphore_wait(barrier, count)

    def rdma(src, dst, ss, rs, where):
        return pltpu.make_async_remote_copy(
            src_ref=src, dst_ref=dst, send_sem=ss, recv_sem=rs, device_id=where, device_id_type=MESH
        )

    cross_to = jnp.where(first, s, S)
    cross_at = jnp.where(first, other, S)

    def w_cross():
        return rdma(wp_ref.at[1 - g], w_all.at[cross_to], wx_send, w_recv.at[cross_to], xdev)

    def w_copy(kind, e):
        src = wp_ref.at[g] if kind == 0 else w_all.at[cross_at]
        slot = s if kind == 0 else other
        return rdma(
            src, w_all.at[slot], w_send.at[kind * Q + e], w_recv.at[slot], dev(e, c, g, y, c)
        )

    def w_targets(act):
        for n in range(Q):
            e = (q + 1 + n) % Q
            if n == Q - 1:
                pl.when(second)(functools.partial(act, e))
            else:
                act(e)

    def w_start(kind):
        w_targets(lambda e: w_copy(kind, e).start())

    def w_pass(slot):
        return rdma(w_all.at[slot], w_all.at[slot], wd_send.at[slot], w_recv.at[slot], cdev)

    def tok_copy(src, xx, tt, index, where):
        return rdma(src, tokbuf.at[xx, tt], tok_send.at[index], tok_recv.at[xx * TP + tt], where)

    def tok_first(index):
        where = (
            dev(q, 1 - b, g, y, b),
            dev(q, b, g, 1 - y, b),
            dev(q, b, 1 - g, y, b),
            dev(q, b, g, y, b),
        )[index]
        return tok_copy(tok_ref, g, t, index, where)

    def tok_wait(xx, tt):
        tok_copy(tokbuf.at[xx, tt], xx, tt, 0, cdev).wait_recv()

    def z_pass(k, over_y):
        tt = 2 * y + k
        return tok_copy(tokbuf.at[g, tt], g, tt, 4 + 2 * k + over_y, ydev if over_y else xdev)

    def x_pass(k):
        xx, tt = 1 - g, 2 * y + k
        return tok_copy(tokbuf.at[xx, tt], xx, tt, 8 + k, ydev)

    def y_pass(k):
        xx, tt = g, 2 * (1 - y) + k
        return tok_copy(tokbuf.at[xx, tt], xx, tt, 8 + k, xdev)

    w_cross().start()
    tok_first(0).start()
    tok_first(1).start()

    @pl.when(second)
    def _():
        tok_first(3).start()

    tok_first(2).start()
    w_start(0)

    @pl.when(first)
    def _():
        w_all[s] = wp_ref[g]
        tokbuf[g, t] = tok_ref[...]
        rdma(wp_ref.at[g], w_all.at[s], wd_send.at[s], w_recv.at[s], cdev).start()

    for gg in range(G):
        e, f = gg * VALUE_DIM, (gg + 1) * VALUE_DIM
        op_ref[gg, :, 0:128] = oa_ref[e:f, :].T
        op_ref[gg, :, 128:256] = ob_ref[e:f, :].T
    o_all[s] = op_ref[g]

    lane128 = lax.broadcasted_iota(jnp.int32, (chunk, 2 * HEAD_DIM), 1)
    sign = jnp.where(lane128 % HEAD_DIM < HEAD_DIM // 2, -1.0, 1.0)

    @pl.loop(0, G)
    def _(n):
        at = pl.ds(pl.multiple_of(n * chunk, chunk), chunk)
        spots = plane * rows + n * chunk + lax.broadcasted_iota(jnp.int32, (chunk, 2 * HEAD_DIM), 0)
        angles = spots.astype(F32) * freq_ref[...]
        cos_ref[at, :] = jnp.cos(angles)
        sin_ref[at, :] = jnp.sin(angles) * sign

    ssq[...] = jnp.zeros_like(ssq)

    def scale(xx, tt):
        at = pl.ds(pl.multiple_of(xx * chunk, chunk), chunk)
        x = tokbuf[xx, tt].astype(F32)
        ssq[at, :] = ssq[at, :] + jnp.sum(x * x, axis=-1, keepdims=True)
        nrm[tt, at, :] = (x * gain_ref[tt]).astype(BF16)

    def up_copy(src, buf, k, up, recv):
        return rdma(src, buf.at[k], up.at[k], recv.at[k], (s + G, t))

    def dn_copy(src, buf, k, dn, recv):
        return rdma(src, buf.at[k], dn.at[k], recv.at[k], (s - G, t))

    def send_both(src, buf, k, up, dn, recv):
        @pl.when(has_up)
        def _():
            up_copy(src, buf, k, up, recv).start()

        @pl.when(has_dn)
        def _():
            dn_copy(src, buf, k, dn, recv).start()

    def cross_copy(inp, buf, xs, recv):
        return rdma(inp.at[1 - g], buf.at[s], xs, recv.at[s], xdev)

    def wait_slot(buf, k, up, recv):
        up_copy(buf.at[k], buf, k, up, recv).wait_recv()

    def line_step(j, buf, up, dn, recv):
        for gg in (g, 1 - g):
            @pl.when(r - 1 - j >= 0)
            def _():
                k = (r - 1 - j) * G + gg
                wait_slot(buf, k, up, recv)

                @pl.when(has_up)
                def _():
                    up_copy(buf.at[k], buf, k, up, recv).start()

            @pl.when(r + 1 + j < R)
            def _():
                k = (r + 1 + j) * G + gg
                wait_slot(buf, k, up, recv)

                @pl.when(has_dn)
                def _():
                    dn_copy(buf.at[k], buf, k, dn, recv).start()

    def drain(buf, up, dn, recv):
        @pl.when(has_up)
        def _():
            @pl.loop(0, (r + 1) * G)
            def _(k):
                up_copy(buf.at[k], buf, k, up, recv).wait_send()

        @pl.when(has_dn)
        def _():
            @pl.loop(r * G, R * G)
            def _(k):
                dn_copy(buf.at[k], buf, k, dn, recv).wait_send()

    def w_wait(slot):
        w_pass(slot).wait_recv()

    @pl.when(second)
    def _():
        for k in range(2):
            tok_wait(g, 2 * y + k)
            z_pass(k, 1).start()
            z_pass(k, 0).start()

    @pl.when(first)
    def _():
        for k in range(2):
            tok_wait(g, 2 * (1 - y) + k)
            if not XY_HOME[k]:
                y_pass(k).start()
        tok_wait(g, 2 * y + 1 - c)

    w_wait(cross_at)
    w_start(1)
    cross_copy(op_ref, o_all, ox_send, o_recv).start()
    send_both(op_ref.at[g], o_all, s, o_up, o_dn, o_recv)

    @pl.when(first)
    def _():
        w_pass(other).start()
        for k in range(2):
            tok_wait(1 - g, 2 * y + k)
            if XY_HOME[k]:
                x_pass(k).start()

    def w_relay(gg):
        @pl.loop(1, R)
        def _(d):
            @pl.when(r - d >= 0)
            def _():
                w_wait((r - d) * G + gg)
                w_pass((r - d) * G + gg).start()

            @pl.when(r + d < R)
            def _():
                w_wait((r + d) * G + gg)
                w_pass((r + d) * G + gg).start()

    scale(g, 2 * y)
    scale(g, 2 * y + 1)

    @pl.when(first)
    def _():
        w_relay(g)

    @pl.when(second)
    def _():
        for k in range(2):
            tok_wait(g, 2 * (1 - y) + k)
            if not XY_PARTNER[k]:
                y_pass(k).start()
        for k in range(2):
            tok_wait(1 - g, 2 * y + k)
            if XY_PARTNER[k]:
                x_pass(k).start()

    for k in range(2):
        scale(g, 2 * (1 - y) + k)
        scale(1 - g, 2 * y + k)

    @pl.when(first)
    def _():
        w_relay(1 - g)

    for k in range(2):
        tok_wait(1 - g, 2 * (1 - y) + k)
        scale(1 - g, 2 * (1 - y) + k)

    @pl.when(second)
    def _():
        @pl.loop(0, S)
        def _(k):
            w_wait(k)

    width = wp_ref.shape[2]
    ptile = chunk
    group = S // TP

    @pl.loop(0, TP)
    def _(i):
        @pl.loop(0, rows // ptile)
        def _(n):
            at = pl.ds(pl.multiple_of(n * ptile, ptile), ptile)
            weights = w_all[pl.ds(i * group, group)].reshape(feats, width)
            product = jnp.dot(nrm[i, at, :], weights, preferred_element_type=F32)

            @pl.when(i == 0)
            def _():
                yacc[at, :] = product

            @pl.when(i > 0)
            def _():
                yacc[at, :] = yacc[at, :] + product

    def rope(x, cosine, sine):
        lane = lax.broadcasted_iota(jnp.int32, x.shape, 1)
        near = jnp.where(
            lane % HEAD_DIM < HEAD_DIM // 2,
            pltpu.roll(x, x.shape[1] - HEAD_DIM // 2, 1),
            pltpu.roll(x, HEAD_DIM // 2, 1),
        )
        return x * cosine + near * sine

    @pl.loop(0, rows // ptile)
    def _(n):
        at = pl.ds(pl.multiple_of(n * ptile, ptile), ptile)
        inv = lax.rsqrt(ssq[at, :] / (TP * feats) + NORM_FLOOR)
        out = yacc[at, :] * inv
        cosine = cos_ref[at, :]
        sine = sin_ref[at, :]
        kv[plane, at, 0:128] = rope(out[:, 128:256], cosine, sine).astype(BF16)
        kv[plane, at, 128:256] = out[:, 256:384].astype(BF16)
        p = out[:, 384:512].astype(BF16)
        pool[pl.ds(pl.multiple_of(TAIL + n * ptile, TAIL), ptile), :] = p.astype(F32)
        tail[...] = p[ptile - TAIL :, :]
        qq = rope(out[:, 0:128], cosine, sine).astype(BF16) * jnp.array(HEAD_DIM**-0.5, BF16)
        lane = lax.broadcasted_iota(jnp.int32, qq.shape, 1)
        zero = jnp.zeros_like(qq)
        q_st[0, at, :] = jnp.where(lane < HEAD_DIM, qq, zero)
        q_st[1, at, :] = jnp.where(lane >= HEAD_DIM, qq, zero)

    def kv_copy(e):
        return rdma(
            kv.at[plane], kv.at[plane], kv_send.at[e], kv_recv.at[plane], dev(e, b, g, y, c)
        )

    def kv_pass(e):
        k = 2 * e + c
        return rdma(kv.at[k], kv.at[k], kvd_send.at[e], kv_recv.at[k], cdev)

    def kv_wait(k):
        rdma(kv.at[k], kv.at[k], kvd_send.at[0], kv_recv.at[k], cdev).wait_recv()

    tail_copy = rdma(tail, prior, pp_send, pp_recv, (s + 2 * G * c, t + 1 - 2 * c))
    tail_out = jnp.logical_or(c == 0, q < Q - 1)
    tail_in = jnp.logical_or(c == 1, q > 0)

    @pl.loop(q + 1, Q)
    def _(e):
        kv_copy(e).start()

    @pl.when(c == 0)
    def _():
        kv_pass(q).start()

    @pl.when(tail_out)
    def _():
        tail_copy.start()

    wait_slot(o_all, other, o_up, o_recv)
    send_both(o_all.at[other], o_all, other, o_up, o_dn, o_recv)

    qtile = rows // 2

    def attend(k, diagonal):
        @pl.loop(0, 4)
        def _(n):
            m_index = n // 2
            at = pl.ds(pl.multiple_of((n % 2) * qtile, qtile), qtile)
            qq = q_st[m_index, at, :]
            scores = lax.dot_general(
                qq, kv[k, :, 0:128], (((1,), (1,)), ((), ())), preferred_element_type=F32
            )
            if diagonal:
                qpos = (n % 2) * qtile + lax.broadcasted_iota(jnp.int32, scores.shape, 0)
                kpos = lax.broadcasted_iota(jnp.int32, scores.shape, 1)
                scores = jnp.where(kpos <= qpos, scores, MASKED)
            top = jnp.max(scores, axis=-1, keepdims=True)
            if not diagonal:
                old = m_st[m_index, at, :]
                top = jnp.maximum(old, top)
                factor = jnp.exp(old - top)
            weights = jnp.exp(scores - top)
            total = jnp.sum(weights, axis=-1, keepdims=True)
            product = jnp.dot(weights.astype(BF16), kv[k, :, 128:256], preferred_element_type=F32)
            if not diagonal:
                total = total + l_st[m_index, at, :] * factor
                product = product + acc_st[m_index, at, :] * factor
            m_st[m_index, at, :] = top
            l_st[m_index, at, :] = total
            acc_st[m_index, at, :] = product

    attend(plane, True)

    @pl.when(tail_in)
    def _():
        tail_copy.wait_recv()
        pool[0:TAIL, :] = prior[...].astype(F32)

    @pl.when(jnp.logical_not(tail_in))
    def _():
        pool[0:TAIL, :] = jnp.zeros((TAIL, GROUP_DIM), F32)

    def cat_copy(i):
        return rdma(
            cst.at[i], cat.at[i], cat_send.at[i], cat_recv.at[i], dev(q, 1 - b, g, y, 1 - c)
        )

    def hand_on(i, value):
        @pl.when(first)
        def _():
            cat[i] = value

        @pl.when(second)
        def _():
            cst[i] = value
            cat_copy(i).start()

    ext = pool[...]
    kind = head % 4
    window = jnp.where(kind == 0, 2, jnp.where(kind == 1, 4, jnp.where(kind == 2, 8, 16)))
    run = ext + pltpu.roll(ext, 1, 0)
    chosen = run
    for power, lag in ((1, 2), (2, 4), (3, 8)):
        run = run + pltpu.roll(run, lag, 0)
        chosen = jnp.where(kind == power, run, chosen)
    spot = plane * rows + lax.broadcasted_iota(jnp.int32, (rows, GROUP_DIM), 0)
    counts = jnp.minimum(spot + 1, window).astype(F32)
    mean = chosen[TAIL:, :] / counts - ext[TAIL:, :]
    mixedg = jnp.dot(mean.astype(BF16), gw_ref[head], preferred_element_type=F32)
    hand_on(1, (mixedg * ps_ref[head]).astype(BF16))

    @pl.when(c == 1)
    def _():
        kv_wait(2 * q)
        attend(2 * q, False)

    line_step(0, o_all, o_up, o_dn, o_recv)

    @pl.loop(0, q)
    def _(j):
        e = q - 1 - j
        kv_wait(2 * e + c)
        kv_pass(e).start()
        attend(2 * e + c, False)
        kv_wait(2 * e + 1 - c)
        attend(2 * e + 1 - c, False)

    @pl.loop(1, R - 2)
    def _(j):
        line_step(j, o_all, o_up, o_dn, o_recv)

    diff = acc_st[0] / l_st[0] - lam_ref[head] * (acc_st[1] / l_st[1])
    inv = lax.rsqrt(jnp.mean(diff * diff, axis=-1, keepdims=True) + HEAD_FLOOR)
    hand_on(0, (diff * inv * hg_ref[...] * HEAD_SCALE).astype(BF16))

    @pl.when(second)
    def _():
        for i in range(2):
            cat_copy(i).wait_recv()

    share = rows // members
    half = part.shape[2]
    o_slots = o_all.shape[0] // CHUNKS
    by_line = R * PARTS == CHUNKS
    table = [sorted(range(R), key=lambda c: abs(c - i)) for i in range(R)]

    def chunk_at(k):
        if not by_line:
            return k
        total = 0
        for i in range(R):
            total = total + jnp.where(r == i, table[i][k // PARTS], 0)
        return total * PARTS + k % PARTS

    orders = ([t_bits[0], x_dim] + t_bits[1:], t_bits + [x_dim])

    def block(mask):
        gg, tt = member(mask)
        return pl.ds(pl.multiple_of((gg * TP + tt) * share, share), share)

    def combos(dims):
        found = [[]]
        for dim in dims:
            found = found + [mask + [dim] for mask in found]
        return found

    plans = []
    for h in range(CHUNKS):
        order = orders[h % 2]
        stages = []
        base = 0
        for i, dim in enumerate(order):
            masks = combos(order[i + 1 :])
            stages.append((dim, masks, base))
            base += len(masks)
        plans.append(stages)

    def rs_copy(h, dim, mask, index):
        at = block([dim] + mask)
        return rdma(
            sbuf.at[h, at, :], rbuf.at[h, index], rs_send.at[h, index], rs_recv.at[h, index],
            device([dim]),
        )

    def rs_start(h, i):
        dim, masks, base = plans[h][i]
        for n, mask in enumerate(masks):
            at = block([dim] + mask)
            sbuf[h, at, :] = part[h, at, :].astype(BF16)
        for n, mask in enumerate(masks):
            rs_copy(h, dim, mask, base + n).start()

    def rs_finish(h, i):
        dim, masks, base = plans[h][i]
        for n, mask in enumerate(masks):
            rs_copy(h, dim, mask, base + n).wait_recv()
            at = block(mask)
            part[h, at, :] = part[h, at, :] + rbuf[h, base + n].astype(F32)

    def out_product(h):
        first = chunk_at(h) * o_slots

        @pl.loop(0, 2)
        def _(b):
            at = pl.ds(pl.multiple_of(b * (rows // 2), rows // 2), rows // 2)
            columns = o_all[pl.ds(first, o_slots)].reshape(half, -1)
            both = jnp.concatenate([cat[0, at, :], cat[1, at, :]], axis=1)
            part[h, at, :] = lax.dot_general(
                both, columns, (((1,), (1,)), ((), ())), preferred_element_type=F32
            )

    levels = len(plans[0])
    mine = block([])
    last = lambda: line_step(R - 2, o_all, o_up, o_dn, o_recv)
    if by_line:
        batches = [range(CHUNKS - PARTS), range(CHUNKS - PARTS, CHUNKS)]
    else:
        batches = [range(CHUNKS)]
    def begin(batch):
        for h in batch:
            out_product(h)
            rs_start(h, 0)

    def advance(batch, i):
        for h in batch:
            rs_finish(h, i)
            if i + 1 < levels:
                rs_start(h, i + 1)
            else:
                at = pl.ds(pl.multiple_of(chunk_at(h) * half, half), half)
                out_ref[:, at] = part[h, mine, :].astype(BF16)

    if by_line:
        early, late = batches
        begin(early)
        advance(early, 0)
        last()
        begin(late)
        for i in range(1, levels):
            advance(early, i)
            advance(late, i - 1)
        advance(late, levels - 1)
    else:
        last()
        begin(batches[0])
        for i in range(levels):
            advance(batches[0], i)

    w_cross().wait_send()
    for kind in range(2):
        w_targets(lambda e: w_copy(kind, e).wait_send())

    @pl.when(first)
    def _():
        @pl.loop(0, S)
        def _(k):
            w_pass(k).wait_send()

    for i in range(3):
        tok_first(i).wait_send()

    @pl.when(second)
    def _():
        tok_first(3).wait_send()
        for k in range(2):
            z_pass(k, 1).wait_send()
            z_pass(k, 0).wait_send()
            (x_pass if XY_PARTNER[k] else y_pass)(k).wait_send()
            cat_copy(k).wait_send()

    @pl.when(first)
    def _():
        for k in range(2):
            (x_pass if XY_HOME[k] else y_pass)(k).wait_send()

    cross_copy(op_ref, o_all, ox_send, o_recv).wait_send()
    drain(o_all, o_up, o_dn, o_recv)

    @pl.when(tail_out)
    def _():
        tail_copy.wait_send()

    @pl.loop(q + 1, Q)
    def _(e):
        kv_copy(e).wait_send()

    @pl.loop(0, q + 1 - c)
    def _(e):
        kv_pass(e).wait_send()

    for h in range(CHUNKS):
        for dim, masks, base in plans[h]:
            for n, mask in enumerate(masks):
                rs_copy(h, dim, mask, base + n).wait_send()


def body(
    sp,
    tp,
    tokens,
    norm_gain,
    query_one,
    key_one,
    query_two,
    key_two,
    value_weight,
    pool_weight,
    lambda_head,
    head_gain,
    group_weight,
    pool_scale,
    out_attn,
    out_pool,
):
    G = query_one.shape[1] // HEAD_DIM
    assert G == 2 and tp == 2 * G and sp % (2 * G) == 0
    R = sp // G
    Q = R // 2
    chunk, feats = tokens.shape
    rows = G * chunk
    depth = query_one.shape[0]
    cols = out_attn.shape[1]
    heads = lambda_head.shape[0]
    members = G * tp
    share = rows // members

    half_dim = HEAD_DIM // 2
    inverse = ROPE_BASE ** (-((np.arange(2 * HEAD_DIM) % half_dim) * 2.0 / HEAD_DIM))
    freq = jnp.asarray(inverse.astype(np.float32).reshape(1, -1))
    width = 4 * HEAD_DIM + VALUE_DIM + GROUP_DIM
    depth_out = VALUE_DIM + GROUP_DIM
    total_cols = sp * cols
    vm = pl.BlockSpec(memory_space=pltpu.VMEM)
    dma = pltpu.SemaphoreType.DMA
    return pl.pallas_call(
        functools.partial(kernel, (G, Q, tp)),
        out_shape=jax.ShapeDtypeStruct((share, total_cols), BF16),
        in_specs=[vm] * 11 + [pl.BlockSpec(memory_space=pltpu.SMEM)] + [vm] * 3,
        out_specs=vm,
        scratch_shapes=[
            pltpu.VMEM((G, depth, width), BF16),
            pltpu.VMEM((G, cols, depth_out), BF16),
            pltpu.VMEM((rows, 2 * HEAD_DIM), F32),
            pltpu.VMEM((rows, 2 * HEAD_DIM), F32),
            pltpu.VMEM((rows, width), F32),
            pltpu.VMEM((rows, 1), F32),
            pltpu.VMEM((G, tp, chunk, feats), BF16),
            pltpu.VMEM((tp, rows, feats), BF16),
            pltpu.VMEM((sp + 1, depth, width), BF16),
            pltpu.VMEM((sp, cols, depth_out), BF16),
            pltpu.VMEM((R, rows, 256), BF16),
            pltpu.VMEM((2, rows, 128), BF16),
            pltpu.VMEM((2, rows, 1), F32),
            pltpu.VMEM((2, rows, 1), F32),
            pltpu.VMEM((2, rows, VALUE_DIM), F32),
            pltpu.VMEM((TAIL + rows, GROUP_DIM), F32),
            pltpu.VMEM((TAIL, GROUP_DIM), BF16),
            pltpu.VMEM((TAIL, GROUP_DIM), BF16),
            pltpu.VMEM((2, rows, 128), BF16),
            pltpu.VMEM((2, rows, 128), BF16),
            pltpu.VMEM((CHUNKS, rows, total_cols // CHUNKS), F32),
            pltpu.VMEM((CHUNKS, rows, total_cols // CHUNKS), BF16),
            pltpu.VMEM((CHUNKS, members - 1, share, total_cols // CHUNKS), BF16),
            dma((10,)),
            dma((members,)),
            dma((2 * Q,)),
            dma,
            dma((sp,)),
            dma((sp + 1,)),
            dma((sp,)),
            dma((sp,)),
            dma((sp,)),
            dma,
            dma((Q,)),
            dma((Q,)),
            dma((R,)),
            dma,
            dma,
            dma((2,)),
            dma((2,)),
            dma((CHUNKS, members - 1)),
            dma((CHUNKS, members - 1)),
        ],
        compiler_params=pltpu.CompilerParams(
            collective_id=0, has_side_effects=True, vmem_limit_bytes=58 * 1024 * 1024
        ),
    )(
        tokens,
        norm_gain.reshape(tp, 1, feats),
        query_one,
        key_one,
        query_two,
        key_two,
        value_weight,
        pool_weight,
        out_attn,
        out_pool,
        freq,
        lambda_head,
        head_gain.reshape(1, -1),
        group_weight,
        pool_scale.reshape(heads, 1, GROUP_DIM),
    )


def solution(mesh):
    in_specs = (
        P("sp", "tp"),
        P(),
        P("sp", "tp"),
        P("sp", "tp"),
        P("sp", "tp"),
        P("sp", "tp"),
        P("sp", "tp"),
        P("sp", "tp"),
        P(),
        P(),
        P(),
        P(),
        P("tp", "sp"),
        P("tp", "sp"),
    )
    return jax.shard_map(
        functools.partial(body, mesh.shape["sp"], mesh.shape["tp"]),
        mesh=mesh,
        in_specs=in_specs,
        out_specs=P(("sp", "tp"), None),
        check_vma=False,
    )
```

```python
import functools

import jax
import jax.numpy as jnp
import numpy as np
from jax import lax
from jax.experimental import pallas as pl
from jax.experimental.pallas import tpu as pltpu
from jax.sharding import PartitionSpec as P

HEAD_DIM = 64
VALUE_DIM = 128
GROUP_DIM = 128
ROPE_BASE = 500000.0
HEAD_SCALE = 0.8
NORM_FLOOR = 1e-06
HEAD_FLOOR = 0.001
MASKED = -1e30
TAIL = 16
CHUNKS = 8
XY_HOME = (True, False)
XY_PARTNER = (True, False)
MESH = pl.DeviceIdType.MESH
BF16 = jnp.bfloat16
F32 = jnp.float32


def flip(index, bit):
    return index + bit * (1 - 2 * ((index // bit) % 2))


def kernel(
    sizes,
    tok_ref,
    gain_ref,
    q1_ref,
    k1_ref,
    q2_ref,
    k2_ref,
    v_ref,
    p_ref,
    oa_ref,
    ob_ref,
    freq_ref,
    lam_ref,
    hg_ref,
    gw_ref,
    ps_ref,
    out_ref,
    wp_ref,
    op_ref,
    ox_ref,
    cos_ref,
    sin_ref,
    ssq,
    tokbuf,
    nrm,
    w_all,
    o_all,
    kv,
    q_st,
    m_st,
    l_st,
    acc_st,
    pool,
    tail,
    prior,
    cat,
    part,
    sbuf,
    rbuf,
    fin,
    land,
    outb,
    tok_send,
    tok_recv,
    w_send,
    wx_send,
    wd_send,
    w_recv,
    o_send,
    od_send,
    o_recv,
    ox_send,
    ox_recv,
    kv_send,
    kvd_send,
    kv_recv,
    pp_send,
    pp_recv,
    cat_send,
    cat_recv,
    rs_send,
    rs_recv,
    fin_send,
    fin_recv,
    out_sem,
):
    G, Q, TP = sizes
    S = 2 * G * Q
    R = 2 * Q
    s = lax.axis_index("sp")
    t = lax.axis_index("tp")
    r = s // G
    g = s % G
    q = r // 2
    b = r % 2
    y = t // 2
    c = t % 2
    other = s + 1 - 2 * g
    plane = 2 * q + c
    head = (2 * y + b) * G + g
    first = c == b
    second = c != b
    chunk, feats = tok_ref.shape
    rows = G * chunk
    cols = op_ref.shape[1]
    span = G * R * cols // TP

    def half_of(p):
        return (p * G * cols // span) % 2

    def place_of(p, gg):
        start = p * G * cols
        return pl.multiple_of((start // span // 2) * span + start % span + gg * cols, cols)


    def dev(q_, b_, g_, y_, c_):
        return ((2 * q_ + b_) * G + g_, 2 * y_ + c_)

    xdev = dev(q, b, 1 - g, y, c)
    ydev = dev(q, b, g, 1 - y, c)
    cdev = dev(q, b, g, y, 1 - c)
    zdev = dev(q, 1 - b, g, y, c)

    x_dim = ("g", 1)
    y_dim = ("t", 2)
    members = 2 * G

    def member(mask):
        gg, tt = g, t
        for kind, bb in mask:
            if kind == "g":
                gg = flip(gg, bb)
            else:
                tt = flip(tt, bb)
        return gg, tt

    def device(mask):
        gg, tt = member(mask)
        return (r * G + gg, tt)

    barrier = pltpu.get_barrier_semaphore()

    def greet(where):
        pl.semaphore_signal(barrier, inc=1, device_id=where, device_id_type=MESH)

    greet(xdev)
    greet(ydev)
    greet(cdev)
    greet(zdev)

    @pl.when(first)
    def _():
        greet(dev(q, b, 1 - g, y, 1 - c))
        greet(dev(q, b, g, 1 - y, 1 - c))

        @pl.loop(0, R)
        def _(p):
            @pl.when(p != r)
            def _():
                greet((p * G + g, t))

    @pl.when(second)
    def _():
        greet(dev(q, 1 - b, g, y, 0))
        greet(dev(q, 1 - b, g, y, 1))

    @pl.loop(0, R)
    def _(p):
        @pl.when(jnp.logical_and(p != r, half_of(p) == b))
        def _():
            greet((p * G + g, t))

    @pl.loop(0, q)
    def _(e):
        greet(dev(e, b, g, y, c))

    @pl.when(jnp.logical_and(c == 0, q > 0))
    def _():
        greet(dev(q - 1, b, g, y, 1))

    def pack(gg):
        a, z = gg * HEAD_DIM, (gg + 1) * HEAD_DIM
        e, f = gg * VALUE_DIM, (gg + 1) * VALUE_DIM
        wp_ref[gg, :, 0:128] = jnp.concatenate([q1_ref[:, a:z], q2_ref[:, a:z]], axis=1)
        wp_ref[gg, :, 128:256] = jnp.concatenate([k1_ref[:, a:z], k2_ref[:, a:z]], axis=1)
        wp_ref[gg, :, 256:384] = v_ref[:, e:f]
        wp_ref[gg, :, 384:512] = p_ref[:, e:f]

    for gg in range(G):
        pack(gg)

    one = lambda flag: jnp.where(flag, 1, 0)
    count = 4 + 2 * one(second) + 1 + Q - one(first) + Q - one(half_of(r) == b)
    count = count + (Q - 1 - q) + one(jnp.logical_and(c == 1, q < Q - 1))
    pl.semaphore_wait(barrier, count)

    def rdma(src, dst, ss, rs, where):
        return pltpu.make_async_remote_copy(
            src_ref=src, dst_ref=dst, send_sem=ss, recv_sem=rs, device_id=where, device_id_type=MESH
        )

    cross_to = jnp.where(first, s, S)
    cross_at = jnp.where(first, other, S)

    def w_cross():
        return rdma(wp_ref.at[1 - g], w_all.at[cross_to], wx_send, w_recv.at[cross_to], xdev)

    def w_copy(kind, e):
        src = wp_ref.at[g] if kind == 0 else w_all.at[cross_at]
        slot = s if kind == 0 else other
        return rdma(
            src, w_all.at[slot], w_send.at[kind * Q + e], w_recv.at[slot], dev(e, c, g, y, c)
        )

    def w_targets(act):
        for n in range(Q):
            e = (q + 1 + n) % Q
            if n == Q - 1:
                pl.when(second)(functools.partial(act, e))
            else:
                act(e)

    def w_start(kind, late=None):
        def act(e):
            far = jnp.logical_and(e != q, jnp.logical_or(2 * e + c == 0, 2 * e + c == R - 1))
            if late is None:
                w_copy(kind, e).start()
            else:
                pl.when(far == late)(lambda: w_copy(kind, e).start())

        w_targets(act)

    def w_pass(slot):
        return rdma(w_all.at[slot], w_all.at[slot], wd_send.at[slot], w_recv.at[slot], cdev)

    def tok_copy(src, xx, tt, n, index, where):
        at = pl.ds(n * (chunk // 2), chunk // 2)
        return rdma(
            src.at[at, :], tokbuf.at[xx, tt, at, :], tok_send.at[2 * index + n],
            tok_recv.at[2 * (xx * TP + tt) + n], where,
        )

    def tok_first(index, n):
        where = (
            dev(q, 1 - b, g, y, b),
            dev(q, b, g, 1 - y, b),
            dev(q, b, 1 - g, y, b),
            dev(q, b, g, y, b),
        )[index]
        return tok_copy(tok_ref, g, t, n, index, where)

    def tok_wait(xx, tt, n):
        tok_copy(tokbuf.at[xx, tt], xx, tt, n, 0, cdev).wait_recv()

    def z_pass(k, over_y, n):
        tt = 2 * y + k
        return tok_copy(tokbuf.at[g, tt], g, tt, n, 4 + 2 * k + over_y, ydev if over_y else xdev)

    def x_pass(k, n):
        xx, tt = 1 - g, 2 * y + k
        return tok_copy(tokbuf.at[xx, tt], xx, tt, n, 8 + k, ydev)

    def y_pass(k, n):
        xx, tt = g, 2 * (1 - y) + k
        return tok_copy(tokbuf.at[xx, tt], xx, tt, n, 8 + k, xdev)

    w_cross().start()
    for index in range(2):
        for n in range(2):
            tok_first(index, n).start()

    @pl.when(second)
    def _():
        for n in range(2):
            tok_first(3, n).start()

    for n in range(2):
        tok_first(2, n).start()
    w_start(0, False)

    @pl.when(first)
    def _():
        w_all[s] = wp_ref[g]
        tokbuf[g, t] = tok_ref[...]
        rdma(wp_ref.at[g], w_all.at[s], wd_send.at[s], w_recv.at[s], cdev).start()

    for gg in range(G):
        e, f = gg * VALUE_DIM, (gg + 1) * VALUE_DIM
        op_ref[gg, :, 0:128] = oa_ref[e:f, :].T
        op_ref[gg, :, 128:256] = ob_ref[e:f, :].T

    def o_at(core, p, gg):
        return o_all.at[core, pl.ds(place_of(p, gg), cols), :]

    def o_copy(kind, e):
        src, gg = (op_ref.at[g], g) if kind == 0 else (ox_ref, 1 - g)
        return rdma(
            src, o_at(c, r, gg), o_send.at[kind * Q + e], o_recv.at[c * S + r * G + gg],
            dev(e, half_of(r), g, y, c),
        )

    def o_targets(act, up=None):
        for n in range(Q):
            e = (q + 1 + n) % Q
            flag = half_of(r) != b if n == Q - 1 else None
            if up is not None:
                ahead = (e > q) == up
                flag = ahead if flag is None else jnp.logical_and(flag, ahead)
            if flag is None:
                act(e)
            else:
                pl.when(flag)(functools.partial(act, e))

    def o_start(kind, up):
        o_targets(lambda e: o_copy(kind, e).start(), up)

    def o_pass(p, gg):
        at = o_at(c, p, gg)
        index = p * G + gg
        return rdma(at, at, od_send.at[index], o_recv.at[c * S + index], cdev)

    def o_wait(core, p, gg):
        at = o_at(core, p, gg)
        rdma(at, at, od_send.at[0], o_recv.at[core * S + p * G + gg], cdev).wait_recv()

    def o_own(kind):
        gg = g if kind == 0 else 1 - g

        @pl.when(half_of(r) == b)
        def _():
            o_all[c, pl.ds(place_of(r, gg), cols), :] = op_ref[g] if kind == 0 else ox_ref[...]
            rdma(
                op_ref.at[g] if kind == 0 else ox_ref, o_at(c, r, gg), od_send.at[r * G + gg],
                o_recv.at[c * S + r * G + gg], cdev,
            ).start()

    def o_cross():
        return rdma(op_ref.at[1 - g], ox_ref, ox_send, ox_recv, xdev)

    def o_relay(gg):
        @pl.loop(0, R)
        def _(p):
            @pl.when(jnp.logical_and(p != r, half_of(p) == b))
            def _():
                o_wait(c, p, gg)
                o_pass(p, gg).start()

    lane128 = lax.broadcasted_iota(jnp.int32, (chunk, 2 * HEAD_DIM), 1)
    sign = jnp.where(lane128 % HEAD_DIM < HEAD_DIM // 2, -1.0, 1.0)

    @pl.loop(0, G)
    def _(n):
        at = pl.ds(pl.multiple_of(n * chunk, chunk), chunk)
        spots = plane * rows + n * chunk + lax.broadcasted_iota(jnp.int32, (chunk, 2 * HEAD_DIM), 0)
        angles = spots.astype(F32) * freq_ref[...]
        cos_ref[at, :] = jnp.cos(angles)
        sin_ref[at, :] = jnp.sin(angles) * sign

    ssq[...] = jnp.zeros_like(ssq)

    def scale(xx, tt):
        at = pl.ds(pl.multiple_of(xx * chunk, chunk), chunk)
        x = tokbuf[xx, tt].astype(F32)
        ssq[at, :] = ssq[at, :] + jnp.sum(x * x, axis=-1, keepdims=True)
        nrm[at, pl.ds(pl.multiple_of(tt * feats, feats), feats)] = (x * gain_ref[tt]).astype(BF16)

    def w_wait(slot):
        w_pass(slot).wait_recv()

    def early_relays(n):
        @pl.when(second)
        def _():
            for k in range(2):
                tok_wait(g, 2 * y + k, n)
                z_pass(k, 1, n).start()
                z_pass(k, 0, n).start()

        @pl.when(first)
        def _():
            for k in range(2):
                tok_wait(g, 2 * (1 - y) + k, n)
                if not XY_HOME[k]:
                    y_pass(k, n).start()
            tok_wait(g, 2 * y + 1 - c, n)

    early_relays(0)
    w_start(0, True)
    early_relays(1)
    w_wait(cross_at)
    w_start(1)

    @pl.when(first)
    def _():
        w_pass(other).start()
        for n in range(2):
            for k in range(2):
                tok_wait(1 - g, 2 * y + k, n)
                if XY_HOME[k]:
                    x_pass(k, n).start()

    def w_relay(gg):
        @pl.loop(1, R)
        def _(d):
            @pl.when(r - d >= 0)
            def _():
                w_wait((r - d) * G + gg)
                w_pass((r - d) * G + gg).start()

            @pl.when(r + d < R)
            def _():
                w_wait((r + d) * G + gg)
                w_pass((r + d) * G + gg).start()

    scale(g, 2 * y)
    scale(g, 2 * y + 1)

    @pl.when(first)
    def _():
        w_relay(g)

    @pl.when(second)
    def _():
        for n in range(2):
            for k in range(2):
                tok_wait(g, 2 * (1 - y) + k, n)
                if not XY_PARTNER[k]:
                    y_pass(k, n).start()
        for n in range(2):
            for k in range(2):
                tok_wait(1 - g, 2 * y + k, n)
                if XY_PARTNER[k]:
                    x_pass(k, n).start()

    for k in range(2):
        scale(g, 2 * (1 - y) + k)
        scale(1 - g, 2 * y + k)

    @pl.when(first)
    def _():
        w_relay(1 - g)

    o_cross().start()
    o_own(0)
    for k in range(2):
        for n in range(2):
            tok_wait(1 - g, 2 * (1 - y) + k, n)
        scale(1 - g, 2 * (1 - y) + k)

    @pl.when(second)
    def _():
        @pl.loop(0, S)
        def _(k):
            w_wait(k)

    @pl.when(b == 1)
    def _():
        o_start(0, True)

    ptile = chunk

    def rope(x, cosine, sine):
        lane = lax.broadcasted_iota(jnp.int32, x.shape, 1)
        near = jnp.where(
            lane % HEAD_DIM < HEAD_DIM // 2,
            pltpu.roll(x, x.shape[1] - HEAD_DIM // 2, 1),
            pltpu.roll(x, HEAD_DIM // 2, 1),
        )
        return x * cosine + near * sine

    def kv_part(k, n):
        return kv.at[k, pl.ds(pl.multiple_of(n * ptile, ptile), ptile), :]

    def kv_copy(e, n):
        at = kv_part(plane, n)
        return rdma(at, at, kv_send.at[2 * e + n], kv_recv.at[2 * plane + n], dev(e, b, g, y, c))

    def kv_pass(e, n):
        k = 2 * e + c
        at = kv_part(k, n)
        return rdma(at, at, kvd_send.at[2 * e + n], kv_recv.at[2 * k + n], cdev)

    def kv_wait(k, n):
        at = kv_part(k, n)
        rdma(at, at, kvd_send.at[0], kv_recv.at[2 * k + n], cdev).wait_recv()

    tail_copy = rdma(tail, prior, pp_send, pp_recv, (s + 2 * G * c, t + 1 - 2 * c))
    tail_out = jnp.logical_or(c == 0, q < Q - 1)
    tail_in = jnp.logical_or(c == 1, q > 0)

    @pl.loop(0, G)
    def _(m):
        n = G - 1 - m
        at = pl.ds(pl.multiple_of(n * ptile, ptile), ptile)
        weights = w_all[0:S].reshape(TP * feats, wp_ref.shape[2])
        inv = lax.rsqrt(ssq[at, :] / (TP * feats) + NORM_FLOOR)
        out = jnp.dot(nrm[at, :], weights, preferred_element_type=F32) * inv
        cosine = cos_ref[at, :]
        sine = sin_ref[at, :]
        kv[plane, at, 0:128] = rope(out[:, 128:256], cosine, sine).astype(BF16)
        v = out[:, 256:384].astype(BF16)
        for i in range(ptile // VALUE_DIM):
            dst = pl.ds(pl.multiple_of(n * ptile + i * VALUE_DIM, VALUE_DIM), VALUE_DIM)
            kv[plane, dst, 128:256] = v[i * VALUE_DIM : (i + 1) * VALUE_DIM, :].T
        p = out[:, 384:512].astype(BF16)
        pool[pl.ds(pl.multiple_of(TAIL + n * ptile, TAIL), ptile), :] = p.astype(F32)

        @pl.when(m == 0)
        def _():
            tail[...] = p[ptile - TAIL :, :]

            @pl.when(tail_out)
            def _():
                tail_copy.start()

        @pl.loop(q + 1, Q)
        def _(e):
            kv_copy(e, n).start()

        @pl.when(c == 0)
        def _():
            kv_pass(q, n).start()

        qq = rope(out[:, 0:128], cosine, sine).astype(BF16) * jnp.array(HEAD_DIM**-0.5, BF16)
        lane = lax.broadcasted_iota(jnp.int32, qq.shape, 1)
        zero = jnp.zeros_like(qq)
        q_st[0, :, at] = jnp.where(lane < HEAD_DIM, qq, zero).T
        q_st[1, :, at] = jnp.where(lane >= HEAD_DIM, qq, zero).T

    qtile = rows // 2

    def attend(k, piece, diagonal):
        begin, size = (0, rows) if piece is None else (piece * ptile, ptile)
        keys = pl.ds(begin, size)

        @pl.loop(0, rows // qtile)
        def _(n):
            at = pl.ds(pl.multiple_of(n * qtile, qtile), qtile)
            values = jnp.concatenate(
                [
                    kv[k, pl.ds(begin + i * VALUE_DIM, VALUE_DIM), 128:256]
                    for i in range(size // VALUE_DIM)
                ],
                axis=1,
            )
            for m_index in range(2):
                scores = jnp.dot(
                    kv[k, keys, 0:128], q_st[m_index, :, at], preferred_element_type=F32
                )
                if diagonal:
                    kpos = lax.broadcasted_iota(jnp.int32, scores.shape, 0)
                    qpos = n * qtile + lax.broadcasted_iota(jnp.int32, scores.shape, 1)
                    scores = jnp.where(kpos <= qpos, scores, MASKED)
                top = jnp.max(scores, axis=0, keepdims=True)
                if not diagonal:
                    old = m_st[m_index, :, at]
                    top = jnp.maximum(old, top)
                    factor = jnp.exp(old - top)
                weights = jnp.exp(scores - top)
                total = jnp.sum(weights, axis=0, keepdims=True)
                product = jnp.dot(values, weights.astype(BF16), preferred_element_type=F32)
                if not diagonal:
                    total = total + l_st[m_index, :, at] * factor
                    product = product + acc_st[m_index, :, at] * factor
                m_st[m_index, :, at] = top
                l_st[m_index, :, at] = total
                acc_st[m_index, :, at] = product

    attend(plane, None, True)
    o_start(0, False)
    o_cross().wait_recv()
    o_start(1, False)
    o_own(1)

    @pl.when(tail_in)
    def _():
        tail_copy.wait_recv()
        pool[0:TAIL, :] = prior[...].astype(F32)

    @pl.when(jnp.logical_not(tail_in))
    def _():
        pool[0:TAIL, :] = jnp.zeros((TAIL, GROUP_DIM), F32)

    def cat_copy(i):
        return rdma(cat.at[b, i], cat.at[b, i], cat_send.at[i], cat_recv.at[i], zdev)

    def hand_on(i, value):
        cat[b, i] = value
        cat_copy(i).start()

    ext = pool[...]
    kind = head % 4
    window = jnp.where(kind == 0, 2, jnp.where(kind == 1, 4, jnp.where(kind == 2, 8, 16)))
    run = ext + pltpu.roll(ext, 1, 0)
    chosen = run
    for power, lag in ((1, 2), (2, 4), (3, 8)):
        run = run + pltpu.roll(run, lag, 0)
        chosen = jnp.where(kind == power, run, chosen)
    spot = plane * rows + lax.broadcasted_iota(jnp.int32, (rows, GROUP_DIM), 0)
    counts = jnp.minimum(spot + 1, window).astype(F32)
    mean = chosen[TAIL:, :] / counts - ext[TAIL:, :]
    mixedg = jnp.dot(mean.astype(BF16), gw_ref[head], preferred_element_type=F32)
    hand_on(1, (mixedg * ps_ref[head]).astype(BF16))

    @pl.when(c == 1)
    def _():
        for n in range(G):
            kv_wait(2 * q, n)
        attend(2 * q, None, False)


    @pl.loop(0, q)
    def _(j):
        e = q - 1 - j
        for n in reversed(range(G)):
            kv_wait(2 * e + c, n)
            kv_pass(e, n).start()
            attend(2 * e + c, n, False)
            kv_wait(2 * e + 1 - c, n)
            attend(2 * e + 1 - c, n, False)

    diff = acc_st[0] / l_st[0] - lam_ref[head] * (acc_st[1] / l_st[1])
    inv = lax.rsqrt(jnp.mean(diff * diff, axis=0, keepdims=True) + HEAD_FLOOR)
    hand_on(0, ((diff * inv).T * hg_ref[...] * HEAD_SCALE).astype(BF16))

    share = rows // members
    half = part.shape[2]
    start_at = place_of(r, 0) // half
    near = CHUNKS // Q

    def chunk_at(h):
        return (start_at + h) % CHUNKS

    def head_product(h, bb):
        both = jnp.concatenate([cat[bb, 0], cat[bb, 1]], axis=1)
        rows_at = pl.ds(pl.multiple_of(chunk_at(h) * half, half), half)
        return lax.dot_general(
            both, o_all[bb, rows_at, :], (((1,), (1,)), ((), ())), preferred_element_type=F32
        )

    for gg in range(G):
        pl.when(half_of(r) == b)(functools.partial(o_wait, 1 - c, r, gg))

    def own_product(h):
        part[h] = head_product(h, b)

    for h in range(near):
        own_product(h)
    for i in range(2):
        cat_copy(i).wait_recv()

    @pl.when(b == 0)
    def _():
        o_start(0, True)

    o_start(1, True)
    orders = ([x_dim, y_dim], [y_dim, x_dim])

    def block(mask):
        gg, tt = member(mask)
        return pl.ds(pl.multiple_of((gg * 2 + tt // 2) * share, share), share)

    def combos(dims):
        found = [[]]
        for dim in dims:
            found = found + [mask + [dim] for mask in found]
        return found

    plans = []
    for h in range(CHUNKS):
        order = orders[h % 2]
        stages = []
        base = 0
        for i, dim in enumerate(order):
            masks = combos(order[i + 1 :])
            stages.append((dim, masks, base))
            base += len(masks)
        plans.append(stages)

    def rs_copy(h, dim, mask, index):
        at = block([dim] + mask)
        return rdma(
            sbuf.at[h, at, :], rbuf.at[h, index], rs_send.at[h, index], rs_recv.at[h, index],
            device([dim]),
        )

    def rs_start(h, i):
        dim, masks, base = plans[h][i]
        for n, mask in enumerate(masks):
            at = block([dim] + mask)
            sbuf[h, at, :] = part[h, at, :].astype(BF16)
        for n, mask in enumerate(masks):
            rs_copy(h, dim, mask, base + n).start()

    def rs_finish(h, i):
        dim, masks, base = plans[h][i]
        for n, mask in enumerate(masks):
            rs_copy(h, dim, mask, base + n).wait_recv()
            at = block(mask)
            part[h, at, :] = part[h, at, :] + rbuf[h, base + n].astype(F32)

    def out_product(h, begun):
        product = head_product(h, 1 - b)
        part[h] = (part[h] if begun else head_product(h, b)) + product

    mine = block([])
    lines = share // 2

    def fin_copy(h, core):
        where = dev(q, c, g, y, core)
        at = pl.ds(pl.multiple_of(core * lines, lines), lines)
        return rdma(
            fin.at[h, at, :], land.at[b, h], fin_send.at[h, core], fin_recv.at[b, h], where
        )

    def columns(hb, h):
        start = chunk_at(h) * half
        return pl.ds(pl.multiple_of((2 * (start // span) + hb) * span + start % span, half), half)

    def put(hb, h):
        at = columns(hb, h)
        return pltpu.make_async_copy(outb.at[:, at], out_ref.at[:, at], out_sem.at[hb, h])

    for h in range(near):
        out_product(h, True)
        rs_start(h, 0)
    o_relay(g)
    o_relay(1 - g)

    @pl.loop(0, R)
    def _(p):
        @pl.when(jnp.logical_and(p != r, half_of(p) == b))
        def _():
            for gg in range(G):
                o_wait(1 - c, p, gg)

    for h in range(near, CHUNKS):
        out_product(h, False)
        rs_start(h, 0)
    for h in range(CHUNKS):
        rs_finish(h, 0)
        rs_start(h, 1)
    for h in range(CHUNKS):
        rs_finish(h, 1)
        fin[h] = part[h, mine, :].astype(BF16)

        @pl.when(first)
        def _():
            fin_copy(h, 1 - c).start()
            outb[:, columns(b, h)] = fin[h, pl.ds(pl.multiple_of(c * lines, lines), lines), :]
            put(b, h).start()

        @pl.when(second)
        def _():
            fin_copy(h, 0).start()
            fin_copy(h, 1).start()


    def take(hb, h):
        rdma(
            land.at[hb, h], land.at[hb, h], fin_send.at[h, 0], fin_recv.at[hb, h], cdev
        ).wait_recv()
        outb[:, columns(hb, h)] = land[hb, h]
        put(hb, h).start()

    for h in range(CHUNKS):
        @pl.when(second)
        def _():
            take(b, h)

        take(1 - b, h)

    w_cross().wait_send()
    for kind in range(2):
        w_targets(lambda e: w_copy(kind, e).wait_send())

    @pl.when(first)
    def _():
        @pl.loop(0, S)
        def _(k):
            w_pass(k).wait_send()

    for n in range(2):
        for i in range(3):
            tok_first(i, n).wait_send()

        @pl.when(second)
        def _():
            tok_first(3, n).wait_send()
            for k in range(2):
                z_pass(k, 1, n).wait_send()
                z_pass(k, 0, n).wait_send()
                (x_pass if XY_PARTNER[k] else y_pass)(k, n).wait_send()

        @pl.when(first)
        def _():
            for k in range(2):
                (x_pass if XY_HOME[k] else y_pass)(k, n).wait_send()

    o_cross().wait_send()
    for kind in range(2):
        o_targets(lambda e: o_copy(kind, e).wait_send())
        cat_copy(kind).wait_send()

    @pl.loop(0, R)
    def _(p):
        @pl.when(half_of(p) == b)
        def _():
            for gg in range(G):
                o_pass(p, gg).wait_send()

    @pl.when(tail_out)
    def _():
        tail_copy.wait_send()

    for n in range(G):
        @pl.loop(q + 1, Q)
        def _(e):
            kv_copy(e, n).wait_send()

        @pl.loop(0, q + 1 - c)
        def _(e):
            kv_pass(e, n).wait_send()

    for h in range(CHUNKS):
        for dim, masks, base in plans[h]:
            for n, mask in enumerate(masks):
                rs_copy(h, dim, mask, base + n).wait_send()

        @pl.when(first)
        def _():
            fin_copy(h, 1 - c).wait_send()

        @pl.when(second)
        def _():
            fin_copy(h, 0).wait_send()
            fin_copy(h, 1).wait_send()
    for h in range(CHUNKS):
        for hb in range(2):
            put(hb, h).wait()


def body(
    sp,
    tp,
    tokens,
    norm_gain,
    query_one,
    key_one,
    query_two,
    key_two,
    value_weight,
    pool_weight,
    lambda_head,
    head_gain,
    group_weight,
    pool_scale,
    out_attn,
    out_pool,
):
    G = query_one.shape[1] // HEAD_DIM
    assert G == 2 and tp == 2 * G and sp % (2 * G) == 0
    R = sp // G
    Q = R // 2
    chunk, feats = tokens.shape
    rows = G * chunk
    depth = query_one.shape[0]
    cols = out_attn.shape[1]
    heads = lambda_head.shape[0]
    members = 2 * G
    share = rows // members

    half_dim = HEAD_DIM // 2
    inverse = ROPE_BASE ** (-((np.arange(2 * HEAD_DIM) % half_dim) * 2.0 / HEAD_DIM))
    freq = jnp.asarray(inverse.astype(np.float32).reshape(1, -1))
    width = 4 * HEAD_DIM + VALUE_DIM + GROUP_DIM
    depth_out = VALUE_DIM + GROUP_DIM
    total_cols = sp * cols
    vm = pl.BlockSpec(memory_space=pltpu.VMEM)
    dma = pltpu.SemaphoreType.DMA
    return pl.pallas_call(
        functools.partial(kernel, (G, Q, tp)),
        out_shape=jax.ShapeDtypeStruct((rows // (G * tp), total_cols), BF16),
        in_specs=[vm] * 11 + [pl.BlockSpec(memory_space=pltpu.SMEM)] + [vm] * 3,
        out_specs=pl.BlockSpec(memory_space=pl.ANY),
        scratch_shapes=[
            pltpu.VMEM((G, depth, width), BF16),
            pltpu.VMEM((G, cols, depth_out), BF16),
            pltpu.VMEM((cols, depth_out), BF16),
            pltpu.VMEM((rows, 2 * HEAD_DIM), F32),
            pltpu.VMEM((rows, 2 * HEAD_DIM), F32),
            pltpu.VMEM((rows, 1), F32),
            pltpu.VMEM((G, tp, chunk, feats), BF16),
            pltpu.VMEM((rows, tp * feats), BF16),
            pltpu.VMEM((sp + 1, depth, width), BF16),
            pltpu.VMEM((2, total_cols // 2, depth_out), BF16),
            pltpu.VMEM((R, rows, 256), BF16),
            pltpu.VMEM((2, 128, rows), BF16),
            pltpu.VMEM((2, 1, rows), F32),
            pltpu.VMEM((2, 1, rows), F32),
            pltpu.VMEM((2, VALUE_DIM, rows), F32),
            pltpu.VMEM((TAIL + rows, GROUP_DIM), F32),
            pltpu.VMEM((TAIL, GROUP_DIM), BF16),
            pltpu.VMEM((TAIL, GROUP_DIM), BF16),
            pltpu.VMEM((2, 2, rows, 128), BF16),
            pltpu.VMEM((CHUNKS, rows, total_cols // 2 // CHUNKS), F32),
            pltpu.VMEM((CHUNKS, rows, total_cols // 2 // CHUNKS), BF16),
            pltpu.VMEM((CHUNKS, members - 1, share, total_cols // 2 // CHUNKS), BF16),
            pltpu.VMEM((CHUNKS, share, total_cols // 2 // CHUNKS), BF16),
            pltpu.VMEM((2, CHUNKS, share // 2, total_cols // 2 // CHUNKS), BF16),
            pltpu.VMEM((rows // (G * tp), total_cols), BF16),
            dma((20,)),
            dma((2 * G * tp,)),
            dma((2 * Q,)),
            dma,
            dma((sp,)),
            dma((sp + 1,)),
            dma((2 * Q,)),
            dma((sp,)),
            dma((2 * sp,)),
            dma,
            dma,
            dma((2 * Q,)),
            dma((2 * Q,)),
            dma((2 * R,)),
            dma,
            dma,
            dma((2,)),
            dma((2,)),
            dma((CHUNKS, members - 1)),
            dma((CHUNKS, members - 1)),
            dma((CHUNKS, 2)),
            dma((2, CHUNKS)),
            dma((2, CHUNKS)),
        ],
        compiler_params=pltpu.CompilerParams(
            collective_id=0, has_side_effects=True, vmem_limit_bytes=58 * 1024 * 1024
        ),
    )(
        tokens,
        norm_gain.reshape(tp, 1, feats),
        query_one,
        key_one,
        query_two,
        key_two,
        value_weight,
        pool_weight,
        out_attn,
        out_pool,
        freq,
        lambda_head,
        head_gain.reshape(1, -1),
        group_weight,
        pool_scale.reshape(heads, 1, GROUP_DIM),
    )


def solution(mesh):
    in_specs = (
        P("sp", "tp"),
        P(),
        P("sp", "tp"),
        P("sp", "tp"),
        P("sp", "tp"),
        P("sp", "tp"),
        P("sp", "tp"),
        P("sp", "tp"),
        P(),
        P(),
        P(),
        P(),
        P("tp", "sp"),
        P("tp", "sp"),
    )
    return jax.shard_map(
        functools.partial(body, mesh.shape["sp"], mesh.shape["tp"]),
        mesh=mesh,
        in_specs=in_specs,
        out_specs=P(("sp", "tp"), None),
        check_vma=False,
    )
```

```python
import functools

import jax
import jax.numpy as jnp
import numpy as np
from jax import lax
from jax.experimental import pallas as pl
from jax.experimental.pallas import tpu as pltpu
from jax.sharding import PartitionSpec as P

HEAD_DIM = 64
VALUE_DIM = 128
GROUP_DIM = 128
ROPE_BASE = 500000.0
HEAD_SCALE = 0.8
NORM_FLOOR = 1e-06
HEAD_FLOOR = 0.001
MASKED = -1e30
TAIL = 16
CHUNKS = 8
XY_HOME = (True, False)
XY_PARTNER = (True, False)
MESH = pl.DeviceIdType.MESH
BF16 = jnp.bfloat16
F32 = jnp.float32


def flip(index, bit):
    return index + bit * (1 - 2 * ((index // bit) % 2))


def kernel(
    sizes,
    tok_ref,
    gain_ref,
    q1_ref,
    k1_ref,
    q2_ref,
    k2_ref,
    v_ref,
    p_ref,
    oa_ref,
    ob_ref,
    freq_ref,
    lam_ref,
    hg_ref,
    gw_ref,
    ps_ref,
    out_ref,
    wp_ref,
    op_ref,
    ox_ref,
    cos_ref,
    sin_ref,
    ssq,
    tokbuf,
    nrm,
    w_all,
    o_all,
    kv,
    q_st,
    m_st,
    l_st,
    acc_st,
    pool,
    tail,
    prior,
    cat,
    part,
    sbuf,
    rbuf,
    fin,
    land,
    outb,
    tok_send,
    tok_recv,
    w_send,
    wx_send,
    wd_send,
    w_recv,
    o_send,
    od_send,
    o_recv,
    ox_send,
    ox_recv,
    kv_send,
    kvd_send,
    kv_recv,
    pp_send,
    pp_recv,
    cat_send,
    cat_recv,
    rs_send,
    rs_recv,
    fin_send,
    fin_recv,
    out_sem,
):
    G, Q, TP = sizes
    S = 2 * G * Q
    R = 2 * Q
    s = lax.axis_index("sp")
    t = lax.axis_index("tp")
    r = s // G
    g = s % G
    q = r // 2
    b = r % 2
    y = t // 2
    c = t % 2
    other = s + 1 - 2 * g
    plane = 2 * q + c
    head = (2 * y + b) * G + g
    first = c == b
    second = c != b
    chunk, feats = tok_ref.shape
    rows = G * chunk
    cols = op_ref.shape[1]
    span = G * R * cols // TP

    def half_of(p):
        return (p * G * cols // span) % 2

    def place_of(p, gg):
        start = p * G * cols
        return pl.multiple_of((start // span // 2) * span + start % span + gg * cols, cols)


    def dev(q_, b_, g_, y_, c_):
        return ((2 * q_ + b_) * G + g_, 2 * y_ + c_)

    xdev = dev(q, b, 1 - g, y, c)
    ydev = dev(q, b, g, 1 - y, c)
    cdev = dev(q, b, g, y, 1 - c)
    zdev = dev(q, 1 - b, g, y, c)

    x_dim = ("g", 1)
    y_dim = ("t", 2)
    members = 2 * G

    def member(mask):
        gg, tt = g, t
        for kind, bb in mask:
            if kind == "g":
                gg = flip(gg, bb)
            else:
                tt = flip(tt, bb)
        return gg, tt

    def device(mask):
        gg, tt = member(mask)
        return (r * G + gg, tt)

    barrier = pltpu.get_barrier_semaphore()

    def greet(where):
        pl.semaphore_signal(barrier, inc=1, device_id=where, device_id_type=MESH)

    greet(xdev)
    greet(ydev)
    greet(cdev)
    greet(zdev)

    @pl.when(first)
    def _():
        greet(dev(q, b, 1 - g, y, 1 - c))
        greet(dev(q, b, g, 1 - y, 1 - c))

        @pl.loop(0, R)
        def _(p):
            @pl.when(p != r)
            def _():
                greet((p * G + g, t))

    @pl.when(second)
    def _():
        greet(dev(q, 1 - b, g, y, 0))
        greet(dev(q, 1 - b, g, y, 1))

    @pl.loop(0, R)
    def _(p):
        @pl.when(jnp.logical_and(p != r, half_of(p) == b))
        def _():
            greet((p * G + g, t))

    @pl.loop(0, q)
    def _(e):
        greet(dev(e, b, g, y, c))

    @pl.when(jnp.logical_and(c == 0, q > 0))
    def _():
        greet(dev(q - 1, b, g, y, 1))

    def pack(gg):
        a, z = gg * HEAD_DIM, (gg + 1) * HEAD_DIM
        e, f = gg * VALUE_DIM, (gg + 1) * VALUE_DIM
        wp_ref[gg, :, 0:128] = jnp.concatenate([q1_ref[:, a:z], q2_ref[:, a:z]], axis=1)
        wp_ref[gg, :, 128:256] = jnp.concatenate([k1_ref[:, a:z], k2_ref[:, a:z]], axis=1)
        wp_ref[gg, :, 256:384] = v_ref[:, e:f]
        wp_ref[gg, :, 384:512] = p_ref[:, e:f]

    for gg in range(G):
        pack(gg)

    one = lambda flag: jnp.where(flag, 1, 0)
    count = 4 + 2 * one(second) + 1 + Q - one(first) + Q - one(half_of(r) == b)
    count = count + (Q - 1 - q) + one(jnp.logical_and(c == 1, q < Q - 1))
    pl.semaphore_wait(barrier, count)

    def rdma(src, dst, ss, rs, where):
        return pltpu.make_async_remote_copy(
            src_ref=src, dst_ref=dst, send_sem=ss, recv_sem=rs, device_id=where, device_id_type=MESH
        )

    cross_to = jnp.where(first, s, S)
    cross_at = jnp.where(first, other, S)

    def w_cross():
        return rdma(wp_ref.at[1 - g], w_all.at[cross_to], wx_send, w_recv.at[cross_to], xdev)

    def w_copy(kind, e):
        src = wp_ref.at[g] if kind == 0 else w_all.at[cross_at]
        slot = s if kind == 0 else other
        return rdma(
            src, w_all.at[slot], w_send.at[kind * Q + e], w_recv.at[slot], dev(e, c, g, y, c)
        )

    def w_targets(act):
        for n in range(Q):
            e = (q + 1 + n) % Q
            if n == Q - 1:
                pl.when(second)(functools.partial(act, e))
            else:
                act(e)

    def w_start(kind):
        w_targets(lambda e: w_copy(kind, e).start())

    def w_pass(slot):
        return rdma(w_all.at[slot], w_all.at[slot], wd_send.at[slot], w_recv.at[slot], cdev)

    def tok_copy(src, xx, tt, n, index, where):
        at = pl.ds(n * (chunk // 2), chunk // 2)
        return rdma(
            src.at[at, :], tokbuf.at[xx, tt, at, :], tok_send.at[2 * index + n],
            tok_recv.at[2 * (xx * TP + tt) + n], where,
        )

    def tok_first(index, n):
        where = (
            dev(q, 1 - b, g, y, b),
            dev(q, b, g, 1 - y, b),
            dev(q, b, 1 - g, y, b),
            dev(q, b, g, y, b),
        )[index]
        return tok_copy(tok_ref, g, t, n, index, where)

    def tok_wait(xx, tt, n):
        tok_copy(tokbuf.at[xx, tt], xx, tt, n, 0, cdev).wait_recv()

    def z_pass(k, over_y, n):
        tt = 2 * y + k
        return tok_copy(tokbuf.at[g, tt], g, tt, n, 4 + 2 * k + over_y, ydev if over_y else xdev)

    def x_pass(k, n):
        xx, tt = 1 - g, 2 * y + k
        return tok_copy(tokbuf.at[xx, tt], xx, tt, n, 8 + k, ydev)

    def y_pass(k, n):
        xx, tt = g, 2 * (1 - y) + k
        return tok_copy(tokbuf.at[xx, tt], xx, tt, n, 8 + k, xdev)

    w_cross().start()
    for index in range(2):
        for n in range(2):
            tok_first(index, n).start()

    @pl.when(second)
    def _():
        for n in range(2):
            tok_first(3, n).start()

    for n in range(2):
        tok_first(2, n).start()
    w_start(0)

    @pl.when(first)
    def _():
        w_all[s] = wp_ref[g]
        tokbuf[g, t] = tok_ref[...]
        rdma(wp_ref.at[g], w_all.at[s], wd_send.at[s], w_recv.at[s], cdev).start()

    for gg in range(G):
        e, f = gg * VALUE_DIM, (gg + 1) * VALUE_DIM
        op_ref[gg, :, 0:128] = oa_ref[e:f, :].T
        op_ref[gg, :, 128:256] = ob_ref[e:f, :].T

    def o_at(core, p, gg):
        return o_all.at[core, pl.ds(place_of(p, gg), cols), :]

    def o_copy(kind, e):
        src, gg = (op_ref.at[g], g) if kind == 0 else (ox_ref, 1 - g)
        return rdma(
            src, o_at(c, r, gg), o_send.at[kind * Q + e], o_recv.at[c * S + r * G + gg],
            dev(e, half_of(r), g, y, c),
        )

    def o_targets(act, up=None):
        for n in range(Q):
            e = (q + 1 + n) % Q
            flag = half_of(r) != b if n == Q - 1 else None
            if up is not None:
                ahead = (e > q) == up
                flag = ahead if flag is None else jnp.logical_and(flag, ahead)
            if flag is None:
                act(e)
            else:
                pl.when(flag)(functools.partial(act, e))

    def o_start(kind, up):
        o_targets(lambda e: o_copy(kind, e).start(), up)

    def o_pass(p, gg):
        at = o_at(c, p, gg)
        index = p * G + gg
        return rdma(at, at, od_send.at[index], o_recv.at[c * S + index], cdev)

    def o_wait(core, p, gg):
        at = o_at(core, p, gg)
        rdma(at, at, od_send.at[0], o_recv.at[core * S + p * G + gg], cdev).wait_recv()

    def o_own(kind):
        gg = g if kind == 0 else 1 - g

        @pl.when(half_of(r) == b)
        def _():
            o_all[c, pl.ds(place_of(r, gg), cols), :] = op_ref[g] if kind == 0 else ox_ref[...]
            rdma(
                op_ref.at[g] if kind == 0 else ox_ref, o_at(c, r, gg), od_send.at[r * G + gg],
                o_recv.at[c * S + r * G + gg], cdev,
            ).start()

    def o_cross():
        return rdma(op_ref.at[1 - g], ox_ref, ox_send, ox_recv, xdev)

    def o_relay(gg):
        @pl.loop(0, R)
        def _(p):
            @pl.when(jnp.logical_and(p != r, half_of(p) == b))
            def _():
                o_wait(c, p, gg)
                o_pass(p, gg).start()

    lane128 = lax.broadcasted_iota(jnp.int32, (chunk, 2 * HEAD_DIM), 1)
    sign = jnp.where(lane128 % HEAD_DIM < HEAD_DIM // 2, -1.0, 1.0)

    @pl.loop(0, G)
    def _(n):
        at = pl.ds(pl.multiple_of(n * chunk, chunk), chunk)
        spots = plane * rows + n * chunk + lax.broadcasted_iota(jnp.int32, (chunk, 2 * HEAD_DIM), 0)
        angles = spots.astype(F32) * freq_ref[...]
        cos_ref[at, :] = jnp.cos(angles)
        sin_ref[at, :] = jnp.sin(angles) * sign

    ssq[...] = jnp.zeros_like(ssq)

    def scale(xx, tt):
        at = pl.ds(pl.multiple_of(xx * chunk, chunk), chunk)
        x = tokbuf[xx, tt].astype(F32)
        ssq[at, :] = ssq[at, :] + jnp.sum(x * x, axis=-1, keepdims=True)
        nrm[at, pl.ds(pl.multiple_of(tt * feats, feats), feats)] = (x * gain_ref[tt]).astype(BF16)

    def w_wait(slot):
        w_pass(slot).wait_recv()

    def early_relays(n):
        @pl.when(second)
        def _():
            for k in range(2):
                tok_wait(g, 2 * y + k, n)
                z_pass(k, 1, n).start()
                z_pass(k, 0, n).start()

        @pl.when(first)
        def _():
            for k in range(2):
                tok_wait(g, 2 * (1 - y) + k, n)
                if not XY_HOME[k]:
                    y_pass(k, n).start()
            tok_wait(g, 2 * y + 1 - c, n)

    early_relays(0)
    early_relays(1)
    w_wait(cross_at)
    w_start(1)

    @pl.when(first)
    def _():
        w_pass(other).start()
        for n in range(2):
            for k in range(2):
                tok_wait(1 - g, 2 * y + k, n)
                if XY_HOME[k]:
                    x_pass(k, n).start()

    def w_relay(gg):
        @pl.loop(1, R)
        def _(d):
            @pl.when(r - d >= 0)
            def _():
                w_wait((r - d) * G + gg)
                w_pass((r - d) * G + gg).start()

            @pl.when(r + d < R)
            def _():
                w_wait((r + d) * G + gg)
                w_pass((r + d) * G + gg).start()

    scale(g, 2 * y)
    scale(g, 2 * y + 1)

    @pl.when(first)
    def _():
        w_relay(g)

    @pl.when(second)
    def _():
        for n in range(2):
            for k in range(2):
                tok_wait(g, 2 * (1 - y) + k, n)
                if not XY_PARTNER[k]:
                    y_pass(k, n).start()
        for n in range(2):
            for k in range(2):
                tok_wait(1 - g, 2 * y + k, n)
                if XY_PARTNER[k]:
                    x_pass(k, n).start()

    for k in range(2):
        scale(g, 2 * (1 - y) + k)
        scale(1 - g, 2 * y + k)

    @pl.when(first)
    def _():
        w_relay(1 - g)

    o_cross().start()
    o_own(0)
    for k in range(2):
        for n in range(2):
            tok_wait(1 - g, 2 * (1 - y) + k, n)
        scale(1 - g, 2 * (1 - y) + k)

    @pl.when(second)
    def _():
        @pl.loop(0, S)
        def _(k):
            w_wait(k)

    ptile = chunk

    def rope(x, cosine, sine):
        lane = lax.broadcasted_iota(jnp.int32, x.shape, 1)
        near = jnp.where(
            lane % HEAD_DIM < HEAD_DIM // 2,
            pltpu.roll(x, x.shape[1] - HEAD_DIM // 2, 1),
            pltpu.roll(x, HEAD_DIM // 2, 1),
        )
        return x * cosine + near * sine

    def kv_part(k, n):
        return kv.at[k, pl.ds(pl.multiple_of(n * ptile, ptile), ptile), :]

    def kv_copy(e, n):
        at = kv_part(plane, n)
        return rdma(at, at, kv_send.at[2 * e + n], kv_recv.at[2 * plane + n], dev(e, b, g, y, c))

    def kv_pass(e, n):
        k = 2 * e + c
        at = kv_part(k, n)
        return rdma(at, at, kvd_send.at[2 * e + n], kv_recv.at[2 * k + n], cdev)

    def kv_wait(k, n):
        at = kv_part(k, n)
        rdma(at, at, kvd_send.at[0], kv_recv.at[2 * k + n], cdev).wait_recv()

    tail_copy = rdma(tail, prior, pp_send, pp_recv, (s + 2 * G * c, t + 1 - 2 * c))
    tail_out = jnp.logical_or(c == 0, q < Q - 1)
    tail_in = jnp.logical_or(c == 1, q > 0)

    @pl.loop(0, G)
    def _(m):
        n = G - 1 - m
        at = pl.ds(pl.multiple_of(n * ptile, ptile), ptile)
        weights = w_all[0:S].reshape(TP * feats, wp_ref.shape[2])
        inv = lax.rsqrt(ssq[at, :] / (TP * feats) + NORM_FLOOR)
        out = jnp.dot(nrm[at, :], weights, preferred_element_type=F32) * inv
        cosine = cos_ref[at, :]
        sine = sin_ref[at, :]
        kv[plane, at, 0:128] = rope(out[:, 128:256], cosine, sine).astype(BF16)
        v = out[:, 256:384].astype(BF16)
        for i in range(ptile // VALUE_DIM):
            dst = pl.ds(pl.multiple_of(n * ptile + i * VALUE_DIM, VALUE_DIM), VALUE_DIM)
            kv[plane, dst, 128:256] = v[i * VALUE_DIM : (i + 1) * VALUE_DIM, :].T
        p = out[:, 384:512].astype(BF16)
        pool[pl.ds(pl.multiple_of(TAIL + n * ptile, TAIL), ptile), :] = p.astype(F32)

        @pl.when(m == 0)
        def _():
            tail[...] = p[ptile - TAIL :, :]

            @pl.when(tail_out)
            def _():
                tail_copy.start()

        @pl.loop(q + 1, Q)
        def _(e):
            kv_copy(e, n).start()

        @pl.when(c == 0)
        def _():
            kv_pass(q, n).start()

        qq = rope(out[:, 0:128], cosine, sine).astype(BF16) * jnp.array(HEAD_DIM**-0.5, BF16)
        lane = lax.broadcasted_iota(jnp.int32, qq.shape, 1)
        zero = jnp.zeros_like(qq)
        at_b = pl.ds(pl.multiple_of(rows + n * ptile, ptile), ptile)
        q_st[:, at] = jnp.where(lane < HEAD_DIM, qq, zero).T
        q_st[:, at_b] = jnp.where(lane >= HEAD_DIM, qq, zero).T

    def attend(k, piece, diagonal):
        begin, size = (0, rows) if piece is None else (piece * ptile, ptile)
        values = jnp.concatenate(
            [
                kv[k, pl.ds(begin + i * VALUE_DIM, VALUE_DIM), 128:256]
                for i in range(size // VALUE_DIM)
            ],
            axis=1,
        )
        scores = jnp.dot(kv[k, pl.ds(begin, size), 0:128], q_st[...], preferred_element_type=F32)
        if diagonal:
            kpos = lax.broadcasted_iota(jnp.int32, scores.shape, 0)
            qpos = lax.broadcasted_iota(jnp.int32, scores.shape, 1) % rows
            scores = jnp.where(kpos <= qpos, scores, MASKED)
        top = jnp.max(scores, axis=0, keepdims=True)
        if not diagonal:
            old = m_st[...]
            top = jnp.maximum(old, top)
            factor = jnp.exp(old - top)
        weights = jnp.exp(scores - top)
        total = jnp.sum(weights, axis=0, keepdims=True)
        product = jnp.dot(values, weights.astype(BF16), preferred_element_type=F32)
        if not diagonal:
            total = total + l_st[...] * factor
            product = product + acc_st[...] * factor
        m_st[...] = top
        l_st[...] = total
        acc_st[...] = product

    attend(plane, None, True)
    o_start(0, False)
    o_cross().wait_recv()
    o_start(1, False)
    o_own(1)

    @pl.when(tail_in)
    def _():
        tail_copy.wait_recv()
        pool[0:TAIL, :] = prior[...].astype(F32)

    @pl.when(jnp.logical_not(tail_in))
    def _():
        pool[0:TAIL, :] = jnp.zeros((TAIL, GROUP_DIM), F32)

    def cat_copy(i):
        return rdma(cat.at[b, i], cat.at[b, i], cat_send.at[i], cat_recv.at[i], zdev)

    def hand_on(i, value):
        cat[b, i] = value
        cat_copy(i).start()

    ext = pool[...]
    kind = head % 4
    window = jnp.where(kind == 0, 2, jnp.where(kind == 1, 4, jnp.where(kind == 2, 8, 16)))
    run = ext + pltpu.roll(ext, 1, 0)
    chosen = run
    for power, lag in ((1, 2), (2, 4), (3, 8)):
        run = run + pltpu.roll(run, lag, 0)
        chosen = jnp.where(kind == power, run, chosen)
    spot = plane * rows + lax.broadcasted_iota(jnp.int32, (rows, GROUP_DIM), 0)
    counts = jnp.minimum(spot + 1, window).astype(F32)
    mean = chosen[TAIL:, :] / counts - ext[TAIL:, :]
    mixedg = jnp.dot(mean.astype(BF16), gw_ref[head], preferred_element_type=F32)
    hand_on(1, (mixedg * ps_ref[head]).astype(BF16))

    @pl.when(c == 1)
    def _():
        for n in range(G):
            kv_wait(2 * q, n)
        attend(2 * q, None, False)


    @pl.loop(0, q)
    def _(j):
        e = q - 1 - j
        for n in reversed(range(G)):
            kv_wait(2 * e + c, n)
            kv_pass(e, n).start()
            attend(2 * e + c, n, False)
        for n in range(G):
            kv_wait(2 * e + 1 - c, n)
        attend(2 * e + 1 - c, None, False)

    means = acc_st[...] / l_st[...]
    diff = means[:, :rows] - lam_ref[head] * means[:, rows:]
    inv = lax.rsqrt(jnp.mean(diff * diff, axis=0, keepdims=True) + HEAD_FLOOR)
    hand_on(0, ((diff * inv).T * hg_ref[...] * HEAD_SCALE).astype(BF16))

    share = rows // members
    half = part.shape[2]
    start_at = place_of(r, 0) // half
    near = CHUNKS // Q

    def chunk_at(h):
        return (start_at + h) % CHUNKS

    def head_product(h, bb):
        both = jnp.concatenate([cat[bb, 0], cat[bb, 1]], axis=1)
        rows_at = pl.ds(pl.multiple_of(chunk_at(h) * half, half), half)
        return lax.dot_general(
            both, o_all[bb, rows_at, :], (((1,), (1,)), ((), ())), preferred_element_type=F32
        )

    for gg in range(G):
        pl.when(half_of(r) == b)(functools.partial(o_wait, 1 - c, r, gg))

    def own_product(h):
        part[h] = head_product(h, b)

    for h in range(near):
        own_product(h)
    cat_copy(1).wait_recv()

    @pl.when(b == 1)
    def _():
        o_start(0, True)

    cat_copy(0).wait_recv()

    @pl.when(b == 0)
    def _():
        o_start(0, True)

    o_start(1, True)
    orders = ([x_dim, y_dim], [y_dim, x_dim])

    def block(mask):
        gg, tt = member(mask)
        return pl.ds(pl.multiple_of((gg * 2 + tt // 2) * share, share), share)

    def combos(dims):
        found = [[]]
        for dim in dims:
            found = found + [mask + [dim] for mask in found]
        return found

    plans = []
    for h in range(CHUNKS):
        order = orders[h % 2]
        stages = []
        base = 0
        for i, dim in enumerate(order):
            masks = combos(order[i + 1 :])
            stages.append((dim, masks, base))
            base += len(masks)
        plans.append(stages)

    def rs_copy(h, dim, mask, index):
        at = block([dim] + mask)
        return rdma(
            sbuf.at[h, at, :], rbuf.at[h, index], rs_send.at[h, index], rs_recv.at[h, index],
            device([dim]),
        )

    def rs_start(h, i):
        dim, masks, base = plans[h][i]
        for n, mask in enumerate(masks):
            at = block([dim] + mask)
            sbuf[h, at, :] = part[h, at, :].astype(BF16)
        for n, mask in enumerate(masks):
            rs_copy(h, dim, mask, base + n).start()

    def rs_finish(h, i):
        dim, masks, base = plans[h][i]
        for n, mask in enumerate(masks):
            rs_copy(h, dim, mask, base + n).wait_recv()
            at = block(mask)
            part[h, at, :] = part[h, at, :] + rbuf[h, base + n].astype(F32)

    def out_product(h, begun):
        product = head_product(h, 1 - b)
        part[h] = (part[h] if begun else head_product(h, b)) + product

    mine = block([])
    lines = share // 2

    def fin_copy(h, core):
        where = dev(q, c, g, y, core)
        at = pl.ds(pl.multiple_of(core * lines, lines), lines)
        return rdma(
            fin.at[h, at, :], land.at[b, h], fin_send.at[h, core], fin_recv.at[b, h], where
        )

    def columns(hb, h):
        start = chunk_at(h) * half
        return pl.ds(pl.multiple_of((2 * (start // span) + hb) * span + start % span, half), half)

    def put(hb, h):
        at = columns(hb, h)
        return pltpu.make_async_copy(outb.at[:, at], out_ref.at[:, at], out_sem.at[hb, h])

    for h in range(near):
        out_product(h, True)
        rs_start(h, 0)
    o_relay(g)
    o_relay(1 - g)

    @pl.loop(0, R)
    def _(p):
        @pl.when(jnp.logical_and(p != r, half_of(p) == b))
        def _():
            for gg in range(G):
                o_wait(1 - c, p, gg)

    for h in range(near, CHUNKS):
        out_product(h, False)
        rs_start(h, 0)
    for h in range(CHUNKS):
        rs_finish(h, 0)
        rs_start(h, 1)
    for h in range(CHUNKS):
        rs_finish(h, 1)
        fin[h] = part[h, mine, :].astype(BF16)

        @pl.when(first)
        def _():
            fin_copy(h, 1 - c).start()
            outb[:, columns(b, h)] = fin[h, pl.ds(pl.multiple_of(c * lines, lines), lines), :]
            put(b, h).start()

        @pl.when(second)
        def _():
            fin_copy(h, 0).start()
            fin_copy(h, 1).start()


    def take(hb, h):
        rdma(
            land.at[hb, h], land.at[hb, h], fin_send.at[h, 0], fin_recv.at[hb, h], cdev
        ).wait_recv()
        outb[:, columns(hb, h)] = land[hb, h]
        put(hb, h).start()

    for h in range(CHUNKS):
        @pl.when(second)
        def _():
            take(b, h)

        take(1 - b, h)

    w_cross().wait_send()
    for kind in range(2):
        w_targets(lambda e: w_copy(kind, e).wait_send())

    @pl.when(first)
    def _():
        @pl.loop(0, S)
        def _(k):
            w_pass(k).wait_send()

    for n in range(2):
        for i in range(3):
            tok_first(i, n).wait_send()

        @pl.when(second)
        def _():
            tok_first(3, n).wait_send()
            for k in range(2):
                z_pass(k, 1, n).wait_send()
                z_pass(k, 0, n).wait_send()
                (x_pass if XY_PARTNER[k] else y_pass)(k, n).wait_send()

        @pl.when(first)
        def _():
            for k in range(2):
                (x_pass if XY_HOME[k] else y_pass)(k, n).wait_send()

    o_cross().wait_send()
    for kind in range(2):
        o_targets(lambda e: o_copy(kind, e).wait_send())
        cat_copy(kind).wait_send()

    @pl.loop(0, R)
    def _(p):
        @pl.when(half_of(p) == b)
        def _():
            for gg in range(G):
                o_pass(p, gg).wait_send()

    @pl.when(tail_out)
    def _():
        tail_copy.wait_send()

    for n in range(G):
        @pl.loop(q + 1, Q)
        def _(e):
            kv_copy(e, n).wait_send()

        @pl.loop(0, q + 1 - c)
        def _(e):
            kv_pass(e, n).wait_send()

    for h in range(CHUNKS):
        for dim, masks, base in plans[h]:
            for n, mask in enumerate(masks):
                rs_copy(h, dim, mask, base + n).wait_send()

        @pl.when(first)
        def _():
            fin_copy(h, 1 - c).wait_send()

        @pl.when(second)
        def _():
            fin_copy(h, 0).wait_send()
            fin_copy(h, 1).wait_send()
    for h in range(CHUNKS):
        for hb in range(2):
            put(hb, h).wait()


def body(
    sp,
    tp,
    tokens,
    norm_gain,
    query_one,
    key_one,
    query_two,
    key_two,
    value_weight,
    pool_weight,
    lambda_head,
    head_gain,
    group_weight,
    pool_scale,
    out_attn,
    out_pool,
):
    G = query_one.shape[1] // HEAD_DIM
    assert G == 2 and tp == 2 * G and sp % (2 * G) == 0
    R = sp // G
    Q = R // 2
    chunk, feats = tokens.shape
    rows = G * chunk
    depth = query_one.shape[0]
    cols = out_attn.shape[1]
    heads = lambda_head.shape[0]
    members = 2 * G
    share = rows // members

    half_dim = HEAD_DIM // 2
    inverse = ROPE_BASE ** (-((np.arange(2 * HEAD_DIM) % half_dim) * 2.0 / HEAD_DIM))
    freq = jnp.asarray(inverse.astype(np.float32).reshape(1, -1))
    width = 4 * HEAD_DIM + VALUE_DIM + GROUP_DIM
    depth_out = VALUE_DIM + GROUP_DIM
    total_cols = sp * cols
    vm = pl.BlockSpec(memory_space=pltpu.VMEM)
    dma = pltpu.SemaphoreType.DMA
    return pl.pallas_call(
        functools.partial(kernel, (G, Q, tp)),
        out_shape=jax.ShapeDtypeStruct((rows // (G * tp), total_cols), BF16),
        in_specs=[vm] * 11 + [pl.BlockSpec(memory_space=pltpu.SMEM)] + [vm] * 3,
        out_specs=pl.BlockSpec(memory_space=pl.ANY),
        scratch_shapes=[
            pltpu.VMEM((G, depth, width), BF16),
            pltpu.VMEM((G, cols, depth_out), BF16),
            pltpu.VMEM((cols, depth_out), BF16),
            pltpu.VMEM((rows, 2 * HEAD_DIM), F32),
            pltpu.VMEM((rows, 2 * HEAD_DIM), F32),
            pltpu.VMEM((rows, 1), F32),
            pltpu.VMEM((G, tp, chunk, feats), BF16),
            pltpu.VMEM((rows, tp * feats), BF16),
            pltpu.VMEM((sp + 1, depth, width), BF16),
            pltpu.VMEM((2, total_cols // 2, depth_out), BF16),
            pltpu.VMEM((R, rows, 256), BF16),
            pltpu.VMEM((128, 2 * rows), BF16),
            pltpu.VMEM((1, 2 * rows), F32),
            pltpu.VMEM((1, 2 * rows), F32),
            pltpu.VMEM((VALUE_DIM, 2 * rows), F32),
            pltpu.VMEM((TAIL + rows, GROUP_DIM), F32),
            pltpu.VMEM((TAIL, GROUP_DIM), BF16),
            pltpu.VMEM((TAIL, GROUP_DIM), BF16),
            pltpu.VMEM((2, 2, rows, 128), BF16),
            pltpu.VMEM((CHUNKS, rows, total_cols // 2 // CHUNKS), F32),
            pltpu.VMEM((CHUNKS, rows, total_cols // 2 // CHUNKS), BF16),
            pltpu.VMEM((CHUNKS, members - 1, share, total_cols // 2 // CHUNKS), BF16),
            pltpu.VMEM((CHUNKS, share, total_cols // 2 // CHUNKS), BF16),
            pltpu.VMEM((2, CHUNKS, share // 2, total_cols // 2 // CHUNKS), BF16),
            pltpu.VMEM((rows // (G * tp), total_cols), BF16),
            dma((20,)),
            dma((2 * G * tp,)),
            dma((2 * Q,)),
            dma,
            dma((sp,)),
            dma((sp + 1,)),
            dma((2 * Q,)),
            dma((sp,)),
            dma((2 * sp,)),
            dma,
            dma,
            dma((2 * Q,)),
            dma((2 * Q,)),
            dma((2 * R,)),
            dma,
            dma,
            dma((2,)),
            dma((2,)),
            dma((CHUNKS, members - 1)),
            dma((CHUNKS, members - 1)),
            dma((CHUNKS, 2)),
            dma((2, CHUNKS)),
            dma((2, CHUNKS)),
        ],
        compiler_params=pltpu.CompilerParams(
            collective_id=0, has_side_effects=True, vmem_limit_bytes=58 * 1024 * 1024
        ),
    )(
        tokens,
        norm_gain.reshape(tp, 1, feats),
        query_one,
        key_one,
        query_two,
        key_two,
        value_weight,
        pool_weight,
        out_attn,
        out_pool,
        freq,
        lambda_head,
        head_gain.reshape(1, -1),
        group_weight,
        pool_scale.reshape(heads, 1, GROUP_DIM),
    )


def solution(mesh):
    in_specs = (
        P("sp", "tp"),
        P(),
        P("sp", "tp"),
        P("sp", "tp"),
        P("sp", "tp"),
        P("sp", "tp"),
        P("sp", "tp"),
        P("sp", "tp"),
        P(),
        P(),
        P(),
        P(),
        P("tp", "sp"),
        P("tp", "sp"),
    )
    return jax.shard_map(
        functools.partial(body, mesh.shape["sp"], mesh.shape["tp"]),
        mesh=mesh,
        in_specs=in_specs,
        out_specs=P(("sp", "tp"), None),
        check_vma=False,
    )
```

```python
import functools

import jax
import jax.numpy as jnp
import numpy as np
from jax import lax
from jax.experimental import pallas as pl
from jax.experimental.pallas import tpu as pltpu
from jax.sharding import PartitionSpec as P

HEAD_DIM = 64
VALUE_DIM = 128
GROUP_DIM = 128
ROPE_BASE = 500000.0
HEAD_SCALE = 0.8
NORM_FLOOR = 1e-06
HEAD_FLOOR = 0.001
MASKED = -1e30
TAIL = 16
CHUNKS = 8
XY_HOME = (True, False)
XY_PARTNER = (True, False)
MESH = pl.DeviceIdType.MESH
BF16 = jnp.bfloat16
F32 = jnp.float32


def flip(index, bit):
    return index + bit * (1 - 2 * ((index // bit) % 2))


def kernel(
    sizes,
    tok_in,
    gain_ref,
    q1_in,
    k1_in,
    q2_in,
    k2_in,
    v_in,
    p_in,
    oa_in,
    ob_in,
    freq_ref,
    lam_ref,
    hg_ref,
    gw_in,
    ps_ref,
    out_ref,
    tok_ref,
    q1_ref,
    k1_ref,
    q2_ref,
    k2_ref,
    v_ref,
    p_ref,
    oa_ref,
    ob_ref,
    gw_ref,
    wp_ref,
    op_ref,
    ox_ref,
    cos_ref,
    sin_ref,
    ssq,
    tokbuf,
    nrm,
    w_all,
    o_all,
    kv,
    q_st,
    m_st,
    l_st,
    acc_st,
    pool,
    tail,
    prior,
    cat,
    part,
    sbuf,
    rbuf,
    fin,
    land,
    outb,
    tok_send,
    tok_recv,
    w_send,
    wx_send,
    wd_send,
    w_recv,
    o_send,
    od_send,
    o_recv,
    ox_send,
    ox_recv,
    kv_send,
    kvd_send,
    kv_recv,
    pp_send,
    pp_recv,
    cat_send,
    cat_recv,
    rs_send,
    rs_recv,
    fin_send,
    fin_recv,
    out_sem,
    in_sem,
):
    G, Q, TP = sizes
    S = 2 * G * Q
    R = 2 * Q
    s = lax.axis_index("sp")
    t = lax.axis_index("tp")
    r = s // G
    g = s % G
    q = r // 2
    b = r % 2
    y = t // 2
    c = t % 2
    other = s + 1 - 2 * g
    plane = 2 * q + c
    head = (2 * y + b) * G + g
    first = c == b
    second = c != b
    chunk, feats = tok_in.shape
    rows = G * chunk
    cols = op_ref.shape[1]
    span = G * R * cols // TP

    def half_of(p):
        return (p * G * cols // span) % 2

    def place_of(p, gg):
        start = p * G * cols
        return pl.multiple_of((start // span // 2) * span + start % span + gg * cols, cols)


    def dev(q_, b_, g_, y_, c_):
        return ((2 * q_ + b_) * G + g_, 2 * y_ + c_)

    xdev = dev(q, b, 1 - g, y, c)
    ydev = dev(q, b, g, 1 - y, c)
    cdev = dev(q, b, g, y, 1 - c)
    zdev = dev(q, 1 - b, g, y, c)

    x_dim = ("g", 1)
    y_dim = ("t", 2)
    members = 2 * G

    def member(mask):
        gg, tt = g, t
        for kind, bb in mask:
            if kind == "g":
                gg = flip(gg, bb)
            else:
                tt = flip(tt, bb)
        return gg, tt

    def device(mask):
        gg, tt = member(mask)
        return (r * G + gg, tt)

    barrier = pltpu.get_barrier_semaphore()

    loads = [
        pltpu.make_async_copy(src, dst, in_sem.at[i])
        for i, (src, dst) in enumerate(
            (
                (k1_in, k1_ref), (k2_in, k2_ref), (v_in, v_ref), (p_in, p_ref), (q1_in, q1_ref),
                (q2_in, q2_ref), (tok_in, tok_ref), (oa_in, oa_ref), (ob_in, ob_ref),
                (gw_in.at[head], gw_ref),
            )
        )
    ]
    for load in loads:
        load.start()

    def greet(where):
        pl.semaphore_signal(barrier, inc=1, device_id=where, device_id_type=MESH)

    greet(xdev)
    greet(ydev)
    greet(cdev)
    greet(zdev)

    @pl.when(first)
    def _():
        greet(dev(q, b, 1 - g, y, 1 - c))
        greet(dev(q, b, g, 1 - y, 1 - c))

        @pl.loop(0, R)
        def _(p):
            @pl.when(p != r)
            def _():
                greet((p * G + g, t))

    @pl.when(second)
    def _():
        greet(dev(q, 1 - b, g, y, 0))
        greet(dev(q, 1 - b, g, y, 1))

    @pl.loop(0, R)
    def _(p):
        @pl.when(jnp.logical_and(p != r, half_of(p) == b))
        def _():
            greet((p * G + g, t))

    @pl.loop(0, q)
    def _(e):
        greet(dev(e, b, g, y, c))

    @pl.when(jnp.logical_and(c == 0, q > 0))
    def _():
        greet(dev(q - 1, b, g, y, 1))

    def pack(gg):
        a, z = gg * HEAD_DIM, (gg + 1) * HEAD_DIM
        e, f = gg * VALUE_DIM, (gg + 1) * VALUE_DIM
        wp_ref[gg, :, 0:128] = jnp.concatenate([k1_ref[:, a:z], k2_ref[:, a:z]], axis=1)
        wp_ref[gg, :, 128:256] = v_ref[:, e:f]
        wp_ref[gg, :, 256:384] = p_ref[:, e:f]
        wp_ref[gg, :, 384:512] = jnp.concatenate([q1_ref[:, a:z], q2_ref[:, a:z]], axis=1)

    for load in loads[:6]:
        load.wait()
    for gg in range(G):
        pack(gg)
    loads[6].wait()

    one = lambda flag: jnp.where(flag, 1, 0)
    count = 4 + 2 * one(second) + 1 + Q - one(first) + Q - one(half_of(r) == b)
    count = count + (Q - 1 - q) + one(jnp.logical_and(c == 1, q < Q - 1))
    pl.semaphore_wait(barrier, count)

    def rdma(src, dst, ss, rs, where):
        return pltpu.make_async_remote_copy(
            src_ref=src, dst_ref=dst, send_sem=ss, recv_sem=rs, device_id=where, device_id_type=MESH
        )

    cross_to = jnp.where(first, s, S)
    cross_at = jnp.where(first, other, S)

    early = 2 * HEAD_DIM + VALUE_DIM + GROUP_DIM
    shares = (pl.ds(0, early), pl.ds(early, 2 * HEAD_DIM))
    slots = S + 1

    def w_cross(part_):
        cut = shares[part_]
        return rdma(
            wp_ref.at[1 - g, :, cut], w_all.at[cross_to, :, cut], wx_send.at[part_],
            w_recv.at[part_ * slots + cross_to], xdev,
        )

    def w_copy(part_, kind, e):
        cut = shares[part_]
        src = wp_ref.at[g, :, cut] if kind == 0 else w_all.at[cross_at, :, cut]
        slot = s if kind == 0 else other
        return rdma(
            src, w_all.at[slot, :, cut], w_send.at[(2 * part_ + kind) * Q + e],
            w_recv.at[part_ * slots + slot], dev(e, c, g, y, c),
        )

    def w_targets(act):
        for n in range(Q):
            e = (q + 1 + n) % Q
            if n == Q - 1:
                pl.when(second)(functools.partial(act, e))
            else:
                act(e)

    def w_start(part_, kind):
        w_targets(lambda e: w_copy(part_, kind, e).start())

    def w_pass(part_, slot, src=None):
        at = w_all.at[slot, :, shares[part_]]
        return rdma(
            at if src is None else src, at, wd_send.at[part_ * S + slot],
            w_recv.at[part_ * slots + slot], cdev,
        )

    def tok_copy(src, xx, tt, n, index, where):
        at = pl.ds(n * (chunk // 2), chunk // 2)
        return rdma(
            src.at[at, :], tokbuf.at[xx, tt, at, :], tok_send.at[2 * index + n],
            tok_recv.at[2 * (xx * TP + tt) + n], where,
        )

    def tok_first(index, n):
        where = (
            dev(q, 1 - b, g, y, b),
            dev(q, b, g, 1 - y, b),
            dev(q, b, 1 - g, y, b),
            dev(q, b, g, y, b),
        )[index]
        return tok_copy(tok_ref, g, t, n, index, where)

    def tok_wait(xx, tt, n):
        tok_copy(tokbuf.at[xx, tt], xx, tt, n, 0, cdev).wait_recv()

    def z_pass(k, over_y, n):
        tt = 2 * y + k
        return tok_copy(tokbuf.at[g, tt], g, tt, n, 4 + 2 * k + over_y, ydev if over_y else xdev)

    def x_pass(k, n):
        xx, tt = 1 - g, 2 * y + k
        return tok_copy(tokbuf.at[xx, tt], xx, tt, n, 8 + k, ydev)

    def y_pass(k, n):
        xx, tt = g, 2 * (1 - y) + k
        return tok_copy(tokbuf.at[xx, tt], xx, tt, n, 8 + k, xdev)

    w_cross(0).start()
    for index in range(2):
        for n in range(2):
            tok_first(index, n).start()

    @pl.when(second)
    def _():
        for n in range(2):
            tok_first(3, n).start()

    tok_first(2, 0).start()
    w_cross(1).start()
    tok_first(2, 1).start()
    w_start(0, 0)

    @pl.when(first)
    def _():
        w_all[s] = wp_ref[g]
        tokbuf[g, t] = tok_ref[...]
        for i in range(2):
            w_pass(i, s, wp_ref.at[g, :, shares[i]]).start()

    for load in loads[7:]:
        load.wait()
    for gg in range(G):
        e, f = gg * VALUE_DIM, (gg + 1) * VALUE_DIM
        op_ref[gg, :, 0:128] = oa_ref[e:f, :].T
        op_ref[gg, :, 128:256] = ob_ref[e:f, :].T

    def o_at(core, p, gg):
        return o_all.at[core, pl.ds(place_of(p, gg), cols), :]

    def o_copy(kind, e):
        src, gg = (op_ref.at[g], g) if kind == 0 else (ox_ref, 1 - g)
        return rdma(
            src, o_at(c, r, gg), o_send.at[kind * Q + e], o_recv.at[c * S + r * G + gg],
            dev(e, half_of(r), g, y, c),
        )

    def o_targets(act, up=None):
        for n in range(Q):
            e = (q + 1 + n) % Q
            flag = half_of(r) != b if n == Q - 1 else None
            if up is not None:
                ahead = (e > q) == up
                flag = ahead if flag is None else jnp.logical_and(flag, ahead)
            if flag is None:
                act(e)
            else:
                pl.when(flag)(functools.partial(act, e))

    def o_start(kind, up):
        o_targets(lambda e: o_copy(kind, e).start(), up)

    def o_pass(p, gg):
        at = o_at(c, p, gg)
        index = p * G + gg
        return rdma(at, at, od_send.at[index], o_recv.at[c * S + index], cdev)

    def o_wait(core, p, gg):
        at = o_at(core, p, gg)
        rdma(at, at, od_send.at[0], o_recv.at[core * S + p * G + gg], cdev).wait_recv()

    def o_own(kind):
        gg = g if kind == 0 else 1 - g

        @pl.when(half_of(r) == b)
        def _():
            o_all[c, pl.ds(place_of(r, gg), cols), :] = op_ref[g] if kind == 0 else ox_ref[...]
            rdma(
                op_ref.at[g] if kind == 0 else ox_ref, o_at(c, r, gg), od_send.at[r * G + gg],
                o_recv.at[c * S + r * G + gg], cdev,
            ).start()

    def o_cross():
        return rdma(op_ref.at[1 - g], ox_ref, ox_send, ox_recv, xdev)

    def o_relay(gg):
        @pl.loop(0, R)
        def _(p):
            @pl.when(jnp.logical_and(p != r, half_of(p) == b))
            def _():
                o_wait(c, p, gg)
                o_pass(p, gg).start()

    lane128 = lax.broadcasted_iota(jnp.int32, (chunk, 2 * HEAD_DIM), 1)
    sign = jnp.where(lane128 % HEAD_DIM < HEAD_DIM // 2, -1.0, 1.0)

    @pl.loop(0, G)
    def _(n):
        at = pl.ds(pl.multiple_of(n * chunk, chunk), chunk)
        spots = plane * rows + n * chunk + lax.broadcasted_iota(jnp.int32, (chunk, 2 * HEAD_DIM), 0)
        angles = spots.astype(F32) * freq_ref[...]
        cos_ref[at, :] = jnp.cos(angles)
        sin_ref[at, :] = jnp.sin(angles) * sign

    ssq[...] = jnp.zeros_like(ssq)

    def scale(xx, tt):
        at = pl.ds(pl.multiple_of(xx * chunk, chunk), chunk)
        x = tokbuf[xx, tt].astype(F32)
        ssq[at, :] = ssq[at, :] + jnp.sum(x * x, axis=-1, keepdims=True)
        nrm[at, pl.ds(pl.multiple_of(tt * feats, feats), feats)] = (x * gain_ref[tt]).astype(BF16)

    def w_wait(part_, slot):
        at = w_all.at[slot, :, shares[part_]]
        rdma(at, at, wd_send.at[0], w_recv.at[part_ * slots + slot], cdev).wait_recv()

    def early_relays(n):
        @pl.when(second)
        def _():
            for k in range(2):
                tok_wait(g, 2 * y + k, n)
                z_pass(k, 1, n).start()
                z_pass(k, 0, n).start()

        @pl.when(first)
        def _():
            for k in range(2):
                tok_wait(g, 2 * (1 - y) + k, n)
            tok_wait(g, 2 * y + 1 - c, n)

    early_relays(0)
    early_relays(1)
    w_wait(0, cross_at)
    w_start(0, 1)
    w_start(1, 0)

    @pl.when(first)
    def _():
        w_pass(0, other).start()
        for n in range(2):
            for k in range(2):
                tok_wait(1 - g, 2 * y + k, n)
                if XY_HOME[k]:
                    x_pass(k, n).start()
            if n == 0:
                w_wait(1, cross_at)
                w_start(1, 1)

    def w_relay(part_, gg):
        @pl.loop(1, R)
        def _(d):
            @pl.when(r - d >= 0)
            def _():
                w_wait(part_, (r - d) * G + gg)
                w_pass(part_, (r - d) * G + gg).start()

            @pl.when(r + d < R)
            def _():
                w_wait(part_, (r + d) * G + gg)
                w_pass(part_, (r + d) * G + gg).start()

    scale(g, 2 * y)
    scale(g, 2 * y + 1)

    @pl.when(first)
    def _():
        w_relay(0, g)
        for n in range(2):
            for k in range(2):
                if not XY_HOME[k]:
                    y_pass(k, n).start()

    @pl.when(second)
    def _():
        for n in range(2):
            for k in range(2):
                tok_wait(g, 2 * (1 - y) + k, n)
                if not XY_PARTNER[k]:
                    y_pass(k, n).start()
        w_wait(1, cross_at)
        w_start(1, 1)
        for n in range(2):
            for k in range(2):
                tok_wait(1 - g, 2 * y + k, n)
                if XY_PARTNER[k]:
                    x_pass(k, n).start()

    for k in range(2):
        scale(g, 2 * (1 - y) + k)
        scale(1 - g, 2 * y + k)

    @pl.when(first)
    def _():
        w_relay(0, 1 - g)

    o_cross().start()
    o_own(0)

    for k in range(2):
        for n in range(2):
            tok_wait(1 - g, 2 * (1 - y) + k, n)
        scale(1 - g, 2 * (1 - y) + k)

    @pl.when(second)
    def _():
        @pl.loop(0, S)
        def _(k):
            w_wait(0, k)

    ptile = chunk

    def rope(x, cosine, sine):
        lane = lax.broadcasted_iota(jnp.int32, x.shape, 1)
        near = jnp.where(
            lane % HEAD_DIM < HEAD_DIM // 2,
            pltpu.roll(x, x.shape[1] - HEAD_DIM // 2, 1),
            pltpu.roll(x, HEAD_DIM // 2, 1),
        )
        return x * cosine + near * sine

    def kv_part(k, n):
        return kv.at[k, pl.ds(pl.multiple_of(n * ptile, ptile), ptile), :]

    def kv_copy(e, n):
        at = kv_part(plane, n)
        return rdma(at, at, kv_send.at[2 * e + n], kv_recv.at[2 * plane + n], dev(e, b, g, y, c))

    def kv_pass(e, n):
        k = 2 * e + c
        at = kv_part(k, n)
        return rdma(at, at, kvd_send.at[2 * e + n], kv_recv.at[2 * k + n], cdev)

    def kv_wait(k, n):
        at = kv_part(k, n)
        rdma(at, at, kvd_send.at[0], kv_recv.at[2 * k + n], cdev).wait_recv()

    tail_copy = rdma(tail, prior, pp_send, pp_recv, (s + 2 * G * c, t + 1 - 2 * c))
    tail_out = jnp.logical_or(c == 0, q < Q - 1)
    tail_in = jnp.logical_or(c == 1, q > 0)

    o_start(0, False)

    def project(at, part_):
        weights = w_all[0:S, :, shares[part_]].reshape(TP * feats, shares[part_].size)
        inv = lax.rsqrt(ssq[at, :] / (TP * feats) + NORM_FLOOR)
        return jnp.dot(nrm[at, :], weights, preferred_element_type=F32) * inv

    @pl.loop(0, G)
    def _(m):
        n = G - 1 - m
        at = pl.ds(pl.multiple_of(n * ptile, ptile), ptile)
        out = project(at, 0)
        kv[plane, at, 0:128] = rope(out[:, 0:128], cos_ref[at, :], sin_ref[at, :]).astype(BF16)
        v = out[:, 128:256].astype(BF16)
        for i in range(ptile // VALUE_DIM):
            dst = pl.ds(pl.multiple_of(n * ptile + i * VALUE_DIM, VALUE_DIM), VALUE_DIM)
            kv[plane, dst, 128:256] = v[i * VALUE_DIM : (i + 1) * VALUE_DIM, :].T
        p = out[:, 256:384].astype(BF16)
        pool[pl.ds(pl.multiple_of(TAIL + n * ptile, TAIL), ptile), :] = p.astype(F32)

        @pl.when(m == 0)
        def _():
            tail[...] = p[ptile - TAIL :, :]

            @pl.when(tail_out)
            def _():
                tail_copy.start()

        @pl.loop(q + 1, Q)
        def _(e):
            kv_copy(e, n).start()

        @pl.when(c == 0)
        def _():
            kv_pass(q, n).start()

    @pl.when(first)
    def _():
        w_pass(1, other).start()
        w_relay(1, g)
        w_relay(1, 1 - g)

    @pl.when(second)
    def _():
        @pl.loop(0, S)
        def _(k):
            w_wait(1, k)

    o_cross().wait_recv()
    o_start(1, False)
    o_own(1)

    @pl.loop(0, G)
    def _(n):
        at = pl.ds(pl.multiple_of(n * ptile, ptile), ptile)
        qq = rope(project(at, 1), cos_ref[at, :], sin_ref[at, :]).astype(BF16)
        qq = qq * jnp.array(HEAD_DIM**-0.5, BF16)
        lane = lax.broadcasted_iota(jnp.int32, qq.shape, 1)
        zero = jnp.zeros_like(qq)
        at_b = pl.ds(pl.multiple_of(rows + n * ptile, ptile), ptile)
        q_st[:, at] = jnp.where(lane < HEAD_DIM, qq, zero).T
        q_st[:, at_b] = jnp.where(lane >= HEAD_DIM, qq, zero).T

    def attend(k, piece, diagonal):
        begin, size = (0, rows) if piece is None else (piece * ptile, ptile)
        values = jnp.concatenate(
            [
                kv[k, pl.ds(begin + i * VALUE_DIM, VALUE_DIM), 128:256]
                for i in range(size // VALUE_DIM)
            ],
            axis=1,
        )
        scores = jnp.dot(kv[k, pl.ds(begin, size), 0:128], q_st[...], preferred_element_type=F32)
        if diagonal:
            kpos = lax.broadcasted_iota(jnp.int32, scores.shape, 0)
            qpos = lax.broadcasted_iota(jnp.int32, scores.shape, 1) % rows
            scores = jnp.where(kpos <= qpos, scores, MASKED)
        top = jnp.max(scores, axis=0, keepdims=True)
        if not diagonal:
            old = m_st[...]
            top = jnp.maximum(old, top)
            factor = jnp.exp(old - top)
        weights = jnp.exp(scores - top)
        total = jnp.sum(weights, axis=0, keepdims=True)
        product = jnp.dot(values, weights.astype(BF16), preferred_element_type=F32)
        if not diagonal:
            total = total + l_st[...] * factor
            product = product + acc_st[...] * factor
        m_st[...] = top
        l_st[...] = total
        acc_st[...] = product

    attend(plane, None, True)

    @pl.when(tail_in)
    def _():
        tail_copy.wait_recv()
        pool[0:TAIL, :] = prior[...].astype(F32)

    @pl.when(jnp.logical_not(tail_in))
    def _():
        pool[0:TAIL, :] = jnp.zeros((TAIL, GROUP_DIM), F32)

    def cat_copy(i):
        return rdma(cat.at[b, i], cat.at[b, i], cat_send.at[i], cat_recv.at[i], zdev)

    ext = pool[...]
    kind = head % 4
    window = jnp.where(kind == 0, 2, jnp.where(kind == 1, 4, jnp.where(kind == 2, 8, 16)))
    run = ext + pltpu.roll(ext, 1, 0)
    chosen = run
    for power, lag in ((1, 2), (2, 4), (3, 8)):
        run = run + pltpu.roll(run, lag, 0)
        chosen = jnp.where(kind == power, run, chosen)
    spot = plane * rows + lax.broadcasted_iota(jnp.int32, (rows, GROUP_DIM), 0)
    counts = jnp.minimum(spot + 1, window).astype(F32)
    mean = chosen[TAIL:, :] / counts - ext[TAIL:, :]
    mixedg = jnp.dot(mean.astype(BF16), gw_ref[...], preferred_element_type=F32)
    cat[b, 1] = (mixedg * ps_ref[head]).astype(BF16)
    cat_copy(1).start()

    @pl.when(c == 1)
    def _():
        for n in range(G):
            kv_wait(2 * q, n)
        attend(2 * q, None, False)


    @pl.loop(0, q)
    def _(j):
        e = q - 1 - j
        for n in reversed(range(G)):
            kv_wait(2 * e + c, n)
            kv_pass(e, n).start()
            attend(2 * e + c, n, False)
        for n in range(G):
            kv_wait(2 * e + 1 - c, n)
        attend(2 * e + 1 - c, None, False)

    means = acc_st[...] / l_st[...]
    diff = means[:, :rows] - lam_ref[head] * means[:, rows:]
    inv = lax.rsqrt(jnp.mean(diff * diff, axis=0, keepdims=True) + HEAD_FLOOR)
    cat[b, 0] = ((diff * inv).T * hg_ref[...] * HEAD_SCALE).astype(BF16)
    cat_copy(0).start()

    for n in range(G):
        @pl.loop(q + 1, Q)
        def _(e):
            kv_copy(e, n).wait_send()

    def o_up():
        @pl.when(g == 0)
        def _():
            o_start(0, True)
            o_start(1, True)

        @pl.when(g == 1)
        def _():
            o_start(1, True)
            o_start(0, True)

    o_up()
    share = rows // members
    half = part.shape[2]
    start_at = place_of(r, 0) // half
    near = CHUNKS // Q

    def chunk_at(h):
        return (start_at + h) % CHUNKS

    def head_product(h, bb):
        both = jnp.concatenate([cat[bb, 0], cat[bb, 1]], axis=1)
        rows_at = pl.ds(pl.multiple_of(chunk_at(h) * half, half), half)
        return lax.dot_general(
            both, o_all[bb, rows_at, :], (((1,), (1,)), ((), ())), preferred_element_type=F32
        )

    for gg in range(G):
        pl.when(half_of(r) == b)(functools.partial(o_wait, 1 - c, r, gg))

    def own_product(h):
        part[h] = head_product(h, b)

    for h in range(near):
        own_product(h)
    cat_copy(1).wait_recv()
    cat_copy(0).wait_recv()
    orders = ([x_dim, y_dim], [y_dim, x_dim])

    def block(mask):
        gg, tt = member(mask)
        return pl.ds(pl.multiple_of((gg * 2 + tt // 2) * share, share), share)

    def combos(dims):
        found = [[]]
        for dim in dims:
            found = found + [mask + [dim] for mask in found]
        return found

    plans = []
    for h in range(CHUNKS):
        order = orders[h % 2]
        stages = []
        base = 0
        for i, dim in enumerate(order):
            masks = combos(order[i + 1 :])
            stages.append((dim, masks, base))
            base += len(masks)
        plans.append(stages)

    def rs_copy(h, dim, mask, index):
        at = block([dim] + mask)
        return rdma(
            sbuf.at[h, at, :], rbuf.at[h, index], rs_send.at[h, index], rs_recv.at[h, index],
            device([dim]),
        )

    def rs_start(h, i):
        dim, masks, base = plans[h][i]
        for n, mask in enumerate(masks):
            at = block([dim] + mask)
            sbuf[h, at, :] = part[h, at, :].astype(BF16)
        for n, mask in enumerate(masks):
            rs_copy(h, dim, mask, base + n).start()

    def rs_finish(h, i):
        dim, masks, base = plans[h][i]
        for n, mask in enumerate(masks):
            rs_copy(h, dim, mask, base + n).wait_recv()
            at = block(mask)
            part[h, at, :] = part[h, at, :] + rbuf[h, base + n].astype(F32)

    def out_product(h):
        part[h] = head_product(h, b) + head_product(h, 1 - b)

    mine = block([])
    lines = share // 2

    def fin_copy(h, core):
        where = dev(q, c, g, y, core)
        at = pl.ds(pl.multiple_of(core * lines, lines), lines)
        return rdma(
            fin.at[h, at, :], land.at[b, h], fin_send.at[h, core], fin_recv.at[b, h], where
        )

    def columns(hb, h):
        start = chunk_at(h) * half
        return pl.ds(pl.multiple_of((2 * (start // span) + hb) * span + start % span, half), half)

    def put(hb, h):
        at = columns(hb, h)
        return pltpu.make_async_copy(outb.at[:, at], out_ref.at[:, at], out_sem.at[hb, h])

    for h in range(near):
        part[h] = part[h] + head_product(h, 1 - b)
        rs_start(h, 0)
    def far_weights(gg):
        o_relay(gg)

        @pl.loop(0, R)
        def _(p):
            @pl.when(jnp.logical_and(p != r, half_of(p) == b))
            def _():
                o_wait(1 - c, p, gg)

    in_turn = near > 0 and cols % half == 0
    for gg in range(G):
        far_weights(gg)
        if in_turn or gg == G - 1:
            for h in range(near, CHUNKS):
                if not in_turn or (h * half // cols) % G == gg:
                    out_product(h)
                    rs_start(h, 0)
    for h in range(CHUNKS):
        rs_finish(h, 0)
        rs_start(h, 1)
    for h in range(CHUNKS):
        rs_finish(h, 1)
        fin[h] = part[h, mine, :].astype(BF16)

        @pl.when(first)
        def _():
            fin_copy(h, 1 - c).start()
            outb[:, columns(b, h)] = fin[h, pl.ds(pl.multiple_of(c * lines, lines), lines), :]
            put(b, h).start()

        @pl.when(second)
        def _():
            fin_copy(h, 0).start()
            fin_copy(h, 1).start()


    def take(hb, h):
        rdma(
            land.at[hb, h], land.at[hb, h], fin_send.at[h, 0], fin_recv.at[hb, h], cdev
        ).wait_recv()
        outb[:, columns(hb, h)] = land[hb, h]
        put(hb, h).start()

    for h in range(CHUNKS):
        @pl.when(second)
        def _():
            take(b, h)

        take(1 - b, h)

    for i in range(2):
        w_cross(i).wait_send()
        for kind in range(2):
            w_targets(lambda e: w_copy(i, kind, e).wait_send())

    @pl.when(first)
    def _():
        @pl.loop(0, S)
        def _(k):
            w_pass(0, k).wait_send()
            w_pass(1, k).wait_send()

    for n in range(2):
        for i in range(3):
            tok_first(i, n).wait_send()

        @pl.when(second)
        def _():
            tok_first(3, n).wait_send()
            for k in range(2):
                z_pass(k, 1, n).wait_send()
                z_pass(k, 0, n).wait_send()
                (x_pass if XY_PARTNER[k] else y_pass)(k, n).wait_send()

        @pl.when(first)
        def _():
            for k in range(2):
                (x_pass if XY_HOME[k] else y_pass)(k, n).wait_send()

    o_cross().wait_send()
    for i in range(2):
        cat_copy(i).wait_send()
    for kind in range(2):
        o_targets(lambda e: o_copy(kind, e).wait_send())

    @pl.loop(0, R)
    def _(p):
        @pl.when(half_of(p) == b)
        def _():
            for gg in range(G):
                o_pass(p, gg).wait_send()

    @pl.when(tail_out)
    def _():
        tail_copy.wait_send()

    for n in range(G):
        @pl.loop(0, q + 1 - c)
        def _(e):
            kv_pass(e, n).wait_send()

    for h in range(CHUNKS):
        for dim, masks, base in plans[h]:
            for n, mask in enumerate(masks):
                rs_copy(h, dim, mask, base + n).wait_send()

        @pl.when(first)
        def _():
            fin_copy(h, 1 - c).wait_send()

        @pl.when(second)
        def _():
            fin_copy(h, 0).wait_send()
            fin_copy(h, 1).wait_send()
    for h in range(CHUNKS):
        for hb in range(2):
            put(hb, h).wait()


def body(
    sp,
    tp,
    tokens,
    norm_gain,
    query_one,
    key_one,
    query_two,
    key_two,
    value_weight,
    pool_weight,
    lambda_head,
    head_gain,
    group_weight,
    pool_scale,
    out_attn,
    out_pool,
):
    G = query_one.shape[1] // HEAD_DIM
    assert G == 2 and tp == 2 * G and sp % (2 * G) == 0
    R = sp // G
    Q = R // 2
    chunk, feats = tokens.shape
    rows = G * chunk
    depth = query_one.shape[0]
    cols = out_attn.shape[1]
    heads = lambda_head.shape[0]
    members = 2 * G
    share = rows // members

    half_dim = HEAD_DIM // 2
    inverse = ROPE_BASE ** (-((np.arange(2 * HEAD_DIM) % half_dim) * 2.0 / HEAD_DIM))
    freq = jnp.asarray(inverse.astype(np.float32).reshape(1, -1))
    width = 4 * HEAD_DIM + VALUE_DIM + GROUP_DIM
    depth_out = VALUE_DIM + GROUP_DIM
    total_cols = sp * cols
    vm = pl.BlockSpec(memory_space=pltpu.VMEM)
    far = pl.BlockSpec(memory_space=pl.ANY)
    dma = pltpu.SemaphoreType.DMA
    return pl.pallas_call(
        functools.partial(kernel, (G, Q, tp)),
        out_shape=jax.ShapeDtypeStruct((rows // (G * tp), total_cols), BF16),
        in_specs=[far, vm] + [far] * 8 + [vm, pl.BlockSpec(memory_space=pltpu.SMEM), vm, far, vm],
        out_specs=pl.BlockSpec(memory_space=pl.ANY),
        scratch_shapes=[
            pltpu.VMEM((chunk, feats), BF16),
            pltpu.VMEM((depth, G * HEAD_DIM), BF16),
            pltpu.VMEM((depth, G * HEAD_DIM), BF16),
            pltpu.VMEM((depth, G * HEAD_DIM), BF16),
            pltpu.VMEM((depth, G * HEAD_DIM), BF16),
            pltpu.VMEM((depth, G * VALUE_DIM), BF16),
            pltpu.VMEM((depth, G * GROUP_DIM), BF16),
            pltpu.VMEM((G * VALUE_DIM, cols), BF16),
            pltpu.VMEM((G * GROUP_DIM, cols), BF16),
            pltpu.VMEM((GROUP_DIM, GROUP_DIM), BF16),
            pltpu.VMEM((G, depth, width), BF16),
            pltpu.VMEM((G, cols, depth_out), BF16),
            pltpu.VMEM((cols, depth_out), BF16),
            pltpu.VMEM((rows, 2 * HEAD_DIM), F32),
            pltpu.VMEM((rows, 2 * HEAD_DIM), F32),
            pltpu.VMEM((rows, 1), F32),
            pltpu.VMEM((G, tp, chunk, feats), BF16),
            pltpu.VMEM((rows, tp * feats), BF16),
            pltpu.VMEM((sp + 1, depth, width), BF16),
            pltpu.VMEM((2, total_cols // 2, depth_out), BF16),
            pltpu.VMEM((R, rows, 256), BF16),
            pltpu.VMEM((128, 2 * rows), BF16),
            pltpu.VMEM((1, 2 * rows), F32),
            pltpu.VMEM((1, 2 * rows), F32),
            pltpu.VMEM((VALUE_DIM, 2 * rows), F32),
            pltpu.VMEM((TAIL + rows, GROUP_DIM), F32),
            pltpu.VMEM((TAIL, GROUP_DIM), BF16),
            pltpu.VMEM((TAIL, GROUP_DIM), BF16),
            pltpu.VMEM((2, 2, rows, 128), BF16),
            pltpu.VMEM((CHUNKS, rows, total_cols // 2 // CHUNKS), F32),
            pltpu.VMEM((CHUNKS, rows, total_cols // 2 // CHUNKS), BF16),
            pltpu.VMEM((CHUNKS, members - 1, share, total_cols // 2 // CHUNKS), BF16),
            pltpu.VMEM((CHUNKS, share, total_cols // 2 // CHUNKS), BF16),
            pltpu.VMEM((2, CHUNKS, share // 2, total_cols // 2 // CHUNKS), BF16),
            pltpu.VMEM((rows // (G * tp), total_cols), BF16),
            dma((20,)),
            dma((2 * G * tp,)),
            dma((4 * Q,)),
            dma((2,)),
            dma((2 * sp,)),
            dma((2 * (sp + 1),)),
            dma((2 * Q,)),
            dma((sp,)),
            dma((2 * sp,)),
            dma,
            dma,
            dma((2 * Q,)),
            dma((2 * Q,)),
            dma((2 * R,)),
            dma,
            dma,
            dma((2,)),
            dma((2,)),
            dma((CHUNKS, members - 1)),
            dma((CHUNKS, members - 1)),
            dma((CHUNKS, 2)),
            dma((2, CHUNKS)),
            dma((2, CHUNKS)),
            dma((10,)),
        ],
        compiler_params=pltpu.CompilerParams(
            collective_id=0, has_side_effects=True, vmem_limit_bytes=58 * 1024 * 1024
        ),
    )(
        tokens,
        norm_gain.reshape(tp, 1, feats),
        query_one,
        key_one,
        query_two,
        key_two,
        value_weight,
        pool_weight,
        out_attn,
        out_pool,
        freq,
        lambda_head,
        head_gain.reshape(1, -1),
        group_weight,
        pool_scale.reshape(heads, 1, GROUP_DIM),
    )


def solution(mesh):
    in_specs = (
        P("sp", "tp"),
        P(),
        P("sp", "tp"),
        P("sp", "tp"),
        P("sp", "tp"),
        P("sp", "tp"),
        P("sp", "tp"),
        P("sp", "tp"),
        P(),
        P(),
        P(),
        P(),
        P("tp", "sp"),
        P("tp", "sp"),
    )
    return jax.shard_map(
        functools.partial(body, mesh.shape["sp"], mesh.shape["tp"]),
        mesh=mesh,
        in_specs=in_specs,
        out_specs=P(("sp", "tp"), None),
        check_vma=False,
    )
```

```python
import functools

import jax
import jax.numpy as jnp
import numpy as np
from jax import lax
from jax.experimental import pallas as pl
from jax.experimental.pallas import tpu as pltpu
from jax.sharding import PartitionSpec as P

HEAD_DIM = 64
VALUE_DIM = 128
GROUP_DIM = 128
ROPE_BASE = 500000.0
HEAD_SCALE = 0.8
NORM_FLOOR = 1e-06
HEAD_FLOOR = 0.001
MASKED = -1e30
TAIL = 16
CHUNKS = 8
XY_HOME = (True, False)
XY_PARTNER = (True, False)
MESH = pl.DeviceIdType.MESH
BF16 = jnp.bfloat16
F32 = jnp.float32


def flip(index, bit):
    return index + bit * (1 - 2 * ((index // bit) % 2))


def kernel(
    sizes,
    tok_in,
    gain_ref,
    q1_in,
    k1_in,
    q2_in,
    k2_in,
    v_in,
    p_in,
    oa_in,
    ob_in,
    freq_ref,
    lam_ref,
    hg_ref,
    gw_in,
    ps_ref,
    out_ref,
    tok_ref,
    q1_ref,
    k1_ref,
    q2_ref,
    k2_ref,
    v_ref,
    p_ref,
    oa_ref,
    ob_ref,
    gw_ref,
    wp_ref,
    op_ref,
    ox_ref,
    cos_ref,
    sin_ref,
    ssq,
    tokbuf,
    nrm,
    w_all,
    o_all,
    kv,
    q_st,
    m_st,
    l_st,
    acc_st,
    pool,
    tail,
    prior,
    cat,
    part,
    sbuf,
    rbuf,
    fin,
    land,
    outb,
    tok_send,
    tok_recv,
    w_send,
    wx_send,
    wd_send,
    w_recv,
    o_send,
    od_send,
    o_recv,
    ox_send,
    ox_recv,
    kv_send,
    kvd_send,
    kv_recv,
    pp_send,
    pp_recv,
    cat_send,
    cat_recv,
    rs_send,
    rs_recv,
    fin_send,
    fin_recv,
    out_sem,
    in_sem,
):
    G, Q, TP = sizes
    S = 2 * G * Q
    R = 2 * Q
    s = lax.axis_index("sp")
    t = lax.axis_index("tp")
    r = s // G
    g = s % G
    q = r // 2
    b = r % 2
    y = t // 2
    c = t % 2
    other = s + 1 - 2 * g
    plane = 2 * q + c
    head = (2 * y + b) * G + g
    first = c == b
    second = c != b
    chunk, feats = tok_in.shape
    rows = G * chunk
    cols = op_ref.shape[1]
    span = G * R * cols // TP

    def half_of(p):
        return (p * G * cols // span) % 2

    def place_of(p, gg):
        start = p * G * cols
        return pl.multiple_of((start // span // 2) * span + start % span + gg * cols, cols)


    def dev(q_, b_, g_, y_, c_):
        return ((2 * q_ + b_) * G + g_, 2 * y_ + c_)

    xdev = dev(q, b, 1 - g, y, c)
    ydev = dev(q, b, g, 1 - y, c)
    cdev = dev(q, b, g, y, 1 - c)
    zdev = dev(q, 1 - b, g, y, c)

    x_dim = ("g", 1)
    y_dim = ("t", 2)
    members = 2 * G

    def member(mask):
        gg, tt = g, t
        for kind, bb in mask:
            if kind == "g":
                gg = flip(gg, bb)
            else:
                tt = flip(tt, bb)
        return gg, tt

    def device(mask):
        gg, tt = member(mask)
        return (r * G + gg, tt)

    barrier = pltpu.get_barrier_semaphore()

    loads = [
        pltpu.make_async_copy(src, dst, in_sem.at[i])
        for i, (src, dst) in enumerate(
            (
                (k1_in, k1_ref), (k2_in, k2_ref), (v_in, v_ref), (p_in, p_ref), (q1_in, q1_ref),
                (q2_in, q2_ref), (tok_in, tok_ref), (oa_in, oa_ref), (ob_in, ob_ref),
                (gw_in.at[head], gw_ref),
            )
        )
    ]
    for load in loads[:7]:
        load.start()

    def greet(where):
        pl.semaphore_signal(barrier, inc=1, device_id=where, device_id_type=MESH)

    greet(xdev)
    greet(ydev)
    greet(cdev)
    greet(zdev)
    greet(dev(q, 1 - b, 1 - g, y, b))
    greet(dev(q, 1 - b, g, 1 - y, b))

    @pl.when(first)
    def _():
        greet(dev(q, b, 1 - g, y, 1 - c))
        greet(dev(q, b, g, 1 - y, 1 - c))

        @pl.loop(0, R)
        def _(p):
            @pl.when(p != r)
            def _():
                greet((p * G + g, t))

    @pl.when(second)
    def _():
        greet(dev(q, 1 - b, g, y, 0))
        greet(dev(q, 1 - b, g, y, 1))

    @pl.loop(0, R)
    def _(p):
        @pl.when(jnp.logical_and(p != r, half_of(p) == b))
        def _():
            greet((p * G + g, t))

    @pl.loop(0, q)
    def _(e):
        greet(dev(e, b, g, y, c))

    @pl.when(jnp.logical_and(c == 0, q > 0))
    def _():
        greet(dev(q - 1, b, g, y, 1))

    def pack(gg):
        a, z = gg * HEAD_DIM, (gg + 1) * HEAD_DIM
        e, f = gg * VALUE_DIM, (gg + 1) * VALUE_DIM
        wp_ref[gg, :, 0:128] = jnp.concatenate([k1_ref[:, a:z], k2_ref[:, a:z]], axis=1)
        wp_ref[gg, :, 128:256] = v_ref[:, e:f]
        wp_ref[gg, :, 256:384] = p_ref[:, e:f]
        wp_ref[gg, :, 384:512] = jnp.concatenate([q1_ref[:, a:z], q2_ref[:, a:z]], axis=1)

    for load in loads[:6]:
        load.wait()
    for gg in range(G):
        pack(gg)
    loads[6].wait()
    for load in loads[7:]:
        load.start()

    one = lambda flag: jnp.where(flag, 1, 0)
    count = 4 + 6 * one(second) + 1 + Q - one(first) + Q - one(half_of(r) == b)
    count = count + (Q - 1 - q) + one(jnp.logical_and(c == 1, q < Q - 1))
    pl.semaphore_wait(barrier, count)

    def rdma(src, dst, ss, rs, where):
        return pltpu.make_async_remote_copy(
            src_ref=src, dst_ref=dst, send_sem=ss, recv_sem=rs, device_id=where, device_id_type=MESH
        )

    cross_to = jnp.where(first, s, S)
    cross_at = jnp.where(first, other, S)

    early = 2 * HEAD_DIM + VALUE_DIM + GROUP_DIM
    shares = (pl.ds(0, early), pl.ds(early, 2 * HEAD_DIM))
    slots = S + 1

    def w_cross(part_):
        cut = shares[part_]
        return rdma(
            wp_ref.at[1 - g, :, cut], w_all.at[cross_to, :, cut], wx_send.at[part_],
            w_recv.at[part_ * slots + cross_to], xdev,
        )

    def w_copy(part_, kind, e):
        cut = shares[part_]
        src = wp_ref.at[g, :, cut] if kind == 0 else w_all.at[cross_at, :, cut]
        slot = s if kind == 0 else other
        return rdma(
            src, w_all.at[slot, :, cut], w_send.at[(2 * part_ + kind) * Q + e],
            w_recv.at[part_ * slots + slot], dev(e, c, g, y, c),
        )

    def w_targets(act):
        for n in range(Q):
            e = (q + 1 + n) % Q
            if n == Q - 1:
                pl.when(second)(functools.partial(act, e))
            else:
                act(e)

    def w_start(part_, kind):
        w_targets(lambda e: w_copy(part_, kind, e).start())

    def w_pass(part_, slot, src=None):
        at = w_all.at[slot, :, shares[part_]]
        return rdma(
            at if src is None else src, at, wd_send.at[part_ * S + slot],
            w_recv.at[part_ * slots + slot], cdev,
        )

    def tok_copy(src, xx, tt, n, index, where):
        at = pl.ds(n * (chunk // 2), chunk // 2)
        return rdma(
            src.at[at, :], tokbuf.at[xx, tt, at, :], tok_send.at[2 * index + n],
            tok_recv.at[2 * (xx * TP + tt) + n], where,
        )

    def tok_first(index, n):
        where = (
            dev(q, 1 - b, g, y, b),
            dev(q, b, g, 1 - y, b),
            dev(q, b, 1 - g, y, b),
            dev(q, b, g, y, b),
        )[index]
        return tok_copy(tok_ref, g, t, n, index, where)

    def tok_wait(xx, tt, n):
        tok_copy(tokbuf.at[xx, tt], xx, tt, n, 0, cdev).wait_recv()

    def z_pass(k, over_y, n):
        tt = 2 * y + k
        return tok_copy(tokbuf.at[g, tt], g, tt, n, 4 + 2 * k + over_y, ydev if over_y else xdev)

    def x_pass(k, n):
        xx, tt = 1 - g, 2 * y + k
        return tok_copy(tokbuf.at[xx, tt], xx, tt, n, 8 + k, ydev)

    def y_pass(k, n):
        xx, tt = g, 2 * (1 - y) + k
        return tok_copy(tokbuf.at[xx, tt], xx, tt, n, 8 + k, xdev)

    w_cross(0).start()
    for index in range(2):
        for n in range(2):
            tok_first(index, n).start()

    @pl.when(second)
    def _():
        for n in range(2):
            tok_first(3, n).start()

    tok_first(2, 0).start()
    w_cross(1).start()
    tok_first(2, 1).start()
    w_start(0, 0)

    @pl.when(first)
    def _():
        w_all[s] = wp_ref[g]
        tokbuf[g, t] = tok_ref[...]
        for i in range(2):
            w_pass(i, s, wp_ref.at[g, :, shares[i]]).start()

    for load in loads[7:]:
        load.wait()
    for gg in range(G):
        e, f = gg * VALUE_DIM, (gg + 1) * VALUE_DIM
        op_ref[gg, :, 0:128] = oa_ref[e:f, :].T
        op_ref[gg, :, 128:256] = ob_ref[e:f, :].T

    def o_at(core, p, gg):
        return o_all.at[core, pl.ds(place_of(p, gg), cols), :]

    def o_copy(kind, e):
        src, gg = (op_ref.at[g], g) if kind == 0 else (ox_ref, 1 - g)
        return rdma(
            src, o_at(c, r, gg), o_send.at[kind * Q + e], o_recv.at[c * S + r * G + gg],
            dev(e, half_of(r), g, y, c),
        )

    def o_targets(act, up=None):
        for n in range(Q):
            e = (q + 1 + n) % Q
            flag = half_of(r) != b if n == Q - 1 else None
            if up is not None:
                ahead = (e > q) == up
                flag = ahead if flag is None else jnp.logical_and(flag, ahead)
            if flag is None:
                act(e)
            else:
                pl.when(flag)(functools.partial(act, e))

    def o_start(kind, up):
        o_targets(lambda e: o_copy(kind, e).start(), up)

    def o_pass(p, gg):
        at = o_at(c, p, gg)
        index = p * G + gg
        return rdma(at, at, od_send.at[index], o_recv.at[c * S + index], cdev)

    def o_wait(core, p, gg):
        at = o_at(core, p, gg)
        rdma(at, at, od_send.at[0], o_recv.at[core * S + p * G + gg], cdev).wait_recv()

    def o_own(kind):
        gg = g if kind == 0 else 1 - g

        @pl.when(half_of(r) == b)
        def _():
            o_all[c, pl.ds(place_of(r, gg), cols), :] = op_ref[g] if kind == 0 else ox_ref[...]
            rdma(
                op_ref.at[g] if kind == 0 else ox_ref, o_at(c, r, gg), od_send.at[r * G + gg],
                o_recv.at[c * S + r * G + gg], cdev,
            ).start()

    def o_cross():
        return rdma(op_ref.at[1 - g], ox_ref, ox_send, ox_recv, xdev)

    def o_relay(gg):
        @pl.loop(0, R)
        def _(p):
            @pl.when(jnp.logical_and(p != r, half_of(p) == b))
            def _():
                o_wait(c, p, gg)
                o_pass(p, gg).start()

    lane128 = lax.broadcasted_iota(jnp.int32, (chunk, 2 * HEAD_DIM), 1)
    sign = jnp.where(lane128 % HEAD_DIM < HEAD_DIM // 2, -1.0, 1.0)

    @pl.loop(0, G)
    def _(n):
        at = pl.ds(pl.multiple_of(n * chunk, chunk), chunk)
        spots = plane * rows + n * chunk + lax.broadcasted_iota(jnp.int32, (chunk, 2 * HEAD_DIM), 0)
        angles = spots.astype(F32) * freq_ref[...]
        cos_ref[at, :] = jnp.cos(angles)
        sin_ref[at, :] = jnp.sin(angles) * sign

    ssq[...] = jnp.zeros_like(ssq)

    def scale(xx, tt):
        at = pl.ds(pl.multiple_of(xx * chunk, chunk), chunk)
        x = tokbuf[xx, tt].astype(F32)
        ssq[at, :] = ssq[at, :] + jnp.sum(x * x, axis=-1, keepdims=True)
        nrm[at, pl.ds(pl.multiple_of(tt * feats, feats), feats)] = (x * gain_ref[tt]).astype(BF16)

    def w_wait(part_, slot):
        at = w_all.at[slot, :, shares[part_]]
        rdma(at, at, wd_send.at[0], w_recv.at[part_ * slots + slot], cdev).wait_recv()

    def early_relays(n):
        @pl.when(second)
        def _():
            for k in range(2):
                tok_wait(g, 2 * y + k, n)
                z_pass(k, 1, n).start()
                z_pass(k, 0, n).start()

        @pl.when(first)
        def _():
            for k in range(2):
                tok_wait(g, 2 * (1 - y) + k, n)
            tok_wait(g, 2 * y + 1 - c, n)

    early_relays(0)
    early_relays(1)
    w_wait(0, cross_at)
    w_start(0, 1)
    w_start(1, 0)

    @pl.when(first)
    def _():
        w_pass(0, other).start()
        for n in range(2):
            for k in range(2):
                tok_wait(1 - g, 2 * y + k, n)
                if XY_HOME[k]:
                    x_pass(k, n).start()
            if n == 0:
                w_wait(1, cross_at)
                w_start(1, 1)

    def w_relay(part_, gg):
        @pl.loop(1, R)
        def _(d):
            @pl.when(r - d >= 0)
            def _():
                w_wait(part_, (r - d) * G + gg)
                w_pass(part_, (r - d) * G + gg).start()

            @pl.when(r + d < R)
            def _():
                w_wait(part_, (r + d) * G + gg)
                w_pass(part_, (r + d) * G + gg).start()

    scale(g, 2 * y)
    scale(g, 2 * y + 1)

    @pl.when(first)
    def _():
        w_relay(0, g)
        for n in range(2):
            for k in range(2):
                if not XY_HOME[k]:
                    y_pass(k, n).start()

    @pl.when(second)
    def _():
        for n in range(2):
            for k in range(2):
                tok_wait(g, 2 * (1 - y) + k, n)
                if not XY_PARTNER[k]:
                    y_pass(k, n).start()
        w_wait(1, cross_at)
        w_start(1, 1)
        for n in range(2):
            for k in range(2):
                tok_wait(1 - g, 2 * y + k, n)
                if XY_PARTNER[k]:
                    x_pass(k, n).start()

    for k in range(2):
        scale(g, 2 * (1 - y) + k)
        scale(1 - g, 2 * y + k)

    @pl.when(first)
    def _():
        w_relay(0, 1 - g)

    o_cross().start()
    o_own(0)

    for k in range(2):
        for n in range(2):
            tok_wait(1 - g, 2 * (1 - y) + k, n)
        scale(1 - g, 2 * (1 - y) + k)

    @pl.when(second)
    def _():
        @pl.loop(0, S)
        def _(k):
            w_wait(0, k)

    ptile = chunk

    def rope(x, cosine, sine):
        lane = lax.broadcasted_iota(jnp.int32, x.shape, 1)
        near = jnp.where(
            lane % HEAD_DIM < HEAD_DIM // 2,
            pltpu.roll(x, x.shape[1] - HEAD_DIM // 2, 1),
            pltpu.roll(x, HEAD_DIM // 2, 1),
        )
        return x * cosine + near * sine

    def kv_part(k, n):
        return kv.at[k, pl.ds(pl.multiple_of(n * ptile, ptile), ptile), :]

    def kv_copy(e, n):
        at = kv_part(plane, n)
        return rdma(at, at, kv_send.at[2 * e + n], kv_recv.at[2 * plane + n], dev(e, b, g, y, c))

    def kv_pass(e, n):
        k = 2 * e + c
        at = kv_part(k, n)
        return rdma(at, at, kvd_send.at[2 * e + n], kv_recv.at[2 * k + n], cdev)

    def kv_wait(k, n):
        at = kv_part(k, n)
        rdma(at, at, kvd_send.at[0], kv_recv.at[2 * k + n], cdev).wait_recv()

    tail_copy = rdma(tail, prior, pp_send, pp_recv, (s + 2 * G * c, t + 1 - 2 * c))
    tail_out = jnp.logical_or(c == 0, q < Q - 1)
    tail_in = jnp.logical_or(c == 1, q > 0)

    o_start(0, False)

    def project(at, part_):
        weights = w_all[0:S, :, shares[part_]].reshape(TP * feats, shares[part_].size)
        inv = lax.rsqrt(ssq[at, :] / (TP * feats) + NORM_FLOOR)
        return jnp.dot(nrm[at, :], weights, preferred_element_type=F32) * inv

    @pl.loop(0, G)
    def _(m):
        n = G - 1 - m
        at = pl.ds(pl.multiple_of(n * ptile, ptile), ptile)
        out = project(at, 0)
        kv[plane, at, 0:128] = rope(out[:, 0:128], cos_ref[at, :], sin_ref[at, :]).astype(BF16)
        v = out[:, 128:256].astype(BF16)
        for i in range(ptile // VALUE_DIM):
            dst = pl.ds(pl.multiple_of(n * ptile + i * VALUE_DIM, VALUE_DIM), VALUE_DIM)
            kv[plane, dst, 128:256] = v[i * VALUE_DIM : (i + 1) * VALUE_DIM, :].T
        p = out[:, 256:384].astype(BF16)
        pool[pl.ds(pl.multiple_of(TAIL + n * ptile, TAIL), ptile), :] = p.astype(F32)

        @pl.when(m == 0)
        def _():
            tail[...] = p[ptile - TAIL :, :]

            @pl.when(tail_out)
            def _():
                tail_copy.start()

        @pl.loop(q + 1, Q)
        def _(e):
            kv_copy(e, n).start()

        @pl.when(c == 0)
        def _():
            kv_pass(q, n).start()

    @pl.when(first)
    def _():
        w_pass(1, other).start()
        w_relay(1, g)
        w_relay(1, 1 - g)

    @pl.when(second)
    def _():
        @pl.loop(0, S)
        def _(k):
            w_wait(1, k)

    o_cross().wait_recv()
    o_start(1, False)
    o_own(1)

    @pl.loop(0, G)
    def _(n):
        at = pl.ds(pl.multiple_of(n * ptile, ptile), ptile)
        qq = rope(project(at, 1), cos_ref[at, :], sin_ref[at, :]).astype(BF16)
        qq = qq * jnp.array(HEAD_DIM**-0.5, BF16)
        lane = lax.broadcasted_iota(jnp.int32, qq.shape, 1)
        zero = jnp.zeros_like(qq)
        at_b = pl.ds(pl.multiple_of(rows + n * ptile, ptile), ptile)
        q_st[:, at] = jnp.where(lane < HEAD_DIM, qq, zero).T
        q_st[:, at_b] = jnp.where(lane >= HEAD_DIM, qq, zero).T

    def attend(k, piece, diagonal):
        begin, size = (0, rows) if piece is None else (piece * ptile, ptile)
        values = jnp.concatenate(
            [
                kv[k, pl.ds(begin + i * VALUE_DIM, VALUE_DIM), 128:256]
                for i in range(size // VALUE_DIM)
            ],
            axis=1,
        )
        scores = jnp.dot(kv[k, pl.ds(begin, size), 0:128], q_st[...], preferred_element_type=F32)
        if diagonal:
            kpos = lax.broadcasted_iota(jnp.int32, scores.shape, 0)
            qpos = lax.broadcasted_iota(jnp.int32, scores.shape, 1) % rows
            scores = jnp.where(kpos <= qpos, scores, MASKED)
        top = jnp.max(scores, axis=0, keepdims=True)
        if not diagonal:
            old = m_st[...]
            top = jnp.maximum(old, top)
            factor = jnp.exp(old - top)
        weights = jnp.exp(scores - top)
        total = jnp.sum(weights, axis=0, keepdims=True)
        product = jnp.dot(values, weights.astype(BF16), preferred_element_type=F32)
        if not diagonal:
            total = total + l_st[...] * factor
            product = product + acc_st[...] * factor
        m_st[...] = top
        l_st[...] = total
        acc_st[...] = product

    attend(plane, None, True)

    @pl.when(tail_in)
    def _():
        tail_copy.wait_recv()
        pool[0:TAIL, :] = prior[...].astype(F32)

    @pl.when(jnp.logical_not(tail_in))
    def _():
        pool[0:TAIL, :] = jnp.zeros((TAIL, GROUP_DIM), F32)

    def cat_copy(i):
        return rdma(cat.at[b, i], cat.at[b, i], cat_send.at[i], cat_recv.at[i], zdev)

    ext = pool[...]
    kind = head % 4
    window = jnp.where(kind == 0, 2, jnp.where(kind == 1, 4, jnp.where(kind == 2, 8, 16)))
    run = ext + pltpu.roll(ext, 1, 0)
    chosen = run
    for power, lag in ((1, 2), (2, 4), (3, 8)):
        run = run + pltpu.roll(run, lag, 0)
        chosen = jnp.where(kind == power, run, chosen)
    spot = plane * rows + lax.broadcasted_iota(jnp.int32, (rows, GROUP_DIM), 0)
    counts = jnp.minimum(spot + 1, window).astype(F32)
    mean = chosen[TAIL:, :] / counts - ext[TAIL:, :]
    mixedg = jnp.dot(mean.astype(BF16), gw_ref[...], preferred_element_type=F32)
    cat[b, 1] = (mixedg * ps_ref[head]).astype(BF16)
    cat_copy(1).start()

    @pl.when(c == 1)
    def _():
        for n in range(G):
            kv_wait(2 * q, n)
        attend(2 * q, None, False)


    @pl.loop(0, q)
    def _(j):
        e = q - 1 - j
        for n in reversed(range(G)):
            kv_wait(2 * e + c, n)
            kv_pass(e, n).start()
            attend(2 * e + c, n, False)
        for n in range(G):
            kv_wait(2 * e + 1 - c, n)
        attend(2 * e + 1 - c, None, False)

    means = acc_st[...] / l_st[...]
    diff = means[:, :rows] - lam_ref[head] * means[:, rows:]
    inv = lax.rsqrt(jnp.mean(diff * diff, axis=0, keepdims=True) + HEAD_FLOOR)
    cat[b, 0] = ((diff * inv).T * hg_ref[...] * HEAD_SCALE).astype(BF16)
    cat_copy(0).start()

    for n in range(G):
        @pl.loop(q + 1, Q)
        def _(e):
            kv_copy(e, n).wait_send()

    def o_up():
        @pl.when(g == 0)
        def _():
            o_start(0, True)
            o_start(1, True)

        @pl.when(g == 1)
        def _():
            o_start(1, True)
            o_start(0, True)

    o_up()
    share = rows // members
    half = part.shape[2]
    start_at = place_of(r, 0) // half
    near = CHUNKS // Q

    def chunk_at(h):
        return (start_at + h) % CHUNKS

    def head_product(h, bb):
        both = jnp.concatenate([cat[bb, 0], cat[bb, 1]], axis=1)
        rows_at = pl.ds(pl.multiple_of(chunk_at(h) * half, half), half)
        return lax.dot_general(
            both, o_all[bb, rows_at, :], (((1,), (1,)), ((), ())), preferred_element_type=F32
        )

    for gg in range(G):
        pl.when(half_of(r) == b)(functools.partial(o_wait, 1 - c, r, gg))

    def own_product(h):
        part[h] = head_product(h, b)

    for h in range(near):
        own_product(h)
    cat_copy(1).wait_recv()
    cat_copy(0).wait_recv()
    orders = ([x_dim, y_dim], [y_dim, x_dim])

    def block(mask):
        gg, tt = member(mask)
        return pl.ds(pl.multiple_of((gg * 2 + tt // 2) * share, share), share)

    def combos(dims):
        found = [[]]
        for dim in dims:
            found = found + [mask + [dim] for mask in found]
        return found

    plans = []
    for h in range(CHUNKS):
        order = orders[h % 2]
        stages = []
        base = 0
        for i, dim in enumerate(order):
            masks = combos(order[i + 1 :])
            stages.append((dim, masks, base))
            base += len(masks)
        plans.append(stages)

    def rs_copy(h, dim, mask, index):
        at = block([dim] + mask)
        return rdma(
            sbuf.at[h, at, :], rbuf.at[h, index], rs_send.at[h, index], rs_recv.at[h, index],
            device([dim]),
        )

    def rs_start(h, i):
        dim, masks, base = plans[h][i]
        for n, mask in enumerate(masks):
            at = block([dim] + mask)
            sbuf[h, at, :] = part[h, at, :].astype(BF16)
        for n, mask in enumerate(masks):
            rs_copy(h, dim, mask, base + n).start()

    def rs_finish(h, i):
        dim, masks, base = plans[h][i]
        for n, mask in enumerate(masks):
            rs_copy(h, dim, mask, base + n).wait_recv()
            at = block(mask)
            part[h, at, :] = part[h, at, :] + rbuf[h, base + n].astype(F32)

    def out_product(h):
        part[h] = head_product(h, b) + head_product(h, 1 - b)

    mine = block([])
    lines = share // 2

    def pass_copy(h):
        at = pl.ds(pl.multiple_of((1 - c) * lines, lines), lines)
        return rdma(fin.at[h, at, :], land.at[0, h], fin_send.at[h, 0], fin_recv.at[0, h], cdev)

    def home_copies(h):
        dim = plans[h][1][0]
        found = []
        for n, mask in enumerate(([], [dim])):
            gg, tt = member(mask)
            for core in range(2):
                start = (gg * 2 + tt // 2) * share + core * lines
                at = pl.ds(pl.multiple_of(start, lines), lines)
                found.append(
                    rdma(
                        sbuf.at[h, at, :], land.at[1 + n, h], fin_send.at[h, 2 * n + core],
                        fin_recv.at[1 + n, h], dev(q, c, gg, tt // 2, core),
                    )
                )
        return found

    def home_start(h):
        dim = plans[h][1][0]
        for mask in ([], [dim]):
            sbuf[h, block(mask), :] = part[h, block(mask), :].astype(BF16)
        for copy in home_copies(h):
            copy.start()

    def columns(hb, h):
        start = chunk_at(h) * half
        return pl.ds(pl.multiple_of((2 * (start // span) + hb) * span + start % span, half), half)

    def put(hb, h):
        at = columns(hb, h)
        return pltpu.make_async_copy(outb.at[:, at], out_ref.at[:, at], out_sem.at[hb, h])

    for h in range(near):
        part[h] = part[h] + head_product(h, 1 - b)
        rs_start(h, 0)
    def far_weights(gg):
        o_relay(gg)

        @pl.loop(0, R)
        def _(p):
            @pl.when(jnp.logical_and(p != r, half_of(p) == b))
            def _():
                o_wait(1 - c, p, gg)

    in_turn = near > 0 and cols % half == 0
    for gg in range(G):
        far_weights(gg)
        if in_turn or gg == G - 1:
            for h in range(near, CHUNKS):
                if not in_turn or (h * half // cols) % G == gg:
                    out_product(h)
                    rs_start(h, 0)
    for h in range(CHUNKS):
        rs_finish(h, 0)
        pl.when(first)(functools.partial(rs_start, h, 1))
        pl.when(second)(functools.partial(home_start, h))
    def last_sum(h):
        rs_finish(h, 1)
        fin[h] = part[h, mine, :].astype(BF16)
        pass_copy(h).start()
        outb[:, columns(b, h)] = fin[h, pl.ds(pl.multiple_of(c * lines, lines), lines), :]
        put(b, h).start()

    @pl.when(first)
    def _():
        for h in range(CHUNKS):
            last_sum(h)


    def arrived(i, h):
        rdma(land.at[i, h], land.at[i, h], fin_send.at[h, 0], fin_recv.at[i, h], cdev).wait_recv()

    for h in range(CHUNKS):
        arrived(1, h)
        arrived(2, h)
        both = land[1, h].astype(F32) + land[2, h].astype(F32)
        outb[:, columns(1 - b, h)] = both.astype(BF16)
        put(1 - b, h).start()

    @pl.when(second)
    def _():
        for h in range(CHUNKS):
            arrived(0, h)
            outb[:, columns(b, h)] = land[0, h]
            put(b, h).start()

    for i in range(2):
        w_cross(i).wait_send()
        for kind in range(2):
            w_targets(lambda e: w_copy(i, kind, e).wait_send())

    @pl.when(first)
    def _():
        @pl.loop(0, S)
        def _(k):
            w_pass(0, k).wait_send()
            w_pass(1, k).wait_send()

    for n in range(2):
        for i in range(3):
            tok_first(i, n).wait_send()

        @pl.when(second)
        def _():
            tok_first(3, n).wait_send()
            for k in range(2):
                z_pass(k, 1, n).wait_send()
                z_pass(k, 0, n).wait_send()
                (x_pass if XY_PARTNER[k] else y_pass)(k, n).wait_send()

        @pl.when(first)
        def _():
            for k in range(2):
                (x_pass if XY_HOME[k] else y_pass)(k, n).wait_send()

    o_cross().wait_send()
    for i in range(2):
        cat_copy(i).wait_send()
    for kind in range(2):
        o_targets(lambda e: o_copy(kind, e).wait_send())

    @pl.loop(0, R)
    def _(p):
        @pl.when(half_of(p) == b)
        def _():
            for gg in range(G):
                o_pass(p, gg).wait_send()

    @pl.when(tail_out)
    def _():
        tail_copy.wait_send()

    for n in range(G):
        @pl.loop(0, q + 1 - c)
        def _(e):
            kv_pass(e, n).wait_send()

    for h in range(CHUNKS):
        for i, (dim, masks, base) in enumerate(plans[h]):
            for n, mask in enumerate(masks):
                copy = rs_copy(h, dim, mask, base + n)
                pl.when(first)(copy.wait_send) if i else copy.wait_send()

        @pl.when(first)
        def _():
            pass_copy(h).wait_send()

        @pl.when(second)
        def _():
            for copy in home_copies(h):
                copy.wait_send()
    for h in range(CHUNKS):
        for hb in range(2):
            put(hb, h).wait()


def body(
    sp,
    tp,
    tokens,
    norm_gain,
    query_one,
    key_one,
    query_two,
    key_two,
    value_weight,
    pool_weight,
    lambda_head,
    head_gain,
    group_weight,
    pool_scale,
    out_attn,
    out_pool,
):
    G = query_one.shape[1] // HEAD_DIM
    assert G == 2 and tp == 2 * G and sp % (2 * G) == 0
    R = sp // G
    Q = R // 2
    chunk, feats = tokens.shape
    rows = G * chunk
    depth = query_one.shape[0]
    cols = out_attn.shape[1]
    heads = lambda_head.shape[0]
    members = 2 * G
    share = rows // members

    half_dim = HEAD_DIM // 2
    inverse = ROPE_BASE ** (-((np.arange(2 * HEAD_DIM) % half_dim) * 2.0 / HEAD_DIM))
    freq = jnp.asarray(inverse.astype(np.float32).reshape(1, -1))
    width = 4 * HEAD_DIM + VALUE_DIM + GROUP_DIM
    depth_out = VALUE_DIM + GROUP_DIM
    total_cols = sp * cols
    vm = pl.BlockSpec(memory_space=pltpu.VMEM)
    far = pl.BlockSpec(memory_space=pl.ANY)
    dma = pltpu.SemaphoreType.DMA
    return pl.pallas_call(
        functools.partial(kernel, (G, Q, tp)),
        out_shape=jax.ShapeDtypeStruct((rows // (G * tp), total_cols), BF16),
        in_specs=[far, vm] + [far] * 8 + [vm, pl.BlockSpec(memory_space=pltpu.SMEM), vm, far, vm],
        out_specs=pl.BlockSpec(memory_space=pl.ANY),
        scratch_shapes=[
            pltpu.VMEM((chunk, feats), BF16),
            pltpu.VMEM((depth, G * HEAD_DIM), BF16),
            pltpu.VMEM((depth, G * HEAD_DIM), BF16),
            pltpu.VMEM((depth, G * HEAD_DIM), BF16),
            pltpu.VMEM((depth, G * HEAD_DIM), BF16),
            pltpu.VMEM((depth, G * VALUE_DIM), BF16),
            pltpu.VMEM((depth, G * GROUP_DIM), BF16),
            pltpu.VMEM((G * VALUE_DIM, cols), BF16),
            pltpu.VMEM((G * GROUP_DIM, cols), BF16),
            pltpu.VMEM((GROUP_DIM, GROUP_DIM), BF16),
            pltpu.VMEM((G, depth, width), BF16),
            pltpu.VMEM((G, cols, depth_out), BF16),
            pltpu.VMEM((cols, depth_out), BF16),
            pltpu.VMEM((rows, 2 * HEAD_DIM), F32),
            pltpu.VMEM((rows, 2 * HEAD_DIM), F32),
            pltpu.VMEM((rows, 1), F32),
            pltpu.VMEM((G, tp, chunk, feats), BF16),
            pltpu.VMEM((rows, tp * feats), BF16),
            pltpu.VMEM((sp + 1, depth, width), BF16),
            pltpu.VMEM((2, total_cols // 2, depth_out), BF16),
            pltpu.VMEM((R, rows, 256), BF16),
            pltpu.VMEM((128, 2 * rows), BF16),
            pltpu.VMEM((1, 2 * rows), F32),
            pltpu.VMEM((1, 2 * rows), F32),
            pltpu.VMEM((VALUE_DIM, 2 * rows), F32),
            pltpu.VMEM((TAIL + rows, GROUP_DIM), F32),
            pltpu.VMEM((TAIL, GROUP_DIM), BF16),
            pltpu.VMEM((TAIL, GROUP_DIM), BF16),
            pltpu.VMEM((2, 2, rows, 128), BF16),
            pltpu.VMEM((CHUNKS, rows, total_cols // 2 // CHUNKS), F32),
            pltpu.VMEM((CHUNKS, rows, total_cols // 2 // CHUNKS), BF16),
            pltpu.VMEM((CHUNKS, members - 1, share, total_cols // 2 // CHUNKS), BF16),
            pltpu.VMEM((CHUNKS, share, total_cols // 2 // CHUNKS), BF16),
            pltpu.VMEM((3, CHUNKS, share // 2, total_cols // 2 // CHUNKS), BF16),
            pltpu.VMEM((rows // (G * tp), total_cols), BF16),
            dma((20,)),
            dma((2 * G * tp,)),
            dma((4 * Q,)),
            dma((2,)),
            dma((2 * sp,)),
            dma((2 * (sp + 1),)),
            dma((2 * Q,)),
            dma((sp,)),
            dma((2 * sp,)),
            dma,
            dma,
            dma((2 * Q,)),
            dma((2 * Q,)),
            dma((2 * R,)),
            dma,
            dma,
            dma((2,)),
            dma((2,)),
            dma((CHUNKS, members - 1)),
            dma((CHUNKS, members - 1)),
            dma((CHUNKS, 4)),
            dma((3, CHUNKS)),
            dma((2, CHUNKS)),
            dma((10,)),
        ],
        compiler_params=pltpu.CompilerParams(
            collective_id=0, has_side_effects=True, vmem_limit_bytes=58 * 1024 * 1024
        ),
    )(
        tokens,
        norm_gain.reshape(tp, 1, feats),
        query_one,
        key_one,
        query_two,
        key_two,
        value_weight,
        pool_weight,
        out_attn,
        out_pool,
        freq,
        lambda_head,
        head_gain.reshape(1, -1),
        group_weight,
        pool_scale.reshape(heads, 1, GROUP_DIM),
    )


def solution(mesh):
    in_specs = (
        P("sp", "tp"),
        P(),
        P("sp", "tp"),
        P("sp", "tp"),
        P("sp", "tp"),
        P("sp", "tp"),
        P("sp", "tp"),
        P("sp", "tp"),
        P(),
        P(),
        P(),
        P(),
        P("tp", "sp"),
        P("tp", "sp"),
    )
    return jax.shard_map(
        functools.partial(body, mesh.shape["sp"], mesh.shape["tp"]),
        mesh=mesh,
        in_specs=in_specs,
        out_specs=P(("sp", "tp"), None),
        check_vma=False,
    )
```

```python
import functools

import jax
import jax.numpy as jnp
import numpy as np
from jax import lax
from jax.experimental import pallas as pl
from jax.experimental.pallas import tpu as pltpu
from jax.sharding import PartitionSpec as P

HEAD_DIM = 64
VALUE_DIM = 128
GROUP_DIM = 128
ROPE_BASE = 500000.0
HEAD_SCALE = 0.8
NORM_FLOOR = 1e-06
HEAD_FLOOR = 0.001
MASKED = -1e30
TAIL = 16
CHUNKS = 8
XY_HOME = (True, False)
XY_PARTNER = (True, True)
MESH = pl.DeviceIdType.MESH
BF16 = jnp.bfloat16
F32 = jnp.float32


def flip(index, bit):
    return index + bit * (1 - 2 * ((index // bit) % 2))


def kernel(
    sizes,
    tok_in,
    gain_ref,
    q1_in,
    k1_in,
    q2_in,
    k2_in,
    v_in,
    p_in,
    oa_in,
    ob_in,
    freq_ref,
    lam_ref,
    hg_ref,
    gw_in,
    ps_ref,
    out_ref,
    tok_ref,
    q1_ref,
    k1_ref,
    q2_ref,
    k2_ref,
    v_ref,
    p_ref,
    oa_ref,
    ob_ref,
    gw_ref,
    wp_ref,
    op_ref,
    ox_ref,
    cos_ref,
    sin_ref,
    ssq,
    tokbuf,
    nrm,
    w_all,
    o_all,
    kv,
    q_st,
    m_st,
    l_st,
    acc_st,
    pool,
    tail,
    prior,
    cat,
    part,
    sbuf,
    rbuf,
    fin,
    land,
    outb,
    tok_send,
    tok_recv,
    w_send,
    wx_send,
    wd_send,
    w_recv,
    o_send,
    od_send,
    o_recv,
    ox_send,
    ox_recv,
    kv_send,
    kvd_send,
    kv_recv,
    pp_send,
    pp_recv,
    cat_send,
    cat_recv,
    rs_send,
    rs_recv,
    fin_send,
    fin_recv,
    out_sem,
    in_sem,
):
    G, Q, TP = sizes
    S = 2 * G * Q
    R = 2 * Q
    s = lax.axis_index("sp")
    t = lax.axis_index("tp")
    r = s // G
    g = s % G
    q = r // 2
    b = r % 2
    y = t // 2
    c = t % 2
    other = s + 1 - 2 * g
    plane = 2 * q + c
    head = (2 * y + b) * G + g
    first = c == b
    second = c != b
    chunk, feats = tok_in.shape
    rows = G * chunk
    cols = op_ref.shape[1]
    span = G * R * cols // TP

    def half_of(p):
        return (p * G * cols // span) % 2

    def place_of(p, gg):
        start = p * G * cols
        return pl.multiple_of((start // span // 2) * span + start % span + gg * cols, cols)


    def dev(q_, b_, g_, y_, c_):
        return ((2 * q_ + b_) * G + g_, 2 * y_ + c_)

    xdev = dev(q, b, 1 - g, y, c)
    ydev = dev(q, b, g, 1 - y, c)
    cdev = dev(q, b, g, y, 1 - c)
    zdev = dev(q, 1 - b, g, y, c)

    x_dim = ("g", 1)
    y_dim = ("t", 2)
    members = 2 * G

    def member(mask):
        gg, tt = g, t
        for kind, bb in mask:
            if kind == "g":
                gg = flip(gg, bb)
            else:
                tt = flip(tt, bb)
        return gg, tt

    def device(mask):
        gg, tt = member(mask)
        return (r * G + gg, tt)

    barrier = pltpu.get_barrier_semaphore()

    loads = [
        pltpu.make_async_copy(src, dst, in_sem.at[i])
        for i, (src, dst) in enumerate(
            (
                (k1_in, k1_ref), (k2_in, k2_ref), (v_in, v_ref), (p_in, p_ref), (q1_in, q1_ref),
                (q2_in, q2_ref), (tok_in, tok_ref), (oa_in, oa_ref), (ob_in, ob_ref),
                (gw_in.at[head], gw_ref),
            )
        )
    ]
    for load in loads[:7]:
        load.start()

    def greet(where):
        pl.semaphore_signal(barrier, inc=1, device_id=where, device_id_type=MESH)

    greet(xdev)
    greet(ydev)
    greet(cdev)
    greet(zdev)
    greet(dev(q, 1 - b, 1 - g, y, b))
    greet(dev(q, 1 - b, g, 1 - y, b))

    @pl.when(first)
    def _():
        greet(dev(q, b, 1 - g, y, 1 - c))
        greet(dev(q, b, g, 1 - y, 1 - c))

        @pl.loop(0, R)
        def _(p):
            @pl.when(p != r)
            def _():
                greet((p * G + g, t))

    @pl.when(second)
    def _():
        greet(dev(q, 1 - b, g, y, 0))
        greet(dev(q, 1 - b, g, y, 1))

    @pl.loop(0, R)
    def _(p):
        @pl.when(jnp.logical_and(p != r, half_of(p) == b))
        def _():
            greet((p * G + g, t))

    @pl.loop(0, q)
    def _(e):
        greet(dev(e, b, g, y, c))

    @pl.when(jnp.logical_and(c == 0, q > 0))
    def _():
        greet(dev(q - 1, b, g, y, 1))

    def pack(gg):
        a, z = gg * HEAD_DIM, (gg + 1) * HEAD_DIM
        e, f = gg * VALUE_DIM, (gg + 1) * VALUE_DIM
        wp_ref[gg, :, 0:128] = jnp.concatenate([k1_ref[:, a:z], k2_ref[:, a:z]], axis=1)
        wp_ref[gg, :, 128:256] = v_ref[:, e:f]
        wp_ref[gg, :, 256:384] = p_ref[:, e:f]
        wp_ref[gg, :, 384:512] = jnp.concatenate([q1_ref[:, a:z], q2_ref[:, a:z]], axis=1)

    for load in loads[:6]:
        load.wait()
    for gg in range(G):
        pack(gg)
    loads[6].wait()
    for load in loads[7:]:
        load.start()

    one = lambda flag: jnp.where(flag, 1, 0)
    count = 4 + 6 * one(second) + 1 + Q - one(first) + Q - one(half_of(r) == b)
    count = count + (Q - 1 - q) + one(jnp.logical_and(c == 1, q < Q - 1))
    pl.semaphore_wait(barrier, count)

    def rdma(src, dst, ss, rs, where):
        return pltpu.make_async_remote_copy(
            src_ref=src, dst_ref=dst, send_sem=ss, recv_sem=rs, device_id=where, device_id_type=MESH
        )

    cross_to = jnp.where(first, s, S)
    cross_at = jnp.where(first, other, S)

    early = 2 * HEAD_DIM + VALUE_DIM + GROUP_DIM
    shares = (pl.ds(0, early), pl.ds(early, 2 * HEAD_DIM))
    slots = S + 1

    def w_cross(part_):
        cut = shares[part_]
        return rdma(
            wp_ref.at[1 - g, :, cut], w_all.at[cross_to, :, cut], wx_send.at[part_],
            w_recv.at[part_ * slots + cross_to], xdev,
        )

    def w_copy(part_, kind, e):
        cut = shares[part_]
        src = wp_ref.at[g, :, cut] if kind == 0 else w_all.at[cross_at, :, cut]
        slot = s if kind == 0 else other
        return rdma(
            src, w_all.at[slot, :, cut], w_send.at[(2 * part_ + kind) * Q + e],
            w_recv.at[part_ * slots + slot], dev(e, c, g, y, c),
        )

    def w_targets(act):
        for n in range(Q):
            e = (q + 1 + n) % Q
            if n == Q - 1:
                pl.when(second)(functools.partial(act, e))
            else:
                act(e)

    def w_start(part_, kind):
        w_targets(lambda e: w_copy(part_, kind, e).start())

    def w_pass(part_, slot, src=None):
        at = w_all.at[slot, :, shares[part_]]
        return rdma(
            at if src is None else src, at, wd_send,
            w_recv.at[part_ * slots + slot], cdev,
        )

    def tok_copy(src, xx, tt, n, index, where):
        at = pl.ds(n * (chunk // 2), chunk // 2)
        return rdma(
            src.at[at, :], tokbuf.at[xx, tt, at, :], tok_send.at[2 * index + n],
            tok_recv.at[2 * (xx * TP + tt) + n], where,
        )

    def tok_first(index, n):
        where = (
            dev(q, 1 - b, g, y, b),
            dev(q, b, g, 1 - y, b),
            dev(q, b, 1 - g, y, b),
            dev(q, b, g, y, b),
        )[index]
        return tok_copy(tok_ref, g, t, n, index, where)

    def tok_wait(xx, tt, n):
        tok_copy(tokbuf.at[xx, tt], xx, tt, n, 0, cdev).wait_recv()

    def z_pass(k, over_y, n):
        tt = 2 * y + k
        return tok_copy(tokbuf.at[g, tt], g, tt, n, 4 + 2 * k + over_y, ydev if over_y else xdev)

    def x_pass(k, n):
        xx, tt = 1 - g, 2 * y + k
        return tok_copy(tokbuf.at[xx, tt], xx, tt, n, 8 + k, ydev)

    def y_pass(k, n):
        xx, tt = g, 2 * (1 - y) + k
        return tok_copy(tokbuf.at[xx, tt], xx, tt, n, 8 + k, xdev)

    w_cross(0).start()
    for index in range(2):
        for n in range(2):
            tok_first(index, n).start()

    @pl.when(second)
    def _():
        for n in range(2):
            tok_first(3, n).start()

    tok_first(2, 0).start()
    w_cross(1).start()
    tok_first(2, 1).start()
    w_start(0, 0)

    @pl.when(first)
    def _():
        w_all[s] = wp_ref[g]
        tokbuf[g, t] = tok_ref[...]
        for i in range(2):
            w_pass(i, s, wp_ref.at[g, :, shares[i]]).start()

    for load in loads[7:]:
        load.wait()
    for gg in range(G):
        e, f = gg * VALUE_DIM, (gg + 1) * VALUE_DIM
        op_ref[gg, :, 0:128] = oa_ref[e:f, :].T
        op_ref[gg, :, 128:256] = ob_ref[e:f, :].T

    def o_at(core, p, gg):
        return o_all.at[core, pl.ds(place_of(p, gg), cols), :]

    def o_copy(kind, e):
        src, gg = (op_ref.at[g], g) if kind == 0 else (ox_ref, 1 - g)
        return rdma(
            src, o_at(c, r, gg), o_send.at[kind * Q + e], o_recv.at[c * S + r * G + gg],
            dev(e, half_of(r), g, y, c),
        )

    def o_targets(act, up=None):
        for n in range(Q):
            e = (q + 1 + n) % Q
            flag = half_of(r) != b if n == Q - 1 else None
            if up is not None:
                ahead = (e > q) == up
                flag = ahead if flag is None else jnp.logical_and(flag, ahead)
            if flag is None:
                act(e)
            else:
                pl.when(flag)(functools.partial(act, e))

    def o_start(kind, up):
        o_targets(lambda e: o_copy(kind, e).start(), up)

    def o_pass(p, gg):
        at = o_at(c, p, gg)
        index = p * G + gg
        return rdma(at, at, od_send, o_recv.at[c * S + index], cdev)

    def o_wait(core, p, gg):
        at = o_at(core, p, gg)
        rdma(at, at, od_send, o_recv.at[core * S + p * G + gg], cdev).wait_recv()

    def o_own(kind):
        gg = g if kind == 0 else 1 - g

        @pl.when(half_of(r) == b)
        def _():
            o_all[c, pl.ds(place_of(r, gg), cols), :] = op_ref[g] if kind == 0 else ox_ref[...]
            rdma(
                op_ref.at[g] if kind == 0 else ox_ref, o_at(c, r, gg), od_send,
                o_recv.at[c * S + r * G + gg], cdev,
            ).start()

    def o_cross():
        return rdma(op_ref.at[1 - g], ox_ref, ox_send, ox_recv, xdev)

    def o_relay(gg):
        @pl.loop(0, R)
        def _(p):
            @pl.when(jnp.logical_and(p != r, half_of(p) == b))
            def _():
                o_wait(c, p, gg)
                o_pass(p, gg).start()

    lane128 = lax.broadcasted_iota(jnp.int32, (chunk, 2 * HEAD_DIM), 1)
    sign = jnp.where(lane128 % HEAD_DIM < HEAD_DIM // 2, -1.0, 1.0)

    @pl.loop(0, G)
    def _(n):
        at = pl.ds(pl.multiple_of(n * chunk, chunk), chunk)
        spots = plane * rows + n * chunk + lax.broadcasted_iota(jnp.int32, (chunk, 2 * HEAD_DIM), 0)
        angles = spots.astype(F32) * freq_ref[...]
        cos_ref[at, :] = jnp.cos(angles)
        sin_ref[at, :] = jnp.sin(angles) * sign

    ssq[...] = jnp.zeros_like(ssq)

    def scale(xx, tt):
        at = pl.ds(pl.multiple_of(xx * chunk, chunk), chunk)
        x = tokbuf[xx, tt].astype(F32)
        ssq[at, :] = ssq[at, :] + jnp.sum(x * x, axis=-1, keepdims=True)
        nrm[at, pl.ds(pl.multiple_of(tt * feats, feats), feats)] = (x * gain_ref[tt]).astype(BF16)

    def w_wait(part_, slot):
        at = w_all.at[slot, :, shares[part_]]
        rdma(at, at, wd_send, w_recv.at[part_ * slots + slot], cdev).wait_recv()

    def early_relays(n):
        @pl.when(second)
        def _():
            for k in range(2):
                tok_wait(g, 2 * y + k, n)
                z_pass(k, 1, n).start()
                z_pass(k, 0, n).start()

        @pl.when(first)
        def _():
            for k in range(2):
                tok_wait(g, 2 * (1 - y) + k, n)
            tok_wait(g, 2 * y + 1 - c, n)

    early_relays(0)
    early_relays(1)
    w_wait(0, cross_at)
    w_start(0, 1)
    w_start(1, 0)

    @pl.when(first)
    def _():
        w_pass(0, other).start()
        for n in range(2):
            for k in range(2):
                tok_wait(1 - g, 2 * y + k, n)
                if XY_HOME[k]:
                    x_pass(k, n).start()
            if n == 0:
                w_wait(1, cross_at)
                w_start(1, 1)

    def w_relay(part_, gg):
        @pl.loop(1, R)
        def _(d):
            @pl.when(r - d >= 0)
            def _():
                w_wait(part_, (r - d) * G + gg)
                w_pass(part_, (r - d) * G + gg).start()

            @pl.when(r + d < R)
            def _():
                w_wait(part_, (r + d) * G + gg)
                w_pass(part_, (r + d) * G + gg).start()

    scale(g, 2 * y)
    scale(g, 2 * y + 1)

    @pl.when(first)
    def _():
        w_relay(0, g)
        for n in range(2):
            for k in range(2):
                if not XY_HOME[k]:
                    y_pass(k, n).start()

    @pl.when(second)
    def _():
        for n in range(2):
            for k in range(2):
                tok_wait(g, 2 * (1 - y) + k, n)
                if not XY_PARTNER[k]:
                    y_pass(k, n).start()
        w_wait(1, cross_at)
        w_start(1, 1)
        for n in range(2):
            for k in range(2):
                tok_wait(1 - g, 2 * y + k, n)
                if XY_PARTNER[k]:
                    x_pass(k, n).start()

    for k in range(2):
        scale(g, 2 * (1 - y) + k)
        scale(1 - g, 2 * y + k)

    @pl.when(first)
    def _():
        w_relay(0, 1 - g)

    o_cross().start()
    o_own(0)

    for k in range(2):
        for n in range(2):
            tok_wait(1 - g, 2 * (1 - y) + k, n)
        scale(1 - g, 2 * (1 - y) + k)

    @pl.when(second)
    def _():
        @pl.loop(0, S)
        def _(k):
            w_wait(0, k)

    ptile = chunk

    def rope(x, cosine, sine):
        lane = lax.broadcasted_iota(jnp.int32, x.shape, 1)
        near = jnp.where(
            lane % HEAD_DIM < HEAD_DIM // 2,
            pltpu.roll(x, x.shape[1] - HEAD_DIM // 2, 1),
            pltpu.roll(x, HEAD_DIM // 2, 1),
        )
        return x * cosine + near * sine

    def kv_part(k, n):
        return kv.at[k, pl.ds(pl.multiple_of(n * ptile, ptile), ptile), :]

    def kv_copy(e, n):
        at = kv_part(plane, n)
        return rdma(at, at, kv_send.at[2 * e + n], kv_recv.at[2 * plane + n], dev(e, b, g, y, c))

    def kv_pass(e, n):
        k = 2 * e + c
        at = kv_part(k, n)
        return rdma(at, at, kvd_send.at[2 * e + n], kv_recv.at[2 * k + n], cdev)

    def kv_wait(k, n):
        at = kv_part(k, n)
        rdma(at, at, kvd_send.at[0], kv_recv.at[2 * k + n], cdev).wait_recv()

    tail_copy = rdma(tail, prior, pp_send, pp_recv, (s + 2 * G * c, t + 1 - 2 * c))
    tail_out = jnp.logical_or(c == 0, q < Q - 1)
    tail_in = jnp.logical_or(c == 1, q > 0)

    o_start(0, False)

    def project(at, part_):
        weights = w_all[0:S, :, shares[part_]].reshape(TP * feats, shares[part_].size)
        inv = lax.rsqrt(ssq[at, :] / (TP * feats) + NORM_FLOOR)
        return jnp.dot(nrm[at, :], weights, preferred_element_type=F32) * inv

    @pl.loop(0, G)
    def _(m):
        n = G - 1 - m
        at = pl.ds(pl.multiple_of(n * ptile, ptile), ptile)
        out = project(at, 0)
        kv[plane, at, 0:128] = rope(out[:, 0:128], cos_ref[at, :], sin_ref[at, :]).astype(BF16)
        v = out[:, 128:256].astype(BF16)
        for i in range(ptile // VALUE_DIM):
            dst = pl.ds(pl.multiple_of(n * ptile + i * VALUE_DIM, VALUE_DIM), VALUE_DIM)
            kv[plane, dst, 128:256] = v[i * VALUE_DIM : (i + 1) * VALUE_DIM, :].T
        p = out[:, 256:384].astype(BF16)
        pool[pl.ds(pl.multiple_of(TAIL + n * ptile, TAIL), ptile), :] = p.astype(F32)

        @pl.when(m == 0)
        def _():
            tail[...] = p[ptile - TAIL :, :]

            @pl.when(tail_out)
            def _():
                tail_copy.start()

        @pl.loop(q + 1, Q)
        def _(e):
            kv_copy(e, n).start()

        @pl.when(c == 0)
        def _():
            kv_pass(q, n).start()

    @pl.when(first)
    def _():
        w_pass(1, other).start()
        w_relay(1, g)
        w_relay(1, 1 - g)

    @pl.when(second)
    def _():
        @pl.loop(0, S)
        def _(k):
            w_wait(1, k)

    o_cross().wait_recv()
    o_start(1, False)
    o_own(1)

    @pl.loop(0, G)
    def _(n):
        at = pl.ds(pl.multiple_of(n * ptile, ptile), ptile)
        qq = rope(project(at, 1), cos_ref[at, :], sin_ref[at, :]).astype(BF16)
        qq = qq * jnp.array(HEAD_DIM**-0.5, BF16)
        lane = lax.broadcasted_iota(jnp.int32, qq.shape, 1)
        zero = jnp.zeros_like(qq)
        at_b = pl.ds(pl.multiple_of(rows + n * ptile, ptile), ptile)
        q_st[:, at] = jnp.where(lane < HEAD_DIM, qq, zero).T
        q_st[:, at_b] = jnp.where(lane >= HEAD_DIM, qq, zero).T

    def attend(k, piece, diagonal):
        begin, size = (0, rows) if piece is None else (piece * ptile, ptile)
        values = jnp.concatenate(
            [
                kv[k, pl.ds(begin + i * VALUE_DIM, VALUE_DIM), 128:256]
                for i in range(size // VALUE_DIM)
            ],
            axis=1,
        )
        scores = jnp.dot(kv[k, pl.ds(begin, size), 0:128], q_st[...], preferred_element_type=F32)
        if diagonal:
            kpos = lax.broadcasted_iota(jnp.int32, scores.shape, 0)
            qpos = lax.broadcasted_iota(jnp.int32, scores.shape, 1) % rows
            scores = jnp.where(kpos <= qpos, scores, MASKED)
        top = jnp.max(scores, axis=0, keepdims=True)
        if not diagonal:
            old = m_st[...]
            top = jnp.maximum(old, top)
            factor = jnp.exp(old - top)
        weights = jnp.exp(scores - top)
        total = jnp.sum(weights, axis=0, keepdims=True)
        product = jnp.dot(values, weights.astype(BF16), preferred_element_type=F32)
        if not diagonal:
            total = total + l_st[...] * factor
            product = product + acc_st[...] * factor
        m_st[...] = top
        l_st[...] = total
        acc_st[...] = product

    attend(plane, None, True)

    @pl.when(tail_in)
    def _():
        tail_copy.wait_recv()
        pool[0:TAIL, :] = prior[...].astype(F32)

    @pl.when(jnp.logical_not(tail_in))
    def _():
        pool[0:TAIL, :] = jnp.zeros((TAIL, GROUP_DIM), F32)

    def cat_copy(i):
        return rdma(cat.at[b, i], cat.at[b, i], cat_send.at[i], cat_recv.at[i], zdev)

    ext = pool[...]
    kind = head % 4
    window = jnp.where(kind == 0, 2, jnp.where(kind == 1, 4, jnp.where(kind == 2, 8, 16)))
    run = ext + pltpu.roll(ext, 1, 0)
    chosen = run
    for power, lag in ((1, 2), (2, 4), (3, 8)):
        run = run + pltpu.roll(run, lag, 0)
        chosen = jnp.where(kind == power, run, chosen)
    spot = plane * rows + lax.broadcasted_iota(jnp.int32, (rows, GROUP_DIM), 0)
    counts = jnp.minimum(spot + 1, window).astype(F32)
    mean = chosen[TAIL:, :] / counts - ext[TAIL:, :]
    mixedg = jnp.dot(mean.astype(BF16), gw_ref[...], preferred_element_type=F32)
    cat[b, 1] = (mixedg * ps_ref[head]).astype(BF16)
    cat_copy(1).start()

    @pl.when(c == 1)
    def _():
        for n in range(G):
            kv_wait(2 * q, n)
        attend(2 * q, None, False)


    @pl.loop(0, q)
    def _(j):
        e = q - 1 - j
        for n in reversed(range(G)):
            kv_wait(2 * e + c, n)
            kv_pass(e, n).start()
            attend(2 * e + c, n, False)
        for n in range(G):
            kv_wait(2 * e + 1 - c, n)
        attend(2 * e + 1 - c, None, False)

    means = acc_st[...] / l_st[...]
    diff = means[:, :rows] - lam_ref[head] * means[:, rows:]
    inv = lax.rsqrt(jnp.mean(diff * diff, axis=0, keepdims=True) + HEAD_FLOOR)
    cat[b, 0] = ((diff * inv).T * hg_ref[...] * HEAD_SCALE).astype(BF16)
    cat_copy(0).start()

    for n in range(G):
        @pl.loop(q + 1, Q)
        def _(e):
            kv_copy(e, n).wait_send()

    def o_up():
        @pl.when(g == 0)
        def _():
            o_start(0, True)
            o_start(1, True)

        @pl.when(g == 1)
        def _():
            o_start(1, True)
            o_start(0, True)

    o_up()
    share = rows // members
    half = part.shape[2]
    start_at = place_of(r, 0) // half
    near = CHUNKS // Q

    def chunk_at(h):
        return (start_at + h) % CHUNKS

    def head_product(h, bb):
        both = jnp.concatenate([cat[bb, 0], cat[bb, 1]], axis=1)
        rows_at = pl.ds(pl.multiple_of(chunk_at(h) * half, half), half)
        return lax.dot_general(
            both, o_all[bb, rows_at, :], (((1,), (1,)), ((), ())), preferred_element_type=F32
        )

    for gg in range(G):
        pl.when(half_of(r) == b)(functools.partial(o_wait, 1 - c, r, gg))

    def own_product(h):
        part[h] = head_product(h, b)

    for h in range(near):
        own_product(h)
    cat_copy(1).wait_recv()
    cat_copy(0).wait_recv()
    orders = ([x_dim, y_dim], [y_dim, x_dim])

    def block(mask):
        gg, tt = member(mask)
        return pl.ds(pl.multiple_of((gg * 2 + tt // 2) * share, share), share)

    def combos(dims):
        found = [[]]
        for dim in dims:
            found = found + [mask + [dim] for mask in found]
        return found

    plans = []
    for h in range(CHUNKS):
        order = orders[h % 2]
        stages = []
        base = 0
        for i, dim in enumerate(order):
            masks = combos(order[i + 1 :])
            stages.append((dim, masks, base))
            base += len(masks)
        plans.append(stages)

    def rs_copy(h, dim, mask, index):
        at = block([dim] + mask)
        return rdma(
            sbuf.at[h, at, :], rbuf.at[h, index], rs_send, rs_recv.at[h, index],
            device([dim]),
        )

    def rs_start(h, i):
        dim, masks, base = plans[h][i]
        for n, mask in enumerate(masks):
            at = block([dim] + mask)
            sbuf[h, at, :] = part[h, at, :].astype(BF16)
        for n, mask in enumerate(masks):
            rs_copy(h, dim, mask, base + n).start()

    def rs_finish(h, i):
        dim, masks, base = plans[h][i]
        for n, mask in enumerate(masks):
            rs_copy(h, dim, mask, base + n).wait_recv()
            at = block(mask)
            part[h, at, :] = part[h, at, :] + rbuf[h, base + n].astype(F32)

    def out_product(h):
        part[h] = head_product(h, b) + head_product(h, 1 - b)

    mine = block([])
    lines = share // 2

    def pass_copy(h):
        at = pl.ds(pl.multiple_of((1 - c) * lines, lines), lines)
        return rdma(fin.at[h, at, :], land.at[0, h], fin_send, fin_recv.at[0, h], cdev)

    def home_copies(h):
        dim = plans[h][1][0]
        found = []
        for n, mask in enumerate(([], [dim])):
            gg, tt = member(mask)
            for core in range(2):
                start = (gg * 2 + tt // 2) * share + core * lines
                at = pl.ds(pl.multiple_of(start, lines), lines)
                found.append(
                    rdma(
                        sbuf.at[h, at, :], land.at[1 + n, h], fin_send,
                        fin_recv.at[1 + n, h], dev(q, c, gg, tt // 2, core),
                    )
                )
        return found

    def home_start(h):
        dim = plans[h][1][0]
        for mask in ([], [dim]):
            sbuf[h, block(mask), :] = part[h, block(mask), :].astype(BF16)
        for copy in home_copies(h):
            copy.start()

    def columns(hb, h):
        start = chunk_at(h) * half
        return pl.ds(pl.multiple_of((2 * (start // span) + hb) * span + start % span, half), half)

    def put(hb, h):
        at = columns(hb, h)
        return pltpu.make_async_copy(outb.at[:, at], out_ref.at[:, at], out_sem)

    for h in range(near):
        part[h] = part[h] + head_product(h, 1 - b)
        rs_start(h, 0)
    def far_weights(gg):
        o_relay(gg)

        @pl.loop(0, R)
        def _(p):
            @pl.when(jnp.logical_and(p != r, half_of(p) == b))
            def _():
                o_wait(1 - c, p, gg)

    in_turn = near > 0 and cols % half == 0
    for gg in range(G):
        far_weights(gg)
        if in_turn or gg == G - 1:
            for h in range(near, CHUNKS):
                if not in_turn or (h * half // cols) % G == gg:
                    out_product(h)
                    rs_start(h, 0)
    for h in range(CHUNKS):
        rs_finish(h, 0)
        pl.when(first)(functools.partial(rs_start, h, 1))
        pl.when(second)(functools.partial(home_start, h))
    def last_sum(h):
        rs_finish(h, 1)
        fin[h] = part[h, mine, :].astype(BF16)
        pass_copy(h).start()
        outb[:, columns(b, h)] = fin[h, pl.ds(pl.multiple_of(c * lines, lines), lines), :]
        put(b, h).start()

    @pl.when(first)
    def _():
        for h in range(CHUNKS):
            last_sum(h)


    def arrived(i, h):
        rdma(land.at[i, h], land.at[i, h], fin_send, fin_recv.at[i, h], cdev).wait_recv()

    for h in range(CHUNKS):
        arrived(1, h)
        arrived(2, h)
        both = land[1, h].astype(F32) + land[2, h].astype(F32)
        outb[:, columns(1 - b, h)] = both.astype(BF16)
        put(1 - b, h).start()

    @pl.when(second)
    def _():
        for h in range(CHUNKS):
            arrived(0, h)
            outb[:, columns(b, h)] = land[0, h]
            put(b, h).start()

    for i in range(2):
        w_cross(i).wait_send()
        for kind in range(2):
            w_targets(lambda e: w_copy(i, kind, e).wait_send())

    for n in range(2):
        for i in range(3):
            tok_first(i, n).wait_send()

        @pl.when(second)
        def _():
            tok_first(3, n).wait_send()
            for k in range(2):
                z_pass(k, 1, n).wait_send()
                z_pass(k, 0, n).wait_send()
                (x_pass if XY_PARTNER[k] else y_pass)(k, n).wait_send()

        @pl.when(first)
        def _():
            for k in range(2):
                (x_pass if XY_HOME[k] else y_pass)(k, n).wait_send()

    o_cross().wait_send()
    for i in range(2):
        cat_copy(i).wait_send()
    for kind in range(2):
        o_targets(lambda e: o_copy(kind, e).wait_send())

    @pl.when(tail_out)
    def _():
        tail_copy.wait_send()

    for n in range(G):
        @pl.loop(0, q + 1 - c)
        def _(e):
            kv_pass(e, n).wait_send()

    def sent(src, sem):
        rdma(src, src, sem, in_sem.at[0], cdev).wait_send()

    @pl.when(first)
    def _():
        sent(w_all.at[0:S], wd_send)
        sent(sbuf.at[0 : CHUNKS * 3 // 4], rs_send)
        sent(fin.at[0 : CHUNKS // 2], fin_send)

    @pl.when(second)
    def _():
        sent(sbuf.at[0 : CHUNKS // 2], rs_send)
        sent(sbuf.at[0 : CHUNKS // 2], fin_send)

    sent(o_all.at[0], od_send)
    pltpu.make_async_copy(outb, out_ref, out_sem).wait()


def body(
    sp,
    tp,
    tokens,
    norm_gain,
    query_one,
    key_one,
    query_two,
    key_two,
    value_weight,
    pool_weight,
    lambda_head,
    head_gain,
    group_weight,
    pool_scale,
    out_attn,
    out_pool,
):
    G = query_one.shape[1] // HEAD_DIM
    assert G == 2 and tp == 2 * G and sp % (2 * G) == 0
    R = sp // G
    Q = R // 2
    chunk, feats = tokens.shape
    rows = G * chunk
    depth = query_one.shape[0]
    cols = out_attn.shape[1]
    heads = lambda_head.shape[0]
    members = 2 * G
    share = rows // members

    half_dim = HEAD_DIM // 2
    inverse = ROPE_BASE ** (-((np.arange(2 * HEAD_DIM) % half_dim) * 2.0 / HEAD_DIM))
    freq = jnp.asarray(inverse.astype(np.float32).reshape(1, -1))
    width = 4 * HEAD_DIM + VALUE_DIM + GROUP_DIM
    depth_out = VALUE_DIM + GROUP_DIM
    total_cols = sp * cols
    vm = pl.BlockSpec(memory_space=pltpu.VMEM)
    far = pl.BlockSpec(memory_space=pl.ANY)
    dma = pltpu.SemaphoreType.DMA
    return pl.pallas_call(
        functools.partial(kernel, (G, Q, tp)),
        out_shape=jax.ShapeDtypeStruct((rows // (G * tp), total_cols), BF16),
        in_specs=[far, vm] + [far] * 8 + [vm, pl.BlockSpec(memory_space=pltpu.SMEM), vm, far, vm],
        out_specs=pl.BlockSpec(memory_space=pl.ANY),
        scratch_shapes=[
            pltpu.VMEM((chunk, feats), BF16),
            pltpu.VMEM((depth, G * HEAD_DIM), BF16),
            pltpu.VMEM((depth, G * HEAD_DIM), BF16),
            pltpu.VMEM((depth, G * HEAD_DIM), BF16),
            pltpu.VMEM((depth, G * HEAD_DIM), BF16),
            pltpu.VMEM((depth, G * VALUE_DIM), BF16),
            pltpu.VMEM((depth, G * GROUP_DIM), BF16),
            pltpu.VMEM((G * VALUE_DIM, cols), BF16),
            pltpu.VMEM((G * GROUP_DIM, cols), BF16),
            pltpu.VMEM((GROUP_DIM, GROUP_DIM), BF16),
            pltpu.VMEM((G, depth, width), BF16),
            pltpu.VMEM((G, cols, depth_out), BF16),
            pltpu.VMEM((cols, depth_out), BF16),
            pltpu.VMEM((rows, 2 * HEAD_DIM), F32),
            pltpu.VMEM((rows, 2 * HEAD_DIM), F32),
            pltpu.VMEM((rows, 1), F32),
            pltpu.VMEM((G, tp, chunk, feats), BF16),
            pltpu.VMEM((rows, tp * feats), BF16),
            pltpu.VMEM((sp + 1, depth, width), BF16),
            pltpu.VMEM((2, total_cols // 2, depth_out), BF16),
            pltpu.VMEM((R, rows, 256), BF16),
            pltpu.VMEM((128, 2 * rows), BF16),
            pltpu.VMEM((1, 2 * rows), F32),
            pltpu.VMEM((1, 2 * rows), F32),
            pltpu.VMEM((VALUE_DIM, 2 * rows), F32),
            pltpu.VMEM((TAIL + rows, GROUP_DIM), F32),
            pltpu.VMEM((TAIL, GROUP_DIM), BF16),
            pltpu.VMEM((TAIL, GROUP_DIM), BF16),
            pltpu.VMEM((2, 2, rows, 128), BF16),
            pltpu.VMEM((CHUNKS, rows, total_cols // 2 // CHUNKS), F32),
            pltpu.VMEM((CHUNKS, rows, total_cols // 2 // CHUNKS), BF16),
            pltpu.VMEM((CHUNKS, members - 1, share, total_cols // 2 // CHUNKS), BF16),
            pltpu.VMEM((CHUNKS, share, total_cols // 2 // CHUNKS), BF16),
            pltpu.VMEM((3, CHUNKS, share // 2, total_cols // 2 // CHUNKS), BF16),
            pltpu.VMEM((rows // (G * tp), total_cols), BF16),
            dma((20,)),
            dma((2 * G * tp,)),
            dma((4 * Q,)),
            dma((2,)),
            dma,
            dma((2 * (sp + 1),)),
            dma((2 * Q,)),
            dma,
            dma((2 * sp,)),
            dma,
            dma,
            dma((2 * Q,)),
            dma((2 * Q,)),
            dma((2 * R,)),
            dma,
            dma,
            dma((2,)),
            dma((2,)),
            dma,
            dma((CHUNKS, members - 1)),
            dma,
            dma((3, CHUNKS)),
            dma,
            dma((10,)),
        ],
        compiler_params=pltpu.CompilerParams(
            collective_id=0, has_side_effects=True, vmem_limit_bytes=58 * 1024 * 1024
        ),
    )(
        tokens,
        norm_gain.reshape(tp, 1, feats),
        query_one,
        key_one,
        query_two,
        key_two,
        value_weight,
        pool_weight,
        out_attn,
        out_pool,
        freq,
        lambda_head,
        head_gain.reshape(1, -1),
        group_weight,
        pool_scale.reshape(heads, 1, GROUP_DIM),
    )


def solution(mesh):
    in_specs = (
        P("sp", "tp"),
        P(),
        P("sp", "tp"),
        P("sp", "tp"),
        P("sp", "tp"),
        P("sp", "tp"),
        P("sp", "tp"),
        P("sp", "tp"),
        P(),
        P(),
        P(),
        P(),
        P("tp", "sp"),
        P("tp", "sp"),
    )
    return jax.shard_map(
        functools.partial(body, mesh.shape["sp"], mesh.shape["tp"]),
        mesh=mesh,
        in_specs=in_specs,
        out_specs=P(("sp", "tp"), None),
        check_vma=False,
    )
```
